128 devices in a mesh: sp: 16 (over z, y), tp: 8 (over x, core).
Axes of the slice: x: 4, y: 4, z: 4, core: 2. Of those that a mesh axis runs over, the one named last changes fastest.
Arguments:
- gate_branch: bfloat16 [12288, 1024], P('sp', 'tp'), may hold values from -6 to 6
- recur_input: bfloat16 [12288, 1024], P('sp', 'tp'), may hold values from -6 to 6
- doc_ids: int32 [12288], P('sp'), may hold values from 0 to 7, never falling along the last dimension, each value on 1 to 4608 neighbouring positions
- conv_taps: bfloat16 [4, 1024], P(None, 'tp'), may hold values from -3 to 3
- gate_map: bfloat16 [16, 64, 64], P('tp'), may hold values from -0.75 to 0.75
- input_map: bfloat16 [16, 64, 64], P('tp'), may hold values from -0.75 to 0.75
- decay_level: float32 [1024], P('tp'), may hold values from 4.8 to 12.3
- decay_extra: float32 [12288, 1024], P('sp', 'tp'), may hold values from -2.1 to -1.9e-05
- out_weight: bfloat16 [1024, 2048], P(None, 'tp'), may hold values from -0.7875 to 0.7875
- residual: bfloat16 [12288, 2048], P('sp', 'tp'), may hold values from -44 to 44
- mix_gain: float32 [2048], P('tp'), may hold values from 0.1 to 1.9
- pre_gain: float32 [2048], P('tp'), may hold values from 0.1 to 1.9
- ffn_gain: float32 [2048], P('tp'), may hold values from 0.1 to 1.9
- gate_weight: bfloat16 [2048, 5632], P('sp', 'tp'), may hold values from -0.125 to 0.125
- up_weight: bfloat16 [2048, 5632], P('sp', 'tp'), may hold values from -0.125 to 0.125
- down_weight: bfloat16 [5632, 2048], P('tp', 'sp'), may hold values from -0.33579113 to 0.33579113
Outputs:
- layer_out: bfloat16 [12288, 2048], P('sp', 'tp')
The draws below stay inside these ranges and needn't reach their ends.
Inputs may be any that keep to these rules, and one draw needn't show every extreme that they name: `doc_ids`: document numbers start at 0 and never fall along the sequence; a document has 1 to 4608 positions, and one has exactly that many.
All inputs are finite; a program needn't handle non-finite values.
Results may differ from the reference program's by a relative error of at most 0.013.
Values may be sent and summed in bfloat16 or wider, within the bound.
A program may use at most 64 MiB of HBM per device.

```python
import math
import jax
import jax.numpy as jnp
import numpy as np
from jax import lax

D = 2048
W = 1024
HEAD = 64
FF = 5632
KCONV = 4
TOK_DEV = 768
TOKENS = 12288
DOCS = 8
N_TP = 8


def column_scales(key, columns, spread):
    ramp = jnp.exp(jnp.log(spread) * jnp.arange(columns, dtype=jnp.float32) / (columns - 1))
    jitter = jnp.exp(jax.random.uniform(key, (columns,), jnp.float32, math.log(0.7), math.log(1.4)))
    return ramp * jitter / math.sqrt(spread)


def scaled_matrix(key, row_count, columns):
    spread = 3.0
    keys = jax.random.split(key, 2)
    base = jnp.clip(jax.random.normal(keys[0], (row_count, columns), jnp.float32), -6.0, 6.0)
    return base * row_count ** (-0.5) * column_scales(keys[1], columns, spread)


def draw_out_weight(key, part):
    return scaled_matrix(jax.random.fold_in(key, 11), W, D).astype(jnp.bfloat16)


def draw_down_weight(key, part):
    return scaled_matrix(jax.random.fold_in(key, 12), FF, D).astype(jnp.bfloat16)


def draw_residual(key, part):
    keys = jax.random.split(jax.random.fold_in(key, 13), 3)
    spread = 3.0
    base = jnp.clip(jax.random.normal(keys[0], (TOKENS, D), jnp.float32), -6.0, 6.0)
    row_scale = jnp.exp(jax.random.uniform(keys[1], (TOKENS, 1), jnp.float32, math.log(0.3), math.log(3.0)))
    return (base * row_scale * column_scales(keys[2], D, spread)).astype(jnp.bfloat16)


def draw_decay_level(key, part):
    keys = jax.random.split(jax.random.fold_in(key, 14), 3)
    share = 0.5
    fast_heads = jax.random.uniform(keys[0], (W // HEAD, 1), jnp.float32) < share
    fast = jnp.broadcast_to(fast_heads, (W // HEAD, HEAD)).reshape(W)
    fast_rate = jnp.exp(jax.random.uniform(keys[1], (W,), jnp.float32, math.log(0.0025), math.log(0.008)))
    slow_rate = jnp.exp(jax.random.uniform(keys[2], (W,), jnp.float32, math.log(5e-06), math.log(2e-05)))
    target = jnp.where(fast, fast_rate, slow_rate)
    return -jnp.log(jnp.expm1(target))


def draw_decay_extra(key, part):
    keys = jax.random.split(jax.random.fold_in(key, 15), 3)
    blocks = TOKENS // TOK_DEV
    baseline = jnp.exp(jax.random.uniform(keys[0], (blocks, 1, W), jnp.float32, math.log(2e-05), math.log(0.0001)))
    baseline = jnp.broadcast_to(baseline, (blocks, TOK_DEV, W)).reshape(TOKENS, W)
    spots = jax.random.randint(keys[1], (3,), 0, TOKENS)
    hits = jnp.sum((jnp.arange(TOKENS)[:, None] == spots[None, :]).astype(jnp.float32), axis=1)
    kept = jax.random.uniform(keys[2], (TOKENS, W), jnp.float32, 0.5, 0.8)
    return -baseline + hits[:, None] * jnp.log(kept)


def level_of(stream_key, extent, cuts, low, high):
    def one(axis_at, blocks):
        draws = jax.random.uniform(jax.random.fold_in(jax.random.fold_in(stream_key, 6), axis_at), (blocks,), jnp.float32, low / len(cuts), high / len(cuts))
        return jnp.repeat(jnp.exp(draws), extent[axis_at] // blocks).reshape((-1,) + (1,) * (len(extent) - axis_at - 1))

    gain = one(*cuts[0])
    for cut in cuts[1:]:
        gain = gain * one(*cut)
    return gain


def length_profile(number_of, total, most, skew):
    loads = [(1 << 20) // math.isqrt(standing ** skew) + 1 for standing in range(2, number_of + 1)]
    spare, counts = total - most - (number_of - 1), [1] * (number_of - 1)
    while spare > 0:
        free = [i for i in range(number_of - 1) if counts[i] < most]
        whole, left = sum([loads[i] for i in free]), spare
        for i in free:
            addition = min(most - counts[i], max(1, left * loads[i] // whole), spare)
            counts[i] = counts[i] + addition
            spare = spare - addition
    return np.array([most] + counts)


def uneven_parts(stream_key, amount, total, most, lean):
    if amount == 2:
        one = jax.random.randint(stream_key, (), max(1, total - most), min(most, total - 1) + 1)
        return jnp.stack([one, total - one])
    sizes = jnp.asarray(length_profile(amount, total, most, lean), jnp.int32)
    couples = (amount - 1) // 2
    donor, taker = sizes[1:1 + 2 * couples:2], sizes[2:2 + 2 * couples:2]
    room = jnp.minimum(donor - 1, most - taker)
    passed = jax.random.randint(jax.random.fold_in(stream_key, 1), (couples,), 0, 1 << 20) % (room + 1)
    sizes = sizes.at[1:1 + 2 * couples:2].set(donor - passed).at[2:2 + 2 * couples:2].set(taker + passed)
    return sizes[jax.random.permutation(jax.random.fold_in(stream_key, 2), amount)]


def centred(key, shape, width, most, cuts=(), kind=jnp.bfloat16):
    loudness = level_of(key, shape, cuts, -0.22, 0.18) if cuts else 1.0
    entries = jax.random.normal(key, shape, jnp.float32) * width * loudness
    return jnp.minimum(jnp.maximum(entries, -most), most).astype(kind)


def setup_inputs(seed: int = 0) -> dict:
    arg_keys = jax.random.split(jax.random.key(seed), 17)
    return {
        "gate_branch": centred(arg_keys[0], (TOKENS, W), 1.0, 6.0, ((0, 16), (1, 8))),
        "recur_input": centred(arg_keys[1], (TOKENS, W), 1.0, 6.0, ((0, 16), (1, 8))),
        "doc_ids": jnp.searchsorted(jnp.cumsum(uneven_parts(arg_keys[2], DOCS, TOKENS, 6 * TOK_DEV, 0)), jnp.arange(TOKENS), side="right").astype(jnp.int32),
        "conv_taps": centred(arg_keys[3], (KCONV, W), 0.5, 3.0, ((1, 8),)),
        "gate_map": centred(arg_keys[4], (W // HEAD, HEAD, HEAD), HEAD ** -0.5, 0.75, ((0, 8),)),
        "input_map": centred(arg_keys[5], (W // HEAD, HEAD, HEAD), HEAD ** -0.5, 0.75, ((0, 8),)),
        "decay_level": draw_decay_level(jax.random.fold_in(arg_keys[16], 71), 0),
        "decay_extra": draw_decay_extra(jax.random.fold_in(arg_keys[16], 71), 0),
        "out_weight": draw_out_weight(jax.random.fold_in(arg_keys[16], 71), 0),
        "residual": draw_residual(jax.random.fold_in(arg_keys[16], 71), 0),
        "mix_gain": jnp.clip(1.0 + 0.18 * jax.random.normal(arg_keys[10], (D,), jnp.float32), 0.1, 1.9),
        "pre_gain": jnp.clip(1.0 + 0.18 * jax.random.normal(arg_keys[11], (D,), jnp.float32), 0.1, 1.9),
        "ffn_gain": jnp.clip(1.0 + 0.18 * jax.random.normal(arg_keys[12], (D,), jnp.float32), 0.1, 1.9),
        "gate_weight": centred(arg_keys[13], (D, FF), D ** -0.5, 0.125, ((0, 16), (1, 8))),
        "up_weight": centred(arg_keys[14], (D, FF), D ** -0.5, 0.125, ((0, 16), (1, 8))),
        "down_weight": draw_down_weight(jax.random.fold_in(arg_keys[16], 71), 0),
    }


epsilon = 1e-06
gate_power = 8.0

def combine(earlier, latter):
    return (earlier[0] * latter[0], latter[0] * earlier[1] + latter[1])

def inverse_rms(values, columns):
    return lax.rsqrt(lax.optimization_barrier(jnp.sum(values * values, axis=1, keepdims=True)) / columns + epsilon)

def reference(gate_branch, recur_input, doc_ids, conv_taps, gate_map, input_map, decay_level, decay_extra, out_weight, residual, mix_gain, pre_gain, ffn_gain, gate_weight, up_weight, down_weight):
    reach_rows = KCONV - 1
    padded_ids = jnp.concatenate([jnp.full((reach_rows,), -1, jnp.int32), doc_ids.astype(jnp.int32)])
    padded_rows = jnp.concatenate([jnp.zeros((reach_rows, W), jnp.float32), recur_input.astype(jnp.float32)])
    tap_weights = conv_taps.astype(jnp.float32)
    convolved = jnp.zeros((TOKENS, W), jnp.float32)
    for offset in range(KCONV):
        start_row = reach_rows - offset
        same_doc = (padded_ids[start_row:start_row + TOKENS] == doc_ids).astype(jnp.float32)[:, None]
        convolved = convolved + same_doc * padded_rows[start_row:start_row + TOKENS] * tap_weights[offset]
    conv_out = convolved.astype(jnp.bfloat16)
    head_rows = conv_out.astype(jnp.float32).reshape(TOKENS, W // HEAD, HEAD)
    recur_gate = jax.nn.sigmoid(jnp.einsum('thd,hde->the', head_rows, gate_map.astype(jnp.float32)).reshape(TOKENS, W))
    input_gate = jax.nn.sigmoid(jnp.einsum('thd,hde->the', head_rows, input_map.astype(jnp.float32)).reshape(TOKENS, W))
    log_decay = gate_power * -jax.nn.softplus(-decay_level) * recur_gate + decay_extra
    continues = (padded_ids[reach_rows - 1:reach_rows - 1 + TOKENS] == doc_ids).astype(jnp.float32)[:, None]
    factor = jnp.exp(log_decay) * continues
    driven = jnp.sqrt(-jnp.expm1(2.0 * log_decay)) * input_gate * conv_out.astype(jnp.float32)
    products, states = lax.associative_scan(combine, (factor, driven), axis=0)
    branch = (states * jax.nn.gelu(gate_branch.astype(jnp.float32))).astype(jnp.bfloat16)
    mixed_out = jnp.dot(branch, out_weight, preferred_element_type=jnp.float32).astype(jnp.bfloat16)
    mixed_f = mixed_out.astype(jnp.float32)
    stream = (residual.astype(jnp.float32) + mixed_f * inverse_rms(mixed_f, D) * mix_gain).astype(jnp.bfloat16)
    stream_f = stream.astype(jnp.float32)
    normed = (stream_f * inverse_rms(stream_f, D) * pre_gain).astype(jnp.bfloat16)
    gate_act = jnp.dot(normed, gate_weight, preferred_element_type=jnp.float32)
    up_act = jnp.dot(normed, up_weight, preferred_element_type=jnp.float32)
    hidden = (jax.nn.silu(gate_act) * up_act).astype(jnp.bfloat16)
    span_cols = FF // N_TP
    ffn_sum = jnp.zeros((TOKENS, D), jnp.float32)
    for member in range(N_TP):
        partial_value = jnp.dot(hidden[:, member * span_cols:(member + 1) * span_cols], down_weight[member * span_cols:(member + 1) * span_cols], preferred_element_type=jnp.float32)
        ffn_sum = ffn_sum + lax.optimization_barrier(partial_value.astype(jnp.bfloat16)).astype(jnp.float32)
    ffn_out = ffn_sum.astype(jnp.bfloat16)
    ffn_f = ffn_out.astype(jnp.float32)
    return (stream_f + ffn_f * inverse_rms(ffn_f, D) * ffn_gain).astype(jnp.bfloat16)
```

```python
import jax
import jax.numpy as jnp
from jax import lax
from jax.experimental import pallas as pl
from jax.experimental.pallas import tpu as pltpu
from jax.sharding import PartitionSpec as P

MESH = pl.DeviceIdType.MESH
F32 = jnp.float32
BF16 = jnp.bfloat16

D = 2048
EPS = 1e-06
GATE_POWER = 8.0
TOK = 768
BLK = 96
HALF = 384
CH = 128
HID = 704
REACH = 6


def neg_expm1(u):
    series = 1.0 + u * (1.0 / 9.0)
    for n in (8.0, 7.0, 6.0, 5.0, 4.0, 3.0, 2.0):
        series = 1.0 + u * (1.0 / n) * series
    return jnp.where(u > -0.5, -u * series, 1.0 - jnp.exp(u))


def softplus(v):
    tail = jnp.exp(-jnp.abs(v))
    w = tail / (2.0 + tail)
    square = w * w
    series = jnp.full_like(w, 1.0 / 15.0)
    for n in (13.0, 11.0, 9.0, 7.0, 5.0, 3.0, 1.0):
        series = 1.0 / n + square * series
    return jnp.maximum(v, 0.0) + 2.0 * w * series


class TorusGather:
    def __init__(self, buf, rows, here, ring_send, ring_recv, pair_send, pair_recv):
        self.buf, self.rows = buf, rows
        self.z, self.y, self.c, self.t = here
        self.ring_send, self.ring_recv = ring_send, ring_recv
        self.pair_send, self.pair_recv = pair_send, pair_recv

    def slot(self, dz, dy):
        return lax.rem(self.z + dz, 4) * 4 + lax.rem(self.y + dy, 4)

    def at(self, half, a, b):
        return (a, b) if half == 0 else (b, a)

    def span(self, half, part):
        quarter = self.rows // 4
        first = half * 2 * quarter
        return (first, 2 * quarter) if part is None else (first + part * quarter, quarter)

    def piece(self, half, where, part=None):
        first, count = self.span(half, part)
        return self.buf.at[self.c, self.slot(*where), pl.ds(first, count)]

    def send(self, half, where, to, part=None):
        ref = self.piece(half, where, part)
        landed = ((where[0] - to[0]) % 4, (where[1] - to[1]) % 4)
        pltpu.make_async_remote_copy(
            src_ref=ref,
            dst_ref=ref,
            send_sem=self.ring_send,
            recv_sem=self.ring_recv.at[half, landed[0] * 4 + landed[1]],
            device_id=(self.slot(*to), self.t),
            device_id_type=MESH,
        ).start()

    def wait(self, half, where):
        ref = self.piece(half, where)
        pltpu.make_async_copy(ref, ref, self.ring_recv.at[half, where[0] * 4 + where[1]]).wait()
        self.pass_over(ref)

    def pass_over(self, ref):
        pltpu.make_async_remote_copy(
            src_ref=ref,
            dst_ref=ref,
            send_sem=self.pair_send,
            recv_sem=self.pair_recv,
            device_id=(self.slot(0, 0), self.t + 1 - 2 * self.c),
            device_id_type=MESH,
        ).start()

    def start(self):
        for first in (True, False):
            for half in (0, 1):
                for step in (1, 3):
                    to = self.at(half, 0, step) if first else self.at(half, step, 0)
                    self.send(half, (0, 0), to)
        self.pass_over(self.buf.at[self.c, self.slot(0, 0)])

    def spread(self, half, b):
        for step in (1, 3):
            self.send(half, self.at(half, 0, b), self.at(half, step, 0))

    def event(self, number):
        at = self.at
        for half in (0, 1):
            if number == 1:
                self.wait(half, at(half, 0, 3))
                self.send(half, at(half, 0, 3), at(half, 0, 1), part=0)
                self.wait(half, at(half, 0, 1))
                self.send(half, at(half, 0, 1), at(half, 0, 3), part=1)
        for half in (0, 1):
            if number == 1:
                self.spread(half, 3)
                self.spread(half, 1)
            if number == 2:
                self.wait(half, at(half, 0, 2))
                self.spread(half, 2)
            if number == 3:
                self.wait(half, at(half, 3, 0))
                self.send(half, at(half, 3, 0), at(half, 1, 0))
                self.wait(half, at(half, 1, 0))
            if number == 4:
                self.wait(half, at(half, 1, 3))
                self.send(half, at(half, 1, 3), at(half, 3, 0))
                self.wait(half, at(half, 3, 3))
            if number == 5:
                self.wait(half, at(half, 3, 1))
                self.send(half, at(half, 3, 1), at(half, 1, 0))
                self.wait(half, at(half, 1, 1))
            if number == 6:
                self.wait(half, at(half, 1, 2))
                self.send(half, at(half, 1, 2), at(half, 3, 0))
                self.wait(half, at(half, 3, 2))
            if number == 7:
                for b in (0, 3, 1, 2):
                    self.wait(half, at(half, 2, b))

    def wait_pair(self):
        ref = self.buf.at[1 - self.c]
        pltpu.make_async_copy(ref, ref, self.pair_recv).wait()

    def finish(self):
        ref = self.buf.at[self.c, pl.ds(0, 15)]
        pltpu.make_async_copy(ref, ref, self.ring_send).wait()
        ref = self.buf.at[self.c]
        pltpu.make_async_copy(ref, ref, self.pair_send).wait()


def layer_kernel(
    gate_ref, rec_ref, ids_ref, taps_ref, gmap_ref, imap_ref, level_ref, extra_ref, ow_ref, res_ref,
    mixg_ref, preg_ref, ffng_ref, gw_ref, uw_ref, dw_ref,
    out_ref,
    GU, DW, OW, BR, BRR, RB, GS, GB, HX, HI, XF, IDF, FA, DV, S, PR, GL, CS, CB, MX, ST, NB, H,
    PB, RA, RC, FO, SQS, SQB, XS, XR, PG,
    gu_ring, dw_ring, gu_sem, dw_sem, ow_ring, ow_sem, ag_ring, rs_recv, rs_send, sem,
):
    s, t = lax.axis_index("sp"), lax.axis_index("tp")
    z, y = lax.div(s, 4), lax.rem(s, 4)
    x, c = lax.div(t, 2), lax.rem(t, 2)
    mine = c * 4 + x

    def remote(src, dst, send_sem, recv_sem, device):
        copy = pltpu.make_async_remote_copy(
            src_ref=src, dst_ref=dst, send_sem=send_sem, recv_sem=recv_sem, device_id=device, device_id_type=MESH
        )
        copy.start()

    def await_bytes(ref, semaphore):
        pltpu.make_async_copy(ref, ref, semaphore).wait()

    def along_x(step):
        return (s, lax.rem(x + step, 4) * 2 + c)

    partner = (s, t + 1 - 2 * c)
    here = (z, y, c, t)
    gu = TorusGather(GU, 128, here, gu_sem.at[0], gu_ring, gu_sem.at[1], gu_sem.at[2])
    dw = TorusGather(DW, HID, here, dw_sem.at[0], dw_ring, dw_sem.at[1], dw_sem.at[2])

    barrier = pltpu.get_barrier_semaphore()
    for k in range(1, REACH + 1):
        for peer in (lax.rem(s + k, 16), lax.rem(s + 16 - k, 16)):
            pl.semaphore_signal(barrier, inc=1, device_id=(peer, t), device_id_type=MESH)
    for k in range(1, 8):
        pl.semaphore_signal(barrier, inc=1, device_id=(s, lax.rem(t + k, 8)), device_id_type=MESH)

    own = z * 4 + y
    for i in range(5):
        GU[c, own, :, 256 * i : 256 * i + 128] = gw_ref[:, 128 * i : 128 * i + 128]
        GU[c, own, :, 256 * i + 128 : 256 * i + 256] = uw_ref[:, 128 * i : 128 * i + 128]
    GU[c, own, :, 1280:1408] = jnp.concatenate([gw_ref[:, 640:704], uw_ref[:, 640:704]], axis=1)
    OW[c, x] = ow_ref[...]
    DW[c, own] = dw_ref[...]
    GS[...] = jnp.zeros_like(GS)
    GS[0:1] = mixg_ref[...]
    GS[1:2] = preg_ref[...]
    GS[2:3] = ffng_ref[...]
    GB[t] = GS[...]
    RB[t] = res_ref[mine]
    IDF[8:] = jnp.concatenate(
        [jnp.broadcast_to(ids_ref[r : r + 1, :].astype(F32), (128, 128)).T for r in range(6)], axis=0
    )
    XF[8:] = rec_ref[...].astype(F32)

    pl.semaphore_wait(barrier, 2 * REACH + 7)

    after = (lax.rem(s + 1, 16), t)
    remote(rec_ref.at[pl.ds(TOK - 16, 16)], HX, sem.at[0], sem.at[1], after)
    remote(ids_ref, HI, sem.at[2], sem.at[3], after)
    gu.start()
    for part, step in ((0, 1), (1, 3), (1, 1), (0, 3)):
        ref = OW.at[c, x, pl.ds(512 * part, 512)]
        remote(ref, ref, ow_sem.at[0], ow_ring.at[0 if step == 1 else 1, part], along_x(step))
    remote(OW.at[c, x], OW.at[c, x], ow_sem.at[1], ow_sem.at[2], partner)
    for k in range(1, 8):
        peer = lax.rem(t + k, 8)
        remote(GS, GB.at[t], sem.at[4], sem.at[5], (s, peer))
        block = lax.rem(peer, 2) * 4 + lax.div(peer, 2)
        remote(res_ref.at[block], RB.at[t], sem.at[6], sem.at[7], (s, peer))

    for r in range(6):
        rows = slice(128 * r, 128 * r + 128)
        GL[rows] = jax.nn.gelu(gate_ref[rows].astype(F32), approximate=True)
    pair = [
        jnp.concatenate(
            [
                jnp.concatenate([m[0].astype(F32), jnp.zeros((64, 64), F32)], axis=1),
                jnp.concatenate([jnp.zeros((64, 64), F32), m[1].astype(F32)], axis=1),
            ],
            axis=0,
        )
        for m in (gmap_ref, imap_ref)
    ]
    maps = jnp.concatenate(pair, axis=1).astype(BF16)
    rate = -GATE_POWER * softplus(-level_ref[...])
    taps = taps_ref[...].astype(F32)

    await_bytes(HX, sem.at[1])
    await_bytes(HI, sem.at[3])
    XF[0:8] = HX[...].astype(F32)[8:16]
    rim_ids = jnp.broadcast_to(HI[5:6, :].astype(F32), (128, 128)).T[120:128]
    IDF[0:8] = jnp.where(s > 0, rim_ids, -1.0)

    for r in range(6):
        at = 8 + 128 * r
        ids = IDF[at : at + 128]
        conv = XF[at : at + 128] * taps[0:1]
        for k in (1, 2, 3):
            same = IDF[at - k : at - k + 128] == ids
            conv = conv + jnp.where(same, XF[at - k : at - k + 128], 0.0) * taps[k : k + 1]
        conv = conv.astype(BF16)
        gates = jax.nn.sigmoid(jnp.dot(conv, maps, preferred_element_type=F32))
        rows = slice(128 * r, 128 * r + 128)
        log_decay = rate * gates[:, :CH] + extra_ref[rows]
        FA[rows] = jnp.where(IDF[at - 1 : at + 127] == ids, jnp.exp(log_decay), 0.0)
        DV[rows] = jnp.sqrt(neg_expm1(2.0 * log_decay)) * gates[:, CH:] * conv.astype(F32)

    state = jnp.zeros((8, CH), F32)
    prod = jnp.ones((8, CH), F32)
    for i in range(BLK):
        at = pl.ds(i, 8, stride=BLK)
        f = FA[at, :]
        state = f * state + DV[at, :]
        prod = f * prod
        S[at, :] = state
        PR[at, :] = prod
    befores = []
    p_all, e_all = jnp.ones((1, CH), F32), jnp.zeros((1, CH), F32)
    for b in range(8):
        befores.append((p_all, e_all))
        e_all = prod[b : b + 1] * e_all + state[b : b + 1]
        p_all = prod[b : b + 1] * p_all
    CS[...] = jnp.concatenate([p_all, e_all, jnp.zeros((6, CH), F32)], axis=0)
    gu.event(1)
    for k in range(1, REACH + 1):
        remote(CS, CB.at[k - 1], sem.at[8], sem.at[9], (lax.rem(s + k, 16), t))

    def ow_event(number):
        if number == 0:
            for part, step in ((0, 1), (1, 3)):
                came = lax.rem(x + 4 - step, 4)
                ref = OW.at[c, came, pl.ds(512 * part, 512)]
                await_bytes(ref, ow_ring.at[0 if step == 1 else 1, part])
                remote(ref, ref, ow_sem.at[0], ow_ring.at[2, part], along_x(step))
                remote(ref, ref, ow_sem.at[1], ow_sem.at[2], partner)
        if number == 1:
            for part, step in ((1, 1), (0, 3)):
                came = lax.rem(x + 4 - step, 4)
                ref = OW.at[c, came, pl.ds(512 * part, 512)]
                await_bytes(ref, ow_ring.at[0 if step == 1 else 1, part])
                remote(ref, ref, ow_sem.at[1], ow_sem.at[2], partner)
        if number == 2:
            came = lax.rem(x + 2, 4)
            for part in (0, 1):
                ref = OW.at[c, came, pl.ds(512 * part, 512)]
                await_bytes(ref, ow_ring.at[2, part])
                remote(ref, ref, ow_sem.at[1], ow_sem.at[2], partner)

    ow_event(0)

    await_bytes(CB, sem.at[9])
    entering = jnp.zeros((1, CH), F32)
    for k in range(REACH, 0, -1):
        entering = jnp.where(s >= k, CB[k - 1, 0:1] * entering + CB[k - 1, 1:2], 0.0)
    for b in range(8):
        rows = slice(BLK * b, BLK * b + BLK)
        p_before, e_before = befores[b]
        states = S[rows] + PR[rows] * (e_before + p_before * entering)
        BR[b] = (states * GL[rows]).astype(BF16)
    BRR[t] = BR[mine]
    gu.event(2)
    for k in range(1, 8):
        peer = lax.rem(t + k, 8)
        block = lax.rem(peer, 2) * 4 + lax.div(peer, 2)
        remote(BR.at[block], BRR.at[t], sem.at[10], sem.at[11], (s, peer))
    gu.event(3)
    gu.event(4)
    ow_event(1)
    gu.event(5)
    dw.start()
    ow_event(2)

    await_bytes(GB.at[pl.ds(0, 7)], sem.at[5])
    await_bytes(RB.at[pl.ds(0, 7)], sem.at[7])
    await_bytes(BRR.at[pl.ds(0, 7)], sem.at[11])
    await_bytes(OW.at[1 - c], ow_sem.at[2])
    PG[...] = jnp.concatenate([GB[j, 1:2] for j in range(8)], axis=1)
    branch = jnp.concatenate([BRR[j] for j in range(8)], axis=1)
    square = jnp.zeros((BLK, 1), F32)
    for j in range(8):
        mixed = jnp.dot(branch, OW[j % 2, j // 2], preferred_element_type=F32).astype(BF16).astype(F32)
        square = square + jnp.sum(mixed * mixed, axis=1, keepdims=True)
        MX[:, 256 * j : 256 * j + 256] = mixed
    scale = lax.rsqrt(square * (1.0 / D) + EPS)
    for j in range(8):
        cols = slice(256 * j, 256 * j + 256)
        mixed = MX[:, cols] * scale * GB[j, 0:1]
        ST[x, :, cols] = (RB[j].astype(F32) + mixed).astype(BF16)

    for part, step in ((0, 1), (1, 3), (1, 1), (0, 3)):
        ref = ST.at[x, pl.ds(48 * part, 48)]
        remote(ref, ref, sem.at[12], ag_ring.at[0 if step == 1 else 1, part], along_x(step))
    gu.event(6)
    for part, step in ((0, 1), (1, 3)):
        came = lax.rem(x + 4 - step, 4)
        ref = ST.at[came, pl.ds(48 * part, 48)]
        await_bytes(ref, ag_ring.at[0 if step == 1 else 1, part])
        remote(ref, ref, sem.at[12], ag_ring.at[2, part], along_x(step))
    gu.event(7)
    gu.wait_pair()

    def feed_forward_in(blocks):
        rows = BLK * len(blocks)
        for n, q in enumerate(blocks):
            for r in range(0, BLK, 16):
                stream = ST[q, r : r + 16].astype(F32)
                total = jnp.sum(stream * stream, axis=1, keepdims=True)
                NB[n, r : r + 16] = (stream * lax.rsqrt(total * (1.0 / D) + EPS) * PG[...]).astype(BF16)

        def lhs():
            return NB[0 : len(blocks)].reshape(rows, D)

        def half(p, carry):
            for i in range(5):
                weights = GU[p, :, :, 256 * i : 256 * i + 256].reshape(D, 256)
                both = jnp.dot(lhs(), weights, preferred_element_type=F32)
                act = (jax.nn.silu(both[:, :128]) * both[:, 128:]).astype(BF16)
                for n, q in enumerate(blocks):
                    H[p, q, :, 128 * i : 128 * i + 128] = act[BLK * n : BLK * n + BLK]
            return carry

        lax.fori_loop(0, 2, half, 0)
        weights = jnp.concatenate([GU[p, :, :, 1280:1408].reshape(D, 128) for p in (0, 1)], axis=1)
        both = jnp.dot(lhs(), weights, preferred_element_type=F32)
        for p in (0, 1):
            tail = both[:, 128 * p : 128 * p + 128]
            act = (jax.nn.silu(tail[:, :64]) * tail[:, 64:]).astype(BF16)
            for n, q in enumerate(blocks):
                H[p, q, :, 640:704] = act[BLK * n : BLK * n + BLK]

    left, right, across = lax.rem(x + 3, 4), lax.rem(x + 1, 4), lax.rem(x + 2, 4)
    feed_forward_in([x])
    dw.event(1)
    for part, step in ((1, 1), (0, 3)):
        came = lax.rem(x + 4 - step, 4)
        await_bytes(ST.at[came, pl.ds(48 * part, 48)], ag_ring.at[0 if step == 1 else 1, part])
    dw.event(2)
    dw.event(3)
    feed_forward_in([left, right])
    dw.event(4)
    for part in (0, 1):
        await_bytes(ST.at[across, pl.ds(48 * part, 48)], ag_ring.at[2, part])
    feed_forward_in([across])
    dw.event(5)
    dw.event(6)
    dw.event(7)
    dw.wait_pair()

    def down(chip, h):
        total = None
        for p in (0, 1):
            weights = jnp.concatenate([DW[p, 4 * chip + 2 * h], DW[p, 4 * chip + 2 * h + 1]], axis=1)
            part = jnp.dot(H[p].reshape(HALF, HID), weights, preferred_element_type=F32)
            total = part if total is None else total + part
        return total

    for h, step in ((0, 1), (1, 3)):
        PB[h] = down(across, h).astype(BF16)
        remote(PB.at[h], RA.at[h], rs_send.at[h], rs_recv.at[h], along_x(step))
    for n, (chip, h, step) in enumerate(((right, 1, 1), (left, 0, 3))):
        PB[2 + n] = down(chip, h).astype(BF16)
        remote(PB.at[2 + n], RC.at[n], rs_send.at[2 + n], rs_recv.at[2 + n], along_x(step))
    FO[0] = down(right, 0)
    FO[1] = down(left, 1)
    for n, step in enumerate((1, 3)):
        await_bytes(RA.at[n], rs_recv.at[n])
        PB[4 + n] = (FO[n] + RA[n].astype(F32)).astype(BF16)
        remote(PB.at[4 + n], RC.at[2 + n], rs_send.at[4 + n], rs_recv.at[4 + n], along_x(step))
    for h in (0, 1):
        FO[h] = down(x, h)
    for n, h in ((0, 1), (1, 0)):
        await_bytes(RC.at[n], rs_recv.at[2 + n])
        FO[h] = FO[h] + RC[n].astype(F32)
    square = jnp.zeros((HALF, 1), F32)
    for n, h in ((0, 0), (1, 1)):
        await_bytes(RC.at[2 + n], rs_recv.at[4 + n])
        total = (FO[h] + RC[2 + n].astype(F32)).astype(BF16).astype(F32)
        FO[h] = total
        square = square + jnp.sum(total * total, axis=1, keepdims=True)

    SQS[...] = jnp.broadcast_to(square, (HALF, 128)).T[0:8]
    for step in (1, 2, 3):
        remote(SQS, SQB.at[step - 1], sem.at[13], sem.at[14], along_x(step))
    await_bytes(SQB, sem.at[14])
    square = SQS[0:1] + SQB[0, 0:1] + SQB[1, 0:1] + SQB[2, 0:1]
    scale = lax.rsqrt(square * (1.0 / D) + EPS)
    scale = jnp.broadcast_to(scale, (128, HALF)).T
    scale = jnp.concatenate([scale, scale], axis=1)
    for h in (0, 1):
        cols = pl.ds(pl.multiple_of(512 * x + 256 * h, 256), 256)
        stream = ST[:, :, cols].reshape(HALF, 256).astype(F32)
        XS[h] = (stream + FO[h] * scale * GB[2 * x + h, 2:3]).astype(BF16)
    remote(XS.at[1 - c], XR, sem.at[15], sem.at[16], partner)
    out_ref[c] = XS[c]

    gu.finish()
    dw.finish()
    await_bytes(HX, sem.at[0])
    await_bytes(HI, sem.at[2])
    await_bytes(GB.at[pl.ds(0, 7)], sem.at[4])
    await_bytes(RB.at[pl.ds(0, 7)], sem.at[6])
    await_bytes(CB, sem.at[8])
    await_bytes(BRR.at[pl.ds(0, 7)], sem.at[10])
    await_bytes(OW.at[c, pl.ds(0, 3)], ow_sem.at[0])
    await_bytes(OW.at[c], ow_sem.at[1])
    await_bytes(ST.at[pl.ds(0, 3)], sem.at[12])
    for n in range(6):
        await_bytes(PB.at[n], rs_send.at[n])
    await_bytes(SQB, sem.at[13])
    await_bytes(XS.at[0], sem.at[15])
    await_bytes(XR, sem.at[16])
    out_ref[1 - c] = XR[...]


def body(
    gate_branch, recur_input, doc_ids, conv_taps, gate_map, input_map, decay_level, decay_extra, out_weight,
    residual, mix_gain, pre_gain, ffn_gain, gate_weight, up_weight, down_weight,
):
    vmem = pl.BlockSpec(memory_space=pltpu.VMEM)
    dma = pltpu.SemaphoreType.DMA
    out = pl.pallas_call(
        layer_kernel,
        name="layer",
        out_shape=jax.ShapeDtypeStruct((2, HALF, 256), BF16),
        in_specs=[vmem] * 16,
        out_specs=vmem,
        scratch_shapes=[
            pltpu.VMEM((2, 16, 128, 1408), BF16),
            pltpu.VMEM((2, 16, HID, 128), BF16),
            pltpu.VMEM((2, 4, 1024, 256), BF16),
            pltpu.VMEM((8, BLK, CH), BF16),
            pltpu.VMEM((8, BLK, CH), BF16),
            pltpu.VMEM((8, BLK, 256), BF16),
            pltpu.VMEM((8, 256), F32),
            pltpu.VMEM((8, 8, 256), F32),
            pltpu.VMEM((16, CH), BF16),
            pltpu.VMEM((6, 128), jnp.int32),
            pltpu.VMEM((TOK + 8, CH), F32),
            pltpu.VMEM((TOK + 8, CH), F32),
            pltpu.VMEM((TOK, CH), F32),
            pltpu.VMEM((TOK, CH), F32),
            pltpu.VMEM((TOK, CH), F32),
            pltpu.VMEM((TOK, CH), F32),
            pltpu.VMEM((TOK, CH), F32),
            pltpu.VMEM((8, CH), F32),
            pltpu.VMEM((REACH, 8, CH), F32),
            pltpu.VMEM((BLK, D), F32),
            pltpu.VMEM((4, BLK, D), BF16),
            pltpu.VMEM((2, BLK, D), BF16),
            pltpu.VMEM((2, 4, BLK, HID), BF16),
            pltpu.VMEM((6, HALF, 256), BF16),
            pltpu.VMEM((2, HALF, 256), BF16),
            pltpu.VMEM((4, HALF, 256), BF16),
            pltpu.VMEM((2, HALF, 256), F32),
            pltpu.VMEM((8, HALF), F32),
            pltpu.VMEM((3, 8, HALF), F32),
            pltpu.VMEM((2, HALF, 256), BF16),
            pltpu.VMEM((HALF, 256), BF16),
            pltpu.VMEM((1, D), F32),
            dma((2, 16)),
            dma((2, 16)),
            dma((3,)),
            dma((3,)),
            dma((3, 2)),
            dma((3,)),
            dma((3, 2)),
            dma((6,)),
            dma((6,)),
            dma((17,)),
        ],
        compiler_params=pltpu.CompilerParams(
            collective_id=0, has_side_effects=True, vmem_limit_bytes=60 * 1024 * 1024
        ),
    )(
        gate_branch,
        recur_input,
        doc_ids.reshape(6, 128),
        conv_taps,
        gate_map,
        input_map,
        decay_level.reshape(1, CH),
        decay_extra,
        out_weight,
        residual.reshape(8, BLK, 256),
        mix_gain.reshape(1, 256),
        pre_gain.reshape(1, 256),
        ffn_gain.reshape(1, 256),
        gate_weight,
        up_weight,
        down_weight,
    )
    return out.reshape(TOK, 256)


def solution(mesh):
    return jax.shard_map(
        body,
        mesh=mesh,
        in_specs=(
            P("sp", "tp"),
            P("sp", "tp"),
            P("sp"),
            P(None, "tp"),
            P("tp", None, None),
            P("tp", None, None),
            P("tp"),
            P("sp", "tp"),
            P(None, "tp"),
            P("sp", "tp"),
            P("tp"),
            P("tp"),
            P("tp"),
            P("sp", "tp"),
            P("sp", "tp"),
            P("tp", "sp"),
        ),
        out_specs=P("sp", "tp"),
        check_vma=False,
    )
```

```python
import jax
import jax.numpy as jnp
from jax import lax
from jax.experimental import pallas as pl
from jax.experimental.pallas import tpu as pltpu
from jax.sharding import PartitionSpec as P

MESH = pl.DeviceIdType.MESH
F32 = jnp.float32
BF16 = jnp.bfloat16

D = 2048
EPS = 1e-06
GATE_POWER = 8.0
TOK = 768
BLK = 96
HALF = 384
CH = 128
HID = 704
REACH = 6


def neg_expm1(u):
    series = 1.0 + u * (1.0 / 9.0)
    for n in (8.0, 7.0, 6.0, 5.0, 4.0, 3.0, 2.0):
        series = 1.0 + u * (1.0 / n) * series
    return jnp.where(u > -0.5, -u * series, 1.0 - jnp.exp(u))


def softplus(v):
    tail = jnp.exp(-jnp.abs(v))
    w = tail / (2.0 + tail)
    square = w * w
    series = jnp.full_like(w, 1.0 / 15.0)
    for n in (13.0, 11.0, 9.0, 7.0, 5.0, 3.0, 1.0):
        series = 1.0 / n + square * series
    return jnp.maximum(v, 0.0) + 2.0 * w * series


class TorusGather:
    def __init__(self, buf, rows, here, ring_send, ring_recv, pair_send, pair_recv):
        self.buf, self.rows = buf, rows
        self.z, self.y, self.c, self.t = here
        self.ring_send, self.ring_recv = ring_send, ring_recv
        self.pair_send, self.pair_recv = pair_send, pair_recv

    def slot(self, dz, dy):
        return lax.rem(self.z + dz, 4) * 4 + lax.rem(self.y + dy, 4)

    def at(self, half, a, b):
        return (a, b) if half == 0 else (b, a)

    def span(self, half, part):
        quarter = self.rows // 4
        first = half * 2 * quarter
        return (first, 2 * quarter) if part is None else (first + part * quarter, quarter)

    def piece(self, half, where, part=None):
        first, count = self.span(half, part)
        return self.buf.at[self.c, self.slot(*where), pl.ds(first, count)]

    def send(self, half, where, to, part=None):
        ref = self.piece(half, where, part)
        landed = ((where[0] - to[0]) % 4, (where[1] - to[1]) % 4)
        pltpu.make_async_remote_copy(
            src_ref=ref,
            dst_ref=ref,
            send_sem=self.ring_send,
            recv_sem=self.ring_recv.at[half, landed[0] * 4 + landed[1]],
            device_id=(self.slot(*to), self.t),
            device_id_type=MESH,
        ).start()

    def wait(self, half, where):
        ref = self.piece(half, where)
        pltpu.make_async_copy(ref, ref, self.ring_recv.at[half, where[0] * 4 + where[1]]).wait()
        self.pass_over(ref)

    def pass_over(self, ref):
        pltpu.make_async_remote_copy(
            src_ref=ref,
            dst_ref=ref,
            send_sem=self.pair_send,
            recv_sem=self.pair_recv,
            device_id=(self.slot(0, 0), self.t + 1 - 2 * self.c),
            device_id_type=MESH,
        ).start()

    def start(self):
        for half in (0, 1):
            for step in (1, 3):
                self.send(half, (0, 0), self.at(half, 0, step))

    def start_second(self):
        for half in (0, 1):
            for step in (1, 3):
                self.send(half, (0, 0), self.at(half, step, 0))
        self.pass_over(self.buf.at[self.c, self.slot(0, 0)])

    def spread(self, half, b):
        for step in (1, 3):
            self.send(half, self.at(half, 0, b), self.at(half, step, 0))

    def event(self, number):
        at = self.at
        for half in (0, 1):
            if number == 1:
                self.wait(half, at(half, 0, 3))
                self.send(half, at(half, 0, 3), at(half, 0, 1), part=0)
                self.wait(half, at(half, 0, 1))
                self.send(half, at(half, 0, 1), at(half, 0, 3), part=1)
        for half in (0, 1):
            if number == 1:
                self.spread(half, 3)
                self.spread(half, 1)
            if number == 2:
                self.wait(half, at(half, 0, 2))
                self.spread(half, 2)
            if number == 3:
                self.wait(half, at(half, 3, 0))
                self.send(half, at(half, 3, 0), at(half, 1, 0))
                self.wait(half, at(half, 1, 0))
            if number == 4:
                self.wait(half, at(half, 1, 3))
                self.send(half, at(half, 1, 3), at(half, 3, 0))
                self.wait(half, at(half, 3, 3))
            if number == 5:
                self.wait(half, at(half, 3, 1))
                self.send(half, at(half, 3, 1), at(half, 1, 0))
                self.wait(half, at(half, 1, 1))
            if number == 6:
                self.wait(half, at(half, 1, 2))
                self.send(half, at(half, 1, 2), at(half, 3, 0))
                self.wait(half, at(half, 3, 2))
            if number == 7:
                for b in (0, 3, 1, 2):
                    self.wait(half, at(half, 2, b))

    def wait_pair(self):
        ref = self.buf.at[1 - self.c]
        pltpu.make_async_copy(ref, ref, self.pair_recv).wait()

    def finish(self):
        ref = self.buf.at[self.c, pl.ds(0, 15)]
        pltpu.make_async_copy(ref, ref, self.ring_send).wait()
        ref = self.buf.at[self.c]
        pltpu.make_async_copy(ref, ref, self.pair_send).wait()


def layer_kernel(
    gate_hbm, rec_hbm, ids_hbm, taps_hbm, gmap_hbm, imap_hbm, level_hbm, extra_hbm, ow_hbm, res_hbm,
    mixg_hbm, preg_hbm, ffng_hbm, gw_hbm, uw_hbm, dw_hbm,
    out_ref,
    gate_ref, rec_ref, ids_ref, taps_ref, gmap_ref, imap_ref, level_ref, extra_ref, res_ref,
    mixg_ref, preg_ref, ffng_ref, gw_ref, uw_ref,
    GU, DW, OW, BR, BRR, RB, GS, GB, HX, HI, XF, IDF, FA, DV, S, PR, GL, CS, CB, MX, ST, NB, H,
    PB, RA, RC, PO, FO, SQB, XR, PG,
    gu_ring, dw_ring, gu_sem, dw_sem, ow_ring, ow_sem, ag_ring, rs_recv, rs_send, in_sem, sem,
):
    s, t = lax.axis_index("sp"), lax.axis_index("tp")
    z, y = lax.div(s, 4), lax.rem(s, 4)
    x, c = lax.div(t, 2), lax.rem(t, 2)
    mine = c * 4 + x

    def remote(src, dst, send_sem, recv_sem, device):
        copy = pltpu.make_async_remote_copy(
            src_ref=src, dst_ref=dst, send_sem=send_sem, recv_sem=recv_sem, device_id=device, device_id_type=MESH
        )
        copy.start()

    def await_bytes(ref, semaphore):
        pltpu.make_async_copy(ref, ref, semaphore).wait()

    def along_x(step):
        return (s, lax.rem(x + step, 4) * 2 + c)

    partner = (s, t + 1 - 2 * c)
    here = (z, y, c, t)
    gu = TorusGather(GU, 128, here, gu_sem.at[0], gu_ring, gu_sem.at[1], gu_sem.at[2])
    dw = TorusGather(DW, HID, here, dw_sem.at[0], dw_ring, dw_sem.at[1], dw_sem.at[2])

    barrier = pltpu.get_barrier_semaphore()
    for k in range(1, REACH + 1):
        for peer in (lax.rem(s + k, 16), lax.rem(s + 16 - k, 16)):
            pl.semaphore_signal(barrier, inc=1, device_id=(peer, t), device_id_type=MESH)
    for k in range(1, 8):
        pl.semaphore_signal(barrier, inc=1, device_id=(s, lax.rem(t + k, 8)), device_id_type=MESH)

    own = z * 4 + y
    loads = []
    for src, dst in (
        (gw_hbm, gw_ref), (uw_hbm, uw_ref), (rec_hbm, rec_ref), (ids_hbm, ids_ref), (mixg_hbm, mixg_ref),
        (preg_hbm, preg_ref), (ffng_hbm, ffng_ref), (ow_hbm, OW.at[c, x]), (gate_hbm, gate_ref), (taps_hbm, taps_ref),
        (gmap_hbm, gmap_ref), (imap_hbm, imap_ref), (level_hbm, level_ref), (extra_hbm, extra_ref),
        (res_hbm, res_ref), (dw_hbm, DW.at[c, own]),
    ):
        loads.append(pltpu.make_async_copy(src, dst, in_sem.at[len(loads)]))
        loads[-1].start()

    loads[0].wait()
    loads[1].wait()
    for i in range(5):
        for n, ref in enumerate((gw_ref, uw_ref)):
            block = ref[128 * i : 128 * i + 128].astype(F32).T.astype(BF16)
            GU[c, own, :, 256 * i + 128 * n : 256 * i + 128 * n + 128] = block
    block = jnp.concatenate([gw_ref[640:704].astype(F32), uw_ref[640:704].astype(F32)], axis=0)
    GU[c, own, :, 1280:1408] = block.T.astype(BF16)
    for load in loads[2:8]:
        load.wait()
    GS[...] = jnp.zeros_like(GS)
    GS[0:1] = mixg_ref[...]
    GS[1:2] = preg_ref[...]
    GS[2:3] = ffng_ref[...]
    GB[t] = GS[...]
    IDF[8:] = jnp.concatenate(
        [jnp.broadcast_to(ids_ref[r : r + 1, :].astype(F32), (128, 128)).T for r in range(6)], axis=0
    )
    XF[8:] = rec_ref[...].astype(F32)

    pl.semaphore_wait(barrier, 2 * REACH + 7)

    after = (lax.rem(s + 1, 16), t)
    remote(rec_ref.at[pl.ds(TOK - 16, 16)], HX, sem.at[0], sem.at[1], after)
    remote(ids_ref, HI, sem.at[2], sem.at[3], after)
    gu.start()
    for part, step in ((0, 1), (1, 3), (1, 1), (0, 3)):
        ref = OW.at[c, x, pl.ds(512 * part, 512)]
        remote(ref, ref, ow_sem.at[0], ow_ring.at[0 if step == 1 else 1, part], along_x(step))
    remote(OW.at[c, x], OW.at[c, x], ow_sem.at[1], ow_sem.at[2], partner)
    for k in range(1, 8):
        peer = lax.rem(t + k, 8)
        remote(GS, GB.at[t], sem.at[4], sem.at[5], (s, peer))
    for load in loads[8:]:
        load.wait()
    RB[t] = res_ref[mine]

    for r in range(6):
        rows = slice(128 * r, 128 * r + 128)
        GL[rows] = jax.nn.gelu(gate_ref[rows].astype(F32), approximate=True)
    pair = [
        jnp.concatenate(
            [
                jnp.concatenate([m[0].astype(F32), jnp.zeros((64, 64), F32)], axis=1),
                jnp.concatenate([jnp.zeros((64, 64), F32), m[1].astype(F32)], axis=1),
            ],
            axis=0,
        )
        for m in (gmap_ref, imap_ref)
    ]
    maps = jnp.concatenate(pair, axis=1).astype(BF16)
    rate = -GATE_POWER * softplus(-level_ref[...])
    taps = taps_ref[...].astype(F32)

    await_bytes(HX, sem.at[1])
    await_bytes(HI, sem.at[3])
    XF[0:8] = HX[...].astype(F32)[8:16]
    rim_ids = jnp.broadcast_to(HI[5:6, :].astype(F32), (128, 128)).T[120:128]
    IDF[0:8] = jnp.where(s > 0, rim_ids, -1.0)

    for r in range(6):
        at = 8 + 128 * r
        ids = IDF[at : at + 128]
        conv = XF[at : at + 128] * taps[0:1]
        for k in (1, 2, 3):
            same = IDF[at - k : at - k + 128] == ids
            conv = conv + jnp.where(same, XF[at - k : at - k + 128], 0.0) * taps[k : k + 1]
        conv = conv.astype(BF16)
        gates = jax.nn.sigmoid(jnp.dot(conv, maps, preferred_element_type=F32))
        rows = slice(128 * r, 128 * r + 128)
        log_decay = rate * gates[:, :CH] + extra_ref[rows]
        FA[rows] = jnp.where(IDF[at - 1 : at + 127] == ids, jnp.exp(log_decay), 0.0)
        DV[rows] = jnp.sqrt(neg_expm1(2.0 * log_decay)) * gates[:, CH:] * conv.astype(F32)

    state = jnp.zeros((8, CH), F32)
    prod = jnp.ones((8, CH), F32)
    for i in range(BLK):
        at = pl.ds(i, 8, stride=BLK)
        f = FA[at, :]
        state = f * state + DV[at, :]
        prod = f * prod
        S[at, :] = state
        PR[at, :] = prod
    befores = []
    p_all, e_all = jnp.ones((1, CH), F32), jnp.zeros((1, CH), F32)
    for b in range(8):
        befores.append((p_all, e_all))
        e_all = prod[b : b + 1] * e_all + state[b : b + 1]
        p_all = prod[b : b + 1] * p_all
    CS[...] = jnp.concatenate([p_all, e_all, jnp.zeros((6, CH), F32)], axis=0)
    for k in range(1, REACH + 1):
        remote(CS, CB.at[k - 1], sem.at[17], sem.at[9], (lax.rem(s + k, 16), t))
    gu.start_second()
    gu.event(1)

    def ow_event(number):
        if number == 0:
            for part, step in ((0, 1), (1, 3)):
                came = lax.rem(x + 4 - step, 4)
                ref = OW.at[c, came, pl.ds(512 * part, 512)]
                await_bytes(ref, ow_ring.at[0 if step == 1 else 1, part])
                remote(ref, ref, ow_sem.at[0], ow_ring.at[2, part], along_x(step))
                remote(ref, ref, ow_sem.at[1], ow_sem.at[2], partner)
        if number == 1:
            for part, step in ((1, 1), (0, 3)):
                came = lax.rem(x + 4 - step, 4)
                ref = OW.at[c, came, pl.ds(512 * part, 512)]
                await_bytes(ref, ow_ring.at[0 if step == 1 else 1, part])
                remote(ref, ref, ow_sem.at[1], ow_sem.at[2], partner)
        if number == 2:
            came = lax.rem(x + 2, 4)
            for part in (0, 1):
                ref = OW.at[c, came, pl.ds(512 * part, 512)]
                await_bytes(ref, ow_ring.at[2, part])
                remote(ref, ref, ow_sem.at[1], ow_sem.at[2], partner)

    ow_event(0)

    await_bytes(CB, sem.at[9])
    entering = jnp.zeros((1, CH), F32)
    for k in range(REACH, 0, -1):
        entering = jnp.where(s >= k, CB[k - 1, 0:1] * entering + CB[k - 1, 1:2], 0.0)
    for b in range(8):
        rows = slice(BLK * b, BLK * b + BLK)
        p_before, e_before = befores[b]
        states = S[rows] + PR[rows] * (e_before + p_before * entering)
        BR[b] = (states * GL[rows]).astype(BF16)
    BRR[t] = BR[mine]
    for k in range(1, 8):
        peer = lax.rem(t + k, 8)
        block = lax.rem(peer, 2) * 4 + lax.div(peer, 2)
        remote(BR.at[block], BRR.at[t], sem.at[10], sem.at[11], (s, peer))
    for k in range(1, 8):
        peer = lax.rem(t + k, 8)
        block = lax.rem(peer, 2) * 4 + lax.div(peer, 2)
        remote(res_ref.at[block], RB.at[t], sem.at[6], sem.at[7], (s, peer))
    gu.event(2)
    gu.event(3)
    ow_event(1)
    gu.event(4)
    ow_event(2)
    gu.event(5)

    await_bytes(GB.at[pl.ds(0, 7)], sem.at[5])
    await_bytes(BRR.at[pl.ds(0, 7)], sem.at[11])
    await_bytes(OW.at[1 - c], ow_sem.at[2])
    PG[...] = jnp.concatenate([GB[j, 1:2] for j in range(8)], axis=1)
    branch = jnp.concatenate([BRR[j] for j in range(8)], axis=1)
    square = jnp.zeros((BLK, 1), F32)
    for j in range(8):
        mixed = jnp.dot(branch, OW[j % 2, j // 2], preferred_element_type=F32).astype(BF16).astype(F32)
        square = square + jnp.sum(mixed * mixed, axis=1, keepdims=True)
        MX[:, 256 * j : 256 * j + 256] = mixed
    scale = lax.rsqrt(square * (1.0 / D) + EPS)
    gu.event(6)
    dw.start()
    dw.start_second()
    await_bytes(RB.at[pl.ds(0, 7)], sem.at[7])
    for j in range(8):
        cols = slice(256 * j, 256 * j + 256)
        mixed = MX[:, cols] * scale * GB[j, 0:1]
        ST[x, :, cols] = (RB[j].astype(F32) + mixed).astype(BF16)

    for part, step in ((0, 1), (1, 3), (1, 1), (0, 3)):
        ref = ST.at[x, pl.ds(48 * part, 48)]
        remote(ref, ref, sem.at[12], ag_ring.at[0 if step == 1 else 1, part], along_x(step))
    for part, step in ((0, 1), (1, 3)):
        came = lax.rem(x + 4 - step, 4)
        ref = ST.at[came, pl.ds(48 * part, 48)]
        await_bytes(ref, ag_ring.at[0 if step == 1 else 1, part])
        remote(ref, ref, sem.at[12], ag_ring.at[2, part], along_x(step))
    gu.event(7)
    gu.wait_pair()

    def normalize(blocks):
        for n, q in enumerate(blocks):
            for r in range(0, BLK, 16):
                stream = ST[q, r : r + 16].astype(F32)
                total = jnp.sum(stream * stream, axis=1, keepdims=True)
                NB[n, r : r + 16] = (stream * lax.rsqrt(total * (1.0 / D) + EPS) * PG[...]).astype(BF16)

    def hidden(blocks, p):
        lhs = NB[0 : len(blocks)].reshape(BLK * len(blocks), D)
        for i in range(5):
            weights = GU[p, :, :, 256 * i : 256 * i + 256].reshape(D, 256)
            both = jnp.dot(lhs, weights, preferred_element_type=F32)
            act = (jax.nn.silu(both[:, :128]) * both[:, 128:]).astype(BF16)
            for n, q in enumerate(blocks):
                H[p, q, :, 128 * i : 128 * i + 128] = act[BLK * n : BLK * n + BLK]

    def hidden_tail(blocks):
        lhs = NB[0 : len(blocks)].reshape(BLK * len(blocks), D)
        weights = jnp.concatenate([GU[p, :, :, 1280:1408].reshape(D, 128) for p in (0, 1)], axis=1)
        both = jnp.dot(lhs, weights, preferred_element_type=F32)
        for p in (0, 1):
            tail = both[:, 128 * p : 128 * p + 128]
            act = (jax.nn.silu(tail[:, :64]) * tail[:, 64:]).astype(BF16)
            for n, q in enumerate(blocks):
                H[p, q, :, 640:704] = act[BLK * n : BLK * n + BLK]

    left, right, across = lax.rem(x + 3, 4), lax.rem(x + 1, 4), lax.rem(x + 2, 4)
    normalize([x])
    hidden([x], 0)
    dw.event(1)
    hidden([x], 1)
    hidden_tail([x])
    for part, step in ((1, 1), (0, 3)):
        came = lax.rem(x + 4 - step, 4)
        await_bytes(ST.at[came, pl.ds(48 * part, 48)], ag_ring.at[0 if step == 1 else 1, part])
    dw.event(2)
    dw.event(3)
    normalize([left, right])
    hidden([left, right], 0)
    dw.event(4)
    hidden([left, right], 1)
    hidden_tail([left, right])
    for part in (0, 1):
        await_bytes(ST.at[across, pl.ds(48 * part, 48)], ag_ring.at[2, part])
    theirs = pl.ds(pl.multiple_of(512 * x + 256 * (1 - c), 256), 256)
    remote(ST.at[:, :, theirs], XR, sem.at[15], sem.at[16], partner)
    dw.event(5)
    normalize([across])
    hidden([across], 0)
    dw.event(6)
    hidden([across], 1)
    hidden_tail([across])
    dw.event(7)
    dw.wait_pair()

    def down(chip, h):
        total = None
        for p in (0, 1):
            weights = jnp.concatenate([DW[p, 4 * chip + 2 * h], DW[p, 4 * chip + 2 * h + 1]], axis=1)
            part = jnp.dot(H[p].reshape(HALF, HID), weights, preferred_element_type=F32)
            total = part if total is None else total + part
        return total

    for h, step in ((0, 1), (1, 3)):
        PB[h] = down(across, h).astype(BF16)
        remote(PB.at[h], RA.at[h], rs_send.at[h], rs_recv.at[4 + h], along_x(step))
    for n, (chip, h) in enumerate(((right, 1), (left, 0))):
        PB[2 + n] = down(chip, h).astype(BF16)
        remote(PB.at[2 + n], RC.at[n, c], rs_send.at[2 + n], rs_recv.at[2 * n + c], (s, 2 * chip + h))
    FO[0] = down(right, 0)
    FO[1] = down(left, 1)
    for n, (chip, h) in enumerate(((right, 0), (left, 1))):
        await_bytes(RA.at[n], rs_recv.at[4 + n])
        PB[4 + n] = (FO[n] + RA[n].astype(F32)).astype(BF16)
        remote(PB.at[4 + n], RC.at[n, c], rs_send.at[4 + n], rs_recv.at[2 * n + c], (s, 2 * chip + h))
    PB[6] = down(x, 1 - c).astype(BF16)
    remote(PB.at[6], PO.at[c], sem.at[8], sem.at[18], partner)
    PO[c] = down(x, c).astype(BF16)
    await_bytes(PO.at[0], sem.at[18])
    for n in (0, 1):
        for k in (0, 1):
            await_bytes(RC.at[n, k], rs_recv.at[2 * n + k])
    rows = []
    for k in (0, 1):
        total = PO[k].astype(F32) + RC[0, k].astype(F32) + RC[1, k].astype(F32)
        total = total.astype(BF16).astype(F32)
        FO[k] = total
        square = jnp.sum(total * total, axis=1, keepdims=True)
        rows.append(jnp.broadcast_to(square, (HALF, 128)).T[0:1])

    SQB[t] = jnp.concatenate(rows, axis=1)
    for k in range(1, 8):
        remote(SQB.at[t], SQB.at[t], sem.at[13], sem.at[14], (s, lax.rem(t + k, 8)))
    await_bytes(XR, sem.at[16])
    await_bytes(SQB.at[pl.ds(0, 7)], sem.at[14])
    square = SQB[0]
    for j in range(1, 8):
        square = square + SQB[j]
    scale = lax.rsqrt(square * (1.0 / D) + EPS)
    scale = jnp.broadcast_to(scale, (128, TOK)).T
    scale = jnp.concatenate([scale, scale], axis=1)
    gain = GS[2:3]
    mine_cols = pl.ds(pl.multiple_of(512 * x + 256 * c, 256), 256)
    for k, stream in ((c, ST[:, :, mine_cols]), (1 - c, XR[...])):
        stream = stream.reshape(HALF, 256).astype(F32)
        factor = jnp.where(k == 0, scale[:HALF], scale[HALF:])
        out_ref[k] = (stream + FO[k] * factor * gain).astype(BF16)

    gu.finish()
    dw.finish()
    await_bytes(HX, sem.at[0])
    await_bytes(HI, sem.at[2])
    await_bytes(GB.at[pl.ds(0, 7)], sem.at[4])
    await_bytes(RB.at[pl.ds(0, 7)], sem.at[6])
    await_bytes(CB, sem.at[17])
    await_bytes(BRR.at[pl.ds(0, 7)], sem.at[10])
    await_bytes(OW.at[c, pl.ds(0, 3)], ow_sem.at[0])
    await_bytes(OW.at[c], ow_sem.at[1])
    await_bytes(ST.at[pl.ds(0, 3)], sem.at[12])
    for n in range(6):
        await_bytes(PB.at[n], rs_send.at[n])
    await_bytes(PB.at[6], sem.at[8])
    await_bytes(SQB.at[pl.ds(0, 7)], sem.at[13])
    await_bytes(XR, sem.at[15])


def body(
    gate_branch, recur_input, doc_ids, conv_taps, gate_map, input_map, decay_level, decay_extra, out_weight,
    residual, mix_gain, pre_gain, ffn_gain, gate_weight, up_weight, down_weight,
):
    vmem = pl.BlockSpec(memory_space=pltpu.VMEM)
    dma = pltpu.SemaphoreType.DMA
    out = pl.pallas_call(
        layer_kernel,
        name="layer",
        out_shape=jax.ShapeDtypeStruct((2, HALF, 256), BF16),
        in_specs=[pl.BlockSpec(memory_space=pl.ANY)] * 16,
        out_specs=vmem,
        scratch_shapes=[
            pltpu.VMEM((TOK, CH), BF16),
            pltpu.VMEM((TOK, CH), BF16),
            pltpu.VMEM((6, 128), jnp.int32),
            pltpu.VMEM((4, CH), BF16),
            pltpu.VMEM((2, 64, 64), BF16),
            pltpu.VMEM((2, 64, 64), BF16),
            pltpu.VMEM((1, CH), F32),
            pltpu.VMEM((TOK, CH), F32),
            pltpu.VMEM((8, BLK, 256), BF16),
            pltpu.VMEM((1, 256), F32),
            pltpu.VMEM((1, 256), F32),
            pltpu.VMEM((1, 256), F32),
            pltpu.VMEM((HID, 128), BF16),
            pltpu.VMEM((HID, 128), BF16),
            pltpu.VMEM((2, 16, 128, 1408), BF16),
            pltpu.VMEM((2, 16, HID, 128), BF16),
            pltpu.VMEM((2, 4, 1024, 256), BF16),
            pltpu.VMEM((8, BLK, CH), BF16),
            pltpu.VMEM((8, BLK, CH), BF16),
            pltpu.VMEM((8, BLK, 256), BF16),
            pltpu.VMEM((8, 256), F32),
            pltpu.VMEM((8, 8, 256), F32),
            pltpu.VMEM((16, CH), BF16),
            pltpu.VMEM((6, 128), jnp.int32),
            pltpu.VMEM((TOK + 8, CH), F32),
            pltpu.VMEM((TOK + 8, CH), F32),
            pltpu.VMEM((TOK, CH), F32),
            pltpu.VMEM((TOK, CH), F32),
            pltpu.VMEM((TOK, CH), F32),
            pltpu.VMEM((TOK, CH), F32),
            pltpu.VMEM((TOK, CH), F32),
            pltpu.VMEM((8, CH), F32),
            pltpu.VMEM((REACH, 8, CH), F32),
            pltpu.VMEM((BLK, D), F32),
            pltpu.VMEM((4, BLK, D), BF16),
            pltpu.VMEM((2, BLK, D), BF16),
            pltpu.VMEM((2, 4, BLK, HID), BF16),
            pltpu.VMEM((7, HALF, 256), BF16),
            pltpu.VMEM((2, HALF, 256), BF16),
            pltpu.VMEM((2, 2, HALF, 256), BF16),
            pltpu.VMEM((2, HALF, 256), BF16),
            pltpu.VMEM((2, HALF, 256), F32),
            pltpu.VMEM((8, 1, TOK), F32),
            pltpu.VMEM((4, BLK, 256), BF16),
            pltpu.VMEM((1, D), F32),
            dma((2, 16)),
            dma((2, 16)),
            dma((3,)),
            dma((3,)),
            dma((3, 2)),
            dma((3,)),
            dma((3, 2)),
            dma((6,)),
            dma((6,)),
            dma((16,)),
            dma((19,)),
        ],
        compiler_params=pltpu.CompilerParams(
            collective_id=0, has_side_effects=True, vmem_limit_bytes=60 * 1024 * 1024
        ),
    )(
        gate_branch,
        recur_input,
        doc_ids.reshape(6, 128),
        conv_taps,
        gate_map,
        input_map,
        decay_level.reshape(1, CH),
        decay_extra,
        out_weight,
        residual.reshape(8, BLK, 256),
        mix_gain.reshape(1, 256),
        pre_gain.reshape(1, 256),
        ffn_gain.reshape(1, 256),
        gate_weight.T,
        up_weight.T,
        down_weight,
    )
    return out.reshape(TOK, 256)


def solution(mesh):
    return jax.shard_map(
        body,
        mesh=mesh,
        in_specs=(
            P("sp", "tp"),
            P("sp", "tp"),
            P("sp"),
            P(None, "tp"),
            P("tp", None, None),
            P("tp", None, None),
            P("tp"),
            P("sp", "tp"),
            P(None, "tp"),
            P("sp", "tp"),
            P("tp"),
            P("tp"),
            P("tp"),
            P("sp", "tp"),
            P("sp", "tp"),
            P("tp", "sp"),
        ),
        out_specs=P("sp", "tp"),
        check_vma=False,
    )
```

```python
import jax
import jax.numpy as jnp
from jax import lax
from jax.experimental import pallas as pl
from jax.experimental.pallas import tpu as pltpu
from jax.sharding import PartitionSpec as P

MESH = pl.DeviceIdType.MESH
F32 = jnp.float32
BF16 = jnp.bfloat16

D = 2048
EPS = 1e-06
GATE_POWER = 8.0
TOK = 768
BLK = 96
HALF = 384
CH = 128
HID = 704
REACH = 6


def neg_expm1(u):
    series = 1.0 + u * (1.0 / 9.0)
    for n in (8.0, 7.0, 6.0, 5.0, 4.0, 3.0, 2.0):
        series = 1.0 + u * (1.0 / n) * series
    return jnp.where(u > -0.5, -u * series, 1.0 - jnp.exp(u))


def softplus(v):
    tail = jnp.exp(-jnp.abs(v))
    w = tail / (2.0 + tail)
    square = w * w
    series = jnp.full_like(w, 1.0 / 15.0)
    for n in (13.0, 11.0, 9.0, 7.0, 5.0, 3.0, 1.0):
        series = 1.0 / n + square * series
    return jnp.maximum(v, 0.0) + 2.0 * w * series


class TorusGather:
    def __init__(self, buf, rows, here, ring_send, ring_recv, pair_send, pair_recv):
        self.buf, self.rows = buf, rows
        self.z, self.y, self.c, self.t = here
        self.ring_send, self.ring_recv = ring_send, ring_recv
        self.pair_send, self.pair_recv = pair_send, pair_recv

    def slot(self, dz, dy):
        return lax.rem(self.z + dz, 4) * 4 + lax.rem(self.y + dy, 4)

    def at(self, half, a, b):
        return (a, b) if half == 0 else (b, a)

    def span(self, half, part):
        quarter = self.rows // 4
        first = half * 2 * quarter
        return (first, 2 * quarter) if part is None else (first + part * quarter, quarter)

    def piece(self, half, where, part=None):
        first, count = self.span(half, part)
        return self.buf.at[self.c, self.slot(*where), pl.ds(first, count)]

    def send(self, half, where, to, part=None):
        ref = self.piece(half, where, part)
        landed = ((where[0] - to[0]) % 4, (where[1] - to[1]) % 4)
        pltpu.make_async_remote_copy(
            src_ref=ref,
            dst_ref=ref,
            send_sem=self.ring_send,
            recv_sem=self.ring_recv.at[half, landed[0] * 4 + landed[1]],
            device_id=(self.slot(*to), self.t),
            device_id_type=MESH,
        ).start()

    def wait(self, half, where):
        ref = self.piece(half, where)
        pltpu.make_async_copy(ref, ref, self.ring_recv.at[half, where[0] * 4 + where[1]]).wait()
        self.pass_over(ref)

    def pass_over(self, ref):
        pltpu.make_async_remote_copy(
            src_ref=ref,
            dst_ref=ref,
            send_sem=self.pair_send,
            recv_sem=self.pair_recv,
            device_id=(self.slot(0, 0), self.t + 1 - 2 * self.c),
            device_id_type=MESH,
        ).start()

    def start(self):
        for half in (0, 1):
            for step in (1, 3):
                self.send(half, (0, 0), self.at(half, 0, step))

    def start_second(self):
        for half in (0, 1):
            for step in (1, 3):
                self.send(half, (0, 0), self.at(half, step, 0))
        self.pass_over(self.buf.at[self.c, self.slot(0, 0)])

    def spread(self, half, b):
        for step in (1, 3):
            self.send(half, self.at(half, 0, b), self.at(half, step, 0))

    def event(self, number):
        at = self.at
        for half in (0, 1):
            if number == 1:
                self.wait(half, at(half, 0, 3))
                self.send(half, at(half, 0, 3), at(half, 0, 1), part=0)
                self.wait(half, at(half, 0, 1))
                self.send(half, at(half, 0, 1), at(half, 0, 3), part=1)
        for half in (0, 1):
            if number == 1:
                self.spread(half, 3)
                self.spread(half, 1)
            if number == 2:
                self.wait(half, at(half, 0, 2))
                self.spread(half, 2)
            if number == 3:
                self.wait(half, at(half, 3, 0))
                self.send(half, at(half, 3, 0), at(half, 1, 0))
                self.wait(half, at(half, 1, 0))
            if number == 4:
                self.wait(half, at(half, 1, 3))
                self.send(half, at(half, 1, 3), at(half, 3, 0))
                self.wait(half, at(half, 3, 3))
            if number == 5:
                self.wait(half, at(half, 3, 1))
                self.send(half, at(half, 3, 1), at(half, 1, 0))
                self.wait(half, at(half, 1, 1))
            if number == 6:
                self.wait(half, at(half, 1, 2))
                self.send(half, at(half, 1, 2), at(half, 3, 0))
                self.wait(half, at(half, 3, 2))
            if number == 7:
                self.wait(half, at(half, 2, 0))
                self.wait(half, at(half, 2, 3))
            if number == 8:
                self.wait(half, at(half, 2, 1))
                self.wait(half, at(half, 2, 2))

    def wait_pair(self):
        ref = self.buf.at[1 - self.c]
        pltpu.make_async_copy(ref, ref, self.pair_recv).wait()

    def finish(self):
        ref = self.buf.at[self.c, pl.ds(0, 15)]
        pltpu.make_async_copy(ref, ref, self.ring_send).wait()
        ref = self.buf.at[self.c]
        pltpu.make_async_copy(ref, ref, self.pair_send).wait()


def layer_kernel(
    gate_hbm, rec_hbm, ids_hbm, taps_hbm, gmap_hbm, imap_hbm, level_hbm, extra_hbm, ow_hbm, res_hbm,
    mixg_hbm, preg_hbm, ffng_hbm, gw_hbm, uw_hbm, dw_hbm,
    out_ref,
    gate_ref, rec_ref, ids_ref, taps_ref, gmap_ref, imap_ref, level_ref, extra_ref, res_ref,
    mixg_ref, preg_ref, ffng_ref, gw_ref, uw_ref,
    GU, DW, OW, BR, BRR, RB, GS, GB, HX, HI, XF, IDF, FA, DV, S, PR, GL, CS, CB, MX, ST, NB, H,
    PB, RA, RC, PO, FO, SQB, XR, PG,
    gu_ring, dw_ring, gu_sem, dw_sem, ow_ring, ow_sem, ag_ring, rs_recv, rs_send, in_sem, sem,
):
    s, t = lax.axis_index("sp"), lax.axis_index("tp")
    z, y = lax.div(s, 4), lax.rem(s, 4)
    x, c = lax.div(t, 2), lax.rem(t, 2)
    mine = c * 4 + x

    def remote(src, dst, send_sem, recv_sem, device):
        copy = pltpu.make_async_remote_copy(
            src_ref=src, dst_ref=dst, send_sem=send_sem, recv_sem=recv_sem, device_id=device, device_id_type=MESH
        )
        copy.start()

    def await_bytes(ref, semaphore):
        pltpu.make_async_copy(ref, ref, semaphore).wait()

    def along_x(step):
        return (s, lax.rem(x + step, 4) * 2 + c)

    partner = (s, t + 1 - 2 * c)
    here = (z, y, c, t)
    gu = TorusGather(GU, 128, here, gu_sem.at[0], gu_ring, gu_sem.at[1], gu_sem.at[2])
    dw = TorusGather(DW, HID, here, dw_sem.at[0], dw_ring, dw_sem.at[1], dw_sem.at[2])

    barrier = pltpu.get_barrier_semaphore()
    for k in range(1, REACH + 1):
        for peer in (lax.rem(s + k, 16), lax.rem(s + 16 - k, 16)):
            pl.semaphore_signal(barrier, inc=1, device_id=(peer, t), device_id_type=MESH)
    for k in range(1, 8):
        pl.semaphore_signal(barrier, inc=1, device_id=(s, lax.rem(t + k, 8)), device_id_type=MESH)

    own = z * 4 + y
    loads = []
    for src, dst in (
        (gw_hbm, gw_ref), (uw_hbm, uw_ref), (rec_hbm, rec_ref), (ids_hbm, ids_ref), (mixg_hbm, mixg_ref),
        (preg_hbm, preg_ref), (ffng_hbm, ffng_ref), (ow_hbm, OW.at[c, x]), (gate_hbm, gate_ref), (taps_hbm, taps_ref),
        (gmap_hbm, gmap_ref), (imap_hbm, imap_ref), (level_hbm, level_ref), (extra_hbm, extra_ref),
        (res_hbm, res_ref), (dw_hbm, DW.at[c, own]),
    ):
        loads.append(pltpu.make_async_copy(src, dst, in_sem.at[len(loads)]))
        loads[-1].start()

    loads[0].wait()
    loads[1].wait()
    for i in range(5):
        for n, ref in enumerate((gw_ref, uw_ref)):
            block = ref[128 * i : 128 * i + 128].astype(F32).T.astype(BF16)
            GU[c, own, :, 256 * i + 128 * n : 256 * i + 128 * n + 128] = block
    block = jnp.concatenate([gw_ref[640:704].astype(F32), uw_ref[640:704].astype(F32)], axis=0)
    GU[c, own, :, 1280:1408] = block.T.astype(BF16)
    for load in loads[2:8]:
        load.wait()
    GS[...] = jnp.zeros_like(GS)
    GS[0:1] = mixg_ref[...]
    GS[1:2] = preg_ref[...]
    GS[2:3] = ffng_ref[...]
    GB[t] = GS[...]
    IDF[8:] = jnp.concatenate(
        [jnp.broadcast_to(ids_ref[r : r + 1, :].astype(F32), (128, 128)).T for r in range(6)], axis=0
    )
    XF[8:] = rec_ref[...].astype(F32)

    pl.semaphore_wait(barrier, 2 * REACH + 7)

    after = (lax.rem(s + 1, 16), t)
    remote(rec_ref.at[pl.ds(TOK - 16, 16)], HX, sem.at[0], sem.at[1], after)
    remote(ids_ref, HI, sem.at[2], sem.at[3], after)
    gu.start()
    for part, step in ((0, 1), (1, 3), (1, 1), (0, 3)):
        ref = OW.at[c, x, pl.ds(512 * part, 512)]
        remote(ref, ref, ow_sem.at[0], ow_ring.at[0 if step == 1 else 1, part], along_x(step))
    remote(OW.at[c, x], OW.at[c, x], ow_sem.at[1], ow_sem.at[2], partner)
    for k in range(1, 8):
        peer = lax.rem(t + k, 8)
        remote(GS, GB.at[t], sem.at[4], sem.at[5], (s, peer))
    for load in loads[8:]:
        load.wait()
    RB[t] = res_ref[mine]

    for r in range(6):
        rows = slice(128 * r, 128 * r + 128)
        GL[rows] = jax.nn.gelu(gate_ref[rows].astype(F32), approximate=True)
    pair = [
        jnp.concatenate(
            [
                jnp.concatenate([m[0].astype(F32), jnp.zeros((64, 64), F32)], axis=1),
                jnp.concatenate([jnp.zeros((64, 64), F32), m[1].astype(F32)], axis=1),
            ],
            axis=0,
        )
        for m in (gmap_ref, imap_ref)
    ]
    maps = jnp.concatenate(pair, axis=1).astype(BF16)
    rate = -GATE_POWER * softplus(-level_ref[...])
    taps = taps_ref[...].astype(F32)

    await_bytes(HX, sem.at[1])
    await_bytes(HI, sem.at[3])
    XF[0:8] = HX[...].astype(F32)[8:16]
    rim_ids = jnp.broadcast_to(HI[5:6, :].astype(F32), (128, 128)).T[120:128]
    IDF[0:8] = jnp.where(s > 0, rim_ids, -1.0)

    for r in range(6):
        at = 8 + 128 * r
        ids = IDF[at : at + 128]
        conv = XF[at : at + 128] * taps[0:1]
        for k in (1, 2, 3):
            same = IDF[at - k : at - k + 128] == ids
            conv = conv + jnp.where(same, XF[at - k : at - k + 128], 0.0) * taps[k : k + 1]
        conv = conv.astype(BF16)
        gates = jax.nn.sigmoid(jnp.dot(conv, maps, preferred_element_type=F32))
        rows = slice(128 * r, 128 * r + 128)
        log_decay = rate * gates[:, :CH] + extra_ref[rows]
        FA[rows] = jnp.where(IDF[at - 1 : at + 127] == ids, jnp.exp(log_decay), 0.0)
        DV[rows] = jnp.sqrt(neg_expm1(2.0 * log_decay)) * gates[:, CH:] * conv.astype(F32)

    state = jnp.zeros((8, CH), F32)
    prod = jnp.ones((8, CH), F32)
    for i in range(BLK):
        at = pl.ds(i, 8, stride=BLK)
        f = FA[at, :]
        state = f * state + DV[at, :]
        prod = f * prod
        S[at, :] = state
        PR[at, :] = prod
    befores = []
    p_all, e_all = jnp.ones((1, CH), F32), jnp.zeros((1, CH), F32)
    for b in range(8):
        befores.append((p_all, e_all))
        e_all = prod[b : b + 1] * e_all + state[b : b + 1]
        p_all = prod[b : b + 1] * p_all
    CS[...] = jnp.concatenate([p_all, e_all, jnp.zeros((6, CH), F32)], axis=0)
    for k in range(1, REACH + 1):
        remote(CS, CB.at[k - 1], sem.at[17], sem.at[9], (lax.rem(s + k, 16), t))
    gu.start_second()
    gu.event(1)

    def ow_event(number):
        if number == 0:
            for part, step in ((0, 1), (1, 3)):
                came = lax.rem(x + 4 - step, 4)
                ref = OW.at[c, came, pl.ds(512 * part, 512)]
                await_bytes(ref, ow_ring.at[0 if step == 1 else 1, part])
                remote(ref, ref, ow_sem.at[0], ow_ring.at[2, part], along_x(step))
                remote(ref, ref, ow_sem.at[1], ow_sem.at[2], partner)
        if number == 1:
            for part, step in ((1, 1), (0, 3)):
                came = lax.rem(x + 4 - step, 4)
                ref = OW.at[c, came, pl.ds(512 * part, 512)]
                await_bytes(ref, ow_ring.at[0 if step == 1 else 1, part])
                remote(ref, ref, ow_sem.at[1], ow_sem.at[2], partner)
        if number == 2:
            came = lax.rem(x + 2, 4)
            for part in (0, 1):
                ref = OW.at[c, came, pl.ds(512 * part, 512)]
                await_bytes(ref, ow_ring.at[2, part])
                remote(ref, ref, ow_sem.at[1], ow_sem.at[2], partner)

    ow_event(0)

    await_bytes(CB, sem.at[9])
    entering = jnp.zeros((1, CH), F32)
    for k in range(REACH, 0, -1):
        entering = jnp.where(s >= k, CB[k - 1, 0:1] * entering + CB[k - 1, 1:2], 0.0)
    for b in range(8):
        rows = slice(BLK * b, BLK * b + BLK)
        p_before, e_before = befores[b]
        states = S[rows] + PR[rows] * (e_before + p_before * entering)
        BR[b] = (states * GL[rows]).astype(BF16)
    BRR[t] = BR[mine]
    for k in range(1, 8):
        peer = lax.rem(t + k, 8)
        block = lax.rem(peer, 2) * 4 + lax.div(peer, 2)
        remote(BR.at[block], BRR.at[t], sem.at[10], sem.at[11], (s, peer))
    for k in range(1, 8):
        peer = lax.rem(t + k, 8)
        block = lax.rem(peer, 2) * 4 + lax.div(peer, 2)
        remote(res_ref.at[block], RB.at[t], sem.at[6], sem.at[7], (s, peer))
    gu.event(2)
    gu.event(3)
    ow_event(1)
    gu.event(4)
    ow_event(2)
    gu.event(5)

    await_bytes(GB.at[pl.ds(0, 7)], sem.at[5])
    await_bytes(BRR.at[pl.ds(0, 7)], sem.at[11])
    await_bytes(OW.at[1 - c], ow_sem.at[2])
    PG[...] = jnp.concatenate([GB[j, 1:2] for j in range(8)], axis=1)
    branch = jnp.concatenate([BRR[j] for j in range(8)], axis=1)
    square = jnp.zeros((BLK, 1), F32)
    for j in range(8):
        mixed = jnp.dot(branch, OW[j % 2, j // 2], preferred_element_type=F32).astype(BF16).astype(F32)
        square = square + jnp.sum(mixed * mixed, axis=1, keepdims=True)
        MX[:, 256 * j : 256 * j + 256] = mixed
    scale = lax.rsqrt(square * (1.0 / D) + EPS)
    gu.event(6)
    dw.start()
    dw.start_second()
    await_bytes(RB.at[pl.ds(0, 7)], sem.at[7])
    for j in range(8):
        cols = slice(256 * j, 256 * j + 256)
        mixed = MX[:, cols] * scale * GB[j, 0:1]
        ST[x, :, cols] = (RB[j].astype(F32) + mixed).astype(BF16)

    for part, step in ((0, 1), (1, 3), (1, 1), (0, 3)):
        ref = ST.at[x, pl.ds(48 * part, 48)]
        remote(ref, ref, sem.at[12], ag_ring.at[0 if step == 1 else 1, part], along_x(step))
    gu.event(7)
    for part, step in ((0, 1), (1, 3)):
        came = lax.rem(x + 4 - step, 4)
        ref = ST.at[came, pl.ds(48 * part, 48)]
        await_bytes(ref, ag_ring.at[0 if step == 1 else 1, part])
        remote(ref, ref, sem.at[12], ag_ring.at[2, part], along_x(step))
    gu.event(8)

    def normalize(blocks):
        for n, q in enumerate(blocks):
            for r in range(0, BLK, 16):
                stream = ST[q, r : r + 16].astype(F32)
                total = jnp.sum(stream * stream, axis=1, keepdims=True)
                NB[n, r : r + 16] = (stream * lax.rsqrt(total * (1.0 / D) + EPS) * PG[...]).astype(BF16)

    def hidden(blocks, p):
        lhs = NB[0 : len(blocks)].reshape(BLK * len(blocks), D)
        for i in range(5):
            weights = GU[p, :, :, 256 * i : 256 * i + 256].reshape(D, 256)
            both = jnp.dot(lhs, weights, preferred_element_type=F32)
            act = (jax.nn.silu(both[:, :128]) * both[:, 128:]).astype(BF16)
            for n, q in enumerate(blocks):
                H[p, q, :, 128 * i : 128 * i + 128] = act[BLK * n : BLK * n + BLK]

    def hidden_tail(blocks):
        lhs = NB[0 : len(blocks)].reshape(BLK * len(blocks), D)
        weights = jnp.concatenate([GU[p, :, :, 1280:1408].reshape(D, 128) for p in (0, 1)], axis=1)
        both = jnp.dot(lhs, weights, preferred_element_type=F32)
        for p in (0, 1):
            tail = both[:, 128 * p : 128 * p + 128]
            act = (jax.nn.silu(tail[:, :64]) * tail[:, 64:]).astype(BF16)
            for n, q in enumerate(blocks):
                H[p, q, :, 640:704] = act[BLK * n : BLK * n + BLK]

    left, right, across = lax.rem(x + 3, 4), lax.rem(x + 1, 4), lax.rem(x + 2, 4)
    normalize([x])
    dw.event(1)
    gu.wait_pair()
    hidden([x], 0)
    dw.event(2)
    dw.event(3)
    hidden([x], 1)
    hidden_tail([x])
    for part, step in ((1, 1), (0, 3)):
        came = lax.rem(x + 4 - step, 4)
        await_bytes(ST.at[came, pl.ds(48 * part, 48)], ag_ring.at[0 if step == 1 else 1, part])
    dw.event(4)
    normalize([left, right])
    hidden([left, right], 0)
    dw.event(5)
    hidden([left, right], 1)
    hidden_tail([left, right])
    for part in (0, 1):
        await_bytes(ST.at[across, pl.ds(48 * part, 48)], ag_ring.at[2, part])
    theirs = pl.ds(pl.multiple_of(512 * x + 256 * (1 - c), 256), 256)
    remote(ST.at[:, :, theirs], XR, sem.at[15], sem.at[16], partner)
    dw.event(6)
    normalize([across])
    hidden([across], 0)
    dw.event(7)
    hidden([across], 1)
    hidden_tail([across])
    dw.event(8)
    dw.wait_pair()

    def down(chip, h):
        total = None
        for p in (0, 1):
            weights = jnp.concatenate([DW[p, 4 * chip + 2 * h], DW[p, 4 * chip + 2 * h + 1]], axis=1)
            part = jnp.dot(H[p].reshape(HALF, HID), weights, preferred_element_type=F32)
            total = part if total is None else total + part
        return total

    for h, step in ((0, 1), (1, 3)):
        PB[h] = down(across, h).astype(BF16)
        remote(PB.at[h], RA.at[h], rs_send.at[h], rs_recv.at[4 + h], along_x(step))
    for n, (chip, h) in enumerate(((right, 1), (left, 0))):
        PB[2 + n] = down(chip, h).astype(BF16)
        remote(PB.at[2 + n], RC.at[n, c], rs_send.at[2 + n], rs_recv.at[2 * n + c], (s, 2 * chip + h))
    FO[0] = down(right, 0)
    FO[1] = down(left, 1)
    for n, (chip, h) in enumerate(((right, 0), (left, 1))):
        await_bytes(RA.at[n], rs_recv.at[4 + n])
        PB[4 + n] = (FO[n] + RA[n].astype(F32)).astype(BF16)
        remote(PB.at[4 + n], RC.at[n, c], rs_send.at[4 + n], rs_recv.at[2 * n + c], (s, 2 * chip + h))
    PB[6] = down(x, 1 - c).astype(BF16)
    remote(PB.at[6], PO.at[c], sem.at[8], sem.at[18], partner)
    PO[c] = down(x, c).astype(BF16)
    await_bytes(PO.at[0], sem.at[18])
    for n in (0, 1):
        for k in (0, 1):
            await_bytes(RC.at[n, k], rs_recv.at[2 * n + k])
    rows = []
    for k in (0, 1):
        total = PO[k].astype(F32) + RC[0, k].astype(F32) + RC[1, k].astype(F32)
        total = total.astype(BF16).astype(F32)
        FO[k] = total
        square = jnp.sum(total * total, axis=1, keepdims=True)
        rows.append(jnp.broadcast_to(square, (HALF, 128)).T[0:1])

    SQB[t] = jnp.concatenate(rows, axis=1)
    for k in range(1, 8):
        remote(SQB.at[t], SQB.at[t], sem.at[13], sem.at[14], (s, lax.rem(t + k, 8)))
    await_bytes(XR, sem.at[16])
    await_bytes(SQB.at[pl.ds(0, 7)], sem.at[14])
    square = SQB[0]
    for j in range(1, 8):
        square = square + SQB[j]
    scale = lax.rsqrt(square * (1.0 / D) + EPS)
    scale = jnp.broadcast_to(scale, (128, TOK)).T
    scale = jnp.concatenate([scale, scale], axis=1)
    gain = GS[2:3]
    mine_cols = pl.ds(pl.multiple_of(512 * x + 256 * c, 256), 256)
    for k, stream in ((c, ST[:, :, mine_cols]), (1 - c, XR[...])):
        stream = stream.reshape(HALF, 256).astype(F32)
        factor = jnp.where(k == 0, scale[:HALF], scale[HALF:])
        out_ref[k] = (stream + FO[k] * factor * gain).astype(BF16)

    gu.finish()
    dw.finish()
    await_bytes(HX, sem.at[0])
    await_bytes(HI, sem.at[2])
    await_bytes(GB.at[pl.ds(0, 7)], sem.at[4])
    await_bytes(RB.at[pl.ds(0, 7)], sem.at[6])
    await_bytes(CB, sem.at[17])
    await_bytes(BRR.at[pl.ds(0, 7)], sem.at[10])
    await_bytes(OW.at[c, pl.ds(0, 3)], ow_sem.at[0])
    await_bytes(OW.at[c], ow_sem.at[1])
    await_bytes(ST.at[pl.ds(0, 3)], sem.at[12])
    for n in range(6):
        await_bytes(PB.at[n], rs_send.at[n])
    await_bytes(PB.at[6], sem.at[8])
    await_bytes(SQB.at[pl.ds(0, 7)], sem.at[13])
    await_bytes(XR, sem.at[15])


def body(
    gate_branch, recur_input, doc_ids, conv_taps, gate_map, input_map, decay_level, decay_extra, out_weight,
    residual, mix_gain, pre_gain, ffn_gain, gate_weight, up_weight, down_weight,
):
    vmem = pl.BlockSpec(memory_space=pltpu.VMEM)
    dma = pltpu.SemaphoreType.DMA
    out = pl.pallas_call(
        layer_kernel,
        name="layer",
        out_shape=jax.ShapeDtypeStruct((2, HALF, 256), BF16),
        in_specs=[pl.BlockSpec(memory_space=pl.ANY)] * 16,
        out_specs=vmem,
        scratch_shapes=[
            pltpu.VMEM((TOK, CH), BF16),
            pltpu.VMEM((TOK, CH), BF16),
            pltpu.VMEM((6, 128), jnp.int32),
            pltpu.VMEM((4, CH), BF16),
            pltpu.VMEM((2, 64, 64), BF16),
            pltpu.VMEM((2, 64, 64), BF16),
            pltpu.VMEM((1, CH), F32),
            pltpu.VMEM((TOK, CH), F32),
            pltpu.VMEM((8, BLK, 256), BF16),
            pltpu.VMEM((1, 256), F32),
            pltpu.VMEM((1, 256), F32),
            pltpu.VMEM((1, 256), F32),
            pltpu.VMEM((HID, 128), BF16),
            pltpu.VMEM((HID, 128), BF16),
            pltpu.VMEM((2, 16, 128, 1408), BF16),
            pltpu.VMEM((2, 16, HID, 128), BF16),
            pltpu.VMEM((2, 4, 1024, 256), BF16),
            pltpu.VMEM((8, BLK, CH), BF16),
            pltpu.VMEM((8, BLK, CH), BF16),
            pltpu.VMEM((8, BLK, 256), BF16),
            pltpu.VMEM((8, 256), F32),
            pltpu.VMEM((8, 8, 256), F32),
            pltpu.VMEM((16, CH), BF16),
            pltpu.VMEM((6, 128), jnp.int32),
            pltpu.VMEM((TOK + 8, CH), F32),
            pltpu.VMEM((TOK + 8, CH), F32),
            pltpu.VMEM((TOK, CH), F32),
            pltpu.VMEM((TOK, CH), F32),
            pltpu.VMEM((TOK, CH), F32),
            pltpu.VMEM((TOK, CH), F32),
            pltpu.VMEM((TOK, CH), F32),
            pltpu.VMEM((8, CH), F32),
            pltpu.VMEM((REACH, 8, CH), F32),
            pltpu.VMEM((BLK, D), F32),
            pltpu.VMEM((4, BLK, D), BF16),
            pltpu.VMEM((2, BLK, D), BF16),
            pltpu.VMEM((2, 4, BLK, HID), BF16),
            pltpu.VMEM((7, HALF, 256), BF16),
            pltpu.VMEM((2, HALF, 256), BF16),
            pltpu.VMEM((2, 2, HALF, 256), BF16),
            pltpu.VMEM((2, HALF, 256), BF16),
            pltpu.VMEM((2, HALF, 256), F32),
            pltpu.VMEM((8, 1, TOK), F32),
            pltpu.VMEM((4, BLK, 256), BF16),
            pltpu.VMEM((1, D), F32),
            dma((2, 16)),
            dma((2, 16)),
            dma((3,)),
            dma((3,)),
            dma((3, 2)),
            dma((3,)),
            dma((3, 2)),
            dma((6,)),
            dma((6,)),
            dma((16,)),
            dma((19,)),
        ],
        compiler_params=pltpu.CompilerParams(
            collective_id=0, has_side_effects=True, vmem_limit_bytes=60 * 1024 * 1024
        ),
    )(
        gate_branch,
        recur_input,
        doc_ids.reshape(6, 128),
        conv_taps,
        gate_map,
        input_map,
        decay_level.reshape(1, CH),
        decay_extra,
        out_weight,
        residual.reshape(8, BLK, 256),
        mix_gain.reshape(1, 256),
        pre_gain.reshape(1, 256),
        ffn_gain.reshape(1, 256),
        gate_weight.T,
        up_weight.T,
        down_weight,
    )
    return out.reshape(TOK, 256)


def solution(mesh):
    return jax.shard_map(
        body,
        mesh=mesh,
        in_specs=(
            P("sp", "tp"),
            P("sp", "tp"),
            P("sp"),
            P(None, "tp"),
            P("tp", None, None),
            P("tp", None, None),
            P("tp"),
            P("sp", "tp"),
            P(None, "tp"),
            P("sp", "tp"),
            P("tp"),
            P("tp"),
            P("tp"),
            P("sp", "tp"),
            P("sp", "tp"),
            P("tp", "sp"),
        ),
        out_specs=P("sp", "tp"),
        check_vma=False,
    )
```

```python
import jax
import jax.numpy as jnp
from jax import lax
from jax.experimental import pallas as pl
from jax.experimental.pallas import tpu as pltpu
from jax.sharding import PartitionSpec as P

MESH = pl.DeviceIdType.MESH
F32 = jnp.float32
BF16 = jnp.bfloat16

D = 2048
EPS = 1e-06
GATE_POWER = 8.0
TOK = 768
BLK = 96
HALF = 384
CH = 128
HID = 704
REACH = 6


def neg_expm1(u):
    series = 1.0 + u * (1.0 / 9.0)
    for n in (8.0, 7.0, 6.0, 5.0, 4.0, 3.0, 2.0):
        series = 1.0 + u * (1.0 / n) * series
    return jnp.where(u > -0.5, -u * series, 1.0 - jnp.exp(u))


def softplus(v):
    tail = jnp.exp(-jnp.abs(v))
    w = tail / (2.0 + tail)
    square = w * w
    series = jnp.full_like(w, 1.0 / 15.0)
    for n in (13.0, 11.0, 9.0, 7.0, 5.0, 3.0, 1.0):
        series = 1.0 / n + square * series
    return jnp.maximum(v, 0.0) + 2.0 * w * series


class TorusGather:
    def __init__(self, buf, rows, here, ring_send, ring_recv, pair_send, pair_recv):
        self.buf, self.rows = buf, rows
        self.z, self.y, self.c, self.t = here
        self.ring_send, self.ring_recv = ring_send, ring_recv
        self.pair_send, self.pair_recv = pair_send, pair_recv

    def slot(self, dz, dy):
        return lax.rem(self.z + dz, 4) * 4 + lax.rem(self.y + dy, 4)

    def at(self, half, a, b):
        return (a, b) if half == 0 else (b, a)

    def span(self, half, part):
        quarter = self.rows // 4
        first = half * 2 * quarter
        return (first, 2 * quarter) if part is None else (first + part * quarter, quarter)

    def piece(self, half, where, part=None):
        first, count = self.span(half, part)
        return self.buf.at[self.c, self.slot(*where), pl.ds(first, count)]

    def send(self, half, where, to, part=None):
        ref = self.piece(half, where, part)
        landed = ((where[0] - to[0]) % 4, (where[1] - to[1]) % 4)
        pltpu.make_async_remote_copy(
            src_ref=ref,
            dst_ref=ref,
            send_sem=self.ring_send,
            recv_sem=self.ring_recv.at[half, landed[0] * 4 + landed[1]],
            device_id=(self.slot(*to), self.t),
            device_id_type=MESH,
        ).start()

    def wait(self, half, where):
        ref = self.piece(half, where)
        pltpu.make_async_copy(ref, ref, self.ring_recv.at[half, where[0] * 4 + where[1]]).wait()
        self.pass_over(ref, where)

    def pass_over(self, ref, where):
        pltpu.make_async_remote_copy(
            src_ref=ref,
            dst_ref=ref,
            send_sem=self.pair_send,
            recv_sem=self.pair_recv.at[1 if where[1] == 2 else 0],
            device_id=(self.slot(0, 0), self.t + 1 - 2 * self.c),
            device_id_type=MESH,
        ).start()

    def start(self):
        for half in (0, 1):
            for step in (1, 3):
                self.send(half, (0, 0), self.at(half, 0, step))

    def start_second(self):
        for half in (0, 1):
            for step in (1, 3):
                self.send(half, (0, 0), self.at(half, step, 0))
        self.pass_over(self.buf.at[self.c, self.slot(0, 0)], (0, 0))

    def spread(self, half, b, steps=(1, 3)):
        for step in steps:
            self.send(half, self.at(half, 0, b), self.at(half, step, 0))

    def relay(self, half, a, b):
        self.wait(half, self.at(half, a, b))
        self.send(half, self.at(half, a, b), self.at(half, 4 - a, 0))

    def event(self, number):
        at, wait = self.at, self.wait
        for half in (0, 1):
            if number == 1:
                wait(half, at(half, 0, 3))
                self.send(half, at(half, 0, 3), at(half, 0, 1), part=0)
                wait(half, at(half, 0, 1))
                self.send(half, at(half, 0, 1), at(half, 0, 3), part=1)
        for half in (0, 1):
            if number == 1:
                self.spread(half, 3)
                self.spread(half, 1)
            if number == 2:
                if half == 0:
                    self.relay(half, 3, 0)
                    wait(half, at(half, 0, 2))
                    self.spread(half, 2, (3,))
                else:
                    wait(half, at(half, 0, 2))
                    self.spread(half, 2)
                    self.relay(half, 3, 0)
                wait(half, at(half, 1, 0))
            if number == 3:
                self.relay(half, 1, 3)
                wait(half, at(half, 3, 3))
            if number == 4:
                self.relay(half, 3, 1)
                if half == 0:
                    self.spread(half, 2, (1,))
                wait(half, at(half, 1, 1))
        if number == 5:
            for half in (0, 1):
                self.relay(half, 1, 2)
            wait(1, at(1, 3, 2))
        if number == 6:
            wait(0, at(0, 2, 0))
            wait(0, at(0, 2, 3))
            wait(0, at(0, 2, 1))
        if number == 7:
            wait(1, at(1, 2, 0))
            wait(1, at(1, 2, 3))
            wait(0, at(0, 3, 2))
            wait(0, at(0, 2, 2))
            wait(1, at(1, 2, 1))
            wait(1, at(1, 2, 2))

    def wait_pair(self, late):
        ref = self.buf.at[1 - self.c, pl.ds(0, 4 if late else 12)]
        pltpu.make_async_copy(ref, ref, self.pair_recv.at[late]).wait()

    def finish(self):
        ref = self.buf.at[self.c, pl.ds(0, 15)]
        pltpu.make_async_copy(ref, ref, self.ring_send).wait()
        ref = self.buf.at[self.c]
        pltpu.make_async_copy(ref, ref, self.pair_send).wait()


def layer_kernel(
    gate_hbm, rec_hbm, ids_hbm, taps_hbm, gmap_hbm, imap_hbm, level_hbm, extra_hbm, ow_hbm, res_hbm,
    mixg_hbm, preg_hbm, ffng_hbm, gw_hbm, uw_hbm, dw_hbm,
    out_ref,
    gate_ref, rec_ref, ids_ref, taps_ref, gmap_ref, imap_ref, level_ref, extra_ref, res_ref,
    mixg_ref, preg_ref, ffng_ref, gw_ref, uw_ref,
    GU, DW, OW, BR, BRR, RB, GS, GB, HX, HI, XF, IDF, FA, DV, S, PR, GL, CS, CB, MX, ST, NB, H,
    PB, RA, RC, PO, FO, FF, SQB, XR, PG,
    gu_ring, dw_ring, gu_sem, dw_sem, gu_pair, dw_pair, ow_ring, ow_sem, ag_ring, ra_recv, rc_recv, rs_send, in_sem, sem,
):
    s, t = lax.axis_index("sp"), lax.axis_index("tp")
    z, y = lax.div(s, 4), lax.rem(s, 4)
    x, c = lax.div(t, 2), lax.rem(t, 2)
    mine = c * 4 + x

    def remote(src, dst, send_sem, recv_sem, device):
        copy = pltpu.make_async_remote_copy(
            src_ref=src, dst_ref=dst, send_sem=send_sem, recv_sem=recv_sem, device_id=device, device_id_type=MESH
        )
        copy.start()

    def await_bytes(ref, semaphore):
        pltpu.make_async_copy(ref, ref, semaphore).wait()

    def along_x(step):
        return (s, lax.rem(x + step, 4) * 2 + c)

    partner = (s, t + 1 - 2 * c)
    here = (z, y, c, t)
    gu = TorusGather(GU, 128, here, gu_sem.at[0], gu_ring, gu_sem.at[1], gu_pair)
    dw = TorusGather(DW, HID, here, dw_sem.at[0], dw_ring, dw_sem.at[1], dw_pair)

    barrier = pltpu.get_barrier_semaphore()
    for k in range(1, REACH + 1):
        for peer in (lax.rem(s + k, 16), lax.rem(s + 16 - k, 16)):
            pl.semaphore_signal(barrier, inc=1, device_id=(peer, t), device_id_type=MESH)
    for k in range(1, 8):
        pl.semaphore_signal(barrier, inc=1, device_id=(s, lax.rem(t + k, 8)), device_id_type=MESH)

    own = z * 4 + y
    loads = []
    for src, dst in (
        (gw_hbm, gw_ref), (uw_hbm, uw_ref), (rec_hbm, rec_ref), (ids_hbm, ids_ref), (mixg_hbm, mixg_ref),
        (preg_hbm, preg_ref), (ffng_hbm, ffng_ref), (ow_hbm, OW.at[c, x]), (gate_hbm, gate_ref), (taps_hbm, taps_ref),
        (gmap_hbm, gmap_ref), (imap_hbm, imap_ref), (level_hbm, level_ref), (extra_hbm, extra_ref),
        (res_hbm, res_ref), (dw_hbm, DW.at[c, own]),
    ):
        loads.append(pltpu.make_async_copy(src, dst, in_sem.at[len(loads)]))
        loads[-1].start()

    loads[0].wait()
    loads[1].wait()
    for i in range(5):
        for n, ref in enumerate((gw_ref, uw_ref)):
            block = ref[128 * i : 128 * i + 128].astype(F32).T.astype(BF16)
            GU[c, own, :, 256 * i + 128 * n : 256 * i + 128 * n + 128] = block
    block = jnp.concatenate([gw_ref[640:704].astype(F32), uw_ref[640:704].astype(F32)], axis=0)
    GU[c, own, :, 1280:1408] = block.T.astype(BF16)
    for load in loads[2:8]:
        load.wait()
    GS[...] = jnp.zeros_like(GS)
    GS[0:1] = mixg_ref[...]
    GS[1:2] = preg_ref[...]
    GS[2:3] = ffng_ref[...]
    GB[t] = GS[...]
    IDF[8:] = jnp.concatenate(
        [jnp.broadcast_to(ids_ref[r : r + 1, :].astype(F32), (128, 128)).T for r in range(6)], axis=0
    )
    XF[8:] = rec_ref[...].astype(F32)

    pl.semaphore_wait(barrier, 2 * REACH + 7)

    after = (lax.rem(s + 1, 16), t)
    remote(rec_ref.at[pl.ds(TOK - 16, 16)], HX, sem.at[0], sem.at[1], after)
    remote(ids_ref, HI, sem.at[2], sem.at[3], after)
    gu.start()
    for part, step in ((0, 1), (1, 3), (1, 1), (0, 3)):
        ref = OW.at[c, x, pl.ds(512 * part, 512)]
        remote(ref, ref, ow_sem.at[0], ow_ring.at[0 if step == 1 else 1, part], along_x(step))
    remote(OW.at[c, x], OW.at[c, x], ow_sem.at[1], ow_sem.at[2], partner)
    for k in range(1, 8):
        peer = lax.rem(t + k, 8)
        remote(GS, GB.at[t], sem.at[4], sem.at[5], (s, peer))
    for load in loads[8:]:
        load.wait()
    RB[t] = res_ref[mine]

    for r in range(6):
        rows = slice(128 * r, 128 * r + 128)
        GL[rows] = jax.nn.gelu(gate_ref[rows].astype(F32), approximate=True)
    pair = [
        jnp.concatenate(
            [
                jnp.concatenate([m[0].astype(F32), jnp.zeros((64, 64), F32)], axis=1),
                jnp.concatenate([jnp.zeros((64, 64), F32), m[1].astype(F32)], axis=1),
            ],
            axis=0,
        )
        for m in (gmap_ref, imap_ref)
    ]
    maps = jnp.concatenate(pair, axis=1).astype(BF16)
    rate = -GATE_POWER * softplus(-level_ref[...])
    taps = taps_ref[...].astype(F32)

    await_bytes(HX, sem.at[1])
    await_bytes(HI, sem.at[3])
    XF[0:8] = HX[...].astype(F32)[8:16]
    rim_ids = jnp.broadcast_to(HI[5:6, :].astype(F32), (128, 128)).T[120:128]
    IDF[0:8] = jnp.where(s > 0, rim_ids, -1.0)

    for r in range(6):
        at = 8 + 128 * r
        ids = IDF[at : at + 128]
        conv = XF[at : at + 128] * taps[0:1]
        for k in (1, 2, 3):
            same = IDF[at - k : at - k + 128] == ids
            conv = conv + jnp.where(same, XF[at - k : at - k + 128], 0.0) * taps[k : k + 1]
        conv = conv.astype(BF16)
        gates = jax.nn.sigmoid(jnp.dot(conv, maps, preferred_element_type=F32))
        rows = slice(128 * r, 128 * r + 128)
        log_decay = rate * gates[:, :CH] + extra_ref[rows]
        FA[rows] = jnp.where(IDF[at - 1 : at + 127] == ids, jnp.exp(log_decay), 0.0)
        DV[rows] = jnp.sqrt(neg_expm1(2.0 * log_decay)) * gates[:, CH:] * conv.astype(F32)

    state = jnp.zeros((8, CH), F32)
    prod = jnp.ones((8, CH), F32)
    for i in range(BLK):
        at = pl.ds(i, 8, stride=BLK)
        f = FA[at, :]
        state = f * state + DV[at, :]
        prod = f * prod
        S[at, :] = state
        PR[at, :] = prod
    befores = []
    p_all, e_all = jnp.ones((1, CH), F32), jnp.zeros((1, CH), F32)
    for b in range(8):
        befores.append((p_all, e_all))
        e_all = prod[b : b + 1] * e_all + state[b : b + 1]
        p_all = prod[b : b + 1] * p_all
    CS[...] = jnp.concatenate([p_all, e_all, jnp.zeros((6, CH), F32)], axis=0)
    for k in range(1, REACH + 1):
        remote(CS, CB.at[k - 1], sem.at[17], sem.at[9], (lax.rem(s + k, 16), t))
    gu.start_second()
    gu.event(1)

    def ow_event(number):
        if number == 0:
            for part, step in ((0, 1), (1, 3)):
                came = lax.rem(x + 4 - step, 4)
                ref = OW.at[c, came, pl.ds(512 * part, 512)]
                await_bytes(ref, ow_ring.at[0 if step == 1 else 1, part])
                remote(ref, ref, ow_sem.at[0], ow_ring.at[2, part], along_x(step))
                remote(ref, ref, ow_sem.at[1], ow_sem.at[2], partner)
        if number == 1:
            for part, step in ((1, 1), (0, 3)):
                came = lax.rem(x + 4 - step, 4)
                ref = OW.at[c, came, pl.ds(512 * part, 512)]
                await_bytes(ref, ow_ring.at[0 if step == 1 else 1, part])
                remote(ref, ref, ow_sem.at[1], ow_sem.at[2], partner)
        if number == 2:
            came = lax.rem(x + 2, 4)
            for part in (0, 1):
                ref = OW.at[c, came, pl.ds(512 * part, 512)]
                await_bytes(ref, ow_ring.at[2, part])
                remote(ref, ref, ow_sem.at[1], ow_sem.at[2], partner)

    ow_event(0)

    await_bytes(CB, sem.at[9])
    entering = jnp.zeros((1, CH), F32)
    for k in range(REACH, 0, -1):
        entering = jnp.where(s >= k, CB[k - 1, 0:1] * entering + CB[k - 1, 1:2], 0.0)
    for b in range(8):
        rows = slice(BLK * b, BLK * b + BLK)
        p_before, e_before = befores[b]
        states = S[rows] + PR[rows] * (e_before + p_before * entering)
        BR[b] = (states * GL[rows]).astype(BF16)
    BRR[t] = BR[mine]
    for k in range(1, 8):
        peer = lax.rem(t + k, 8)
        block = lax.rem(peer, 2) * 4 + lax.div(peer, 2)
        remote(BR.at[block], BRR.at[t], sem.at[10], sem.at[11], (s, peer))
    for k in range(1, 8):
        peer = lax.rem(t + k, 8)
        block = lax.rem(peer, 2) * 4 + lax.div(peer, 2)
        remote(res_ref.at[block], RB.at[t], sem.at[6], sem.at[7], (s, peer))
    gu.event(2)
    ow_event(1)
    gu.event(3)
    ow_event(2)
    gu.event(4)

    await_bytes(GB.at[pl.ds(0, 7)], sem.at[5])
    await_bytes(BRR.at[pl.ds(0, 7)], sem.at[11])
    await_bytes(OW.at[1 - c], ow_sem.at[2])
    PG[...] = jnp.concatenate([GB[j, 1:2] for j in range(8)], axis=1)
    branch = jnp.concatenate([BRR[j] for j in range(8)], axis=1)
    square = jnp.zeros((BLK, 1), F32)
    for j in range(8):
        mixed = jnp.dot(branch, OW[j % 2, j // 2], preferred_element_type=F32).astype(BF16).astype(F32)
        square = square + jnp.sum(mixed * mixed, axis=1, keepdims=True)
        MX[:, 256 * j : 256 * j + 256] = mixed
    scale = lax.rsqrt(square * (1.0 / D) + EPS)
    gu.event(5)
    dw.start()
    dw.start_second()
    await_bytes(RB.at[pl.ds(0, 7)], sem.at[7])
    for j in range(8):
        cols = slice(256 * j, 256 * j + 256)
        mixed = MX[:, cols] * scale * GB[j, 0:1]
        ST[x, :, cols] = (RB[j].astype(F32) + mixed).astype(BF16)

    for part, step in ((0, 1), (1, 3), (1, 1), (0, 3)):
        ref = ST.at[x, pl.ds(48 * part, 48)]
        remote(ref, ref, sem.at[12], ag_ring.at[0 if step == 1 else 1, part], along_x(step))
    gu.event(6)
    gu.event(7)
    for part, step in ((0, 1), (1, 3)):
        came = lax.rem(x + 4 - step, 4)
        ref = ST.at[came, pl.ds(48 * part, 48)]
        await_bytes(ref, ag_ring.at[0 if step == 1 else 1, part])
        remote(ref, ref, sem.at[12], ag_ring.at[2, part], along_x(step))
    def normalize(blocks):
        for n, q in enumerate(blocks):
            for r in range(0, BLK, 16):
                stream = ST[q, r : r + 16].astype(F32)
                total = jnp.sum(stream * stream, axis=1, keepdims=True)
                NB[n, r : r + 16] = (stream * lax.rsqrt(total * (1.0 / D) + EPS) * PG[...]).astype(BF16)

    def hidden(blocks, p):
        lhs = NB[0 : len(blocks)].reshape(BLK * len(blocks), D)
        for i in range(5):
            weights = GU[p, :, :, 256 * i : 256 * i + 256].reshape(D, 256)
            both = jnp.dot(lhs, weights, preferred_element_type=F32)
            act = (jax.nn.silu(both[:, :128]) * both[:, 128:]).astype(BF16)
            for n, q in enumerate(blocks):
                H[p, q, :, 128 * i : 128 * i + 128] = act[BLK * n : BLK * n + BLK]

    def hidden_tail(blocks):
        lhs = NB[0 : len(blocks)].reshape(BLK * len(blocks), D)
        weights = jnp.concatenate([GU[p, :, :, 1280:1408].reshape(D, 128) for p in (0, 1)], axis=1)
        both = jnp.dot(lhs, weights, preferred_element_type=F32)
        for p in (0, 1):
            tail = both[:, 128 * p : 128 * p + 128]
            act = (jax.nn.silu(tail[:, :64]) * tail[:, 64:]).astype(BF16)
            for n, q in enumerate(blocks):
                H[p, q, :, 640:704] = act[BLK * n : BLK * n + BLK]

    left, right, across = lax.rem(x + 3, 4), lax.rem(x + 1, 4), lax.rem(x + 2, 4)
    normalize([x])
    dw.event(1)
    gu.wait_pair(0)
    gu.wait_pair(1)
    hidden([x], 0)
    hidden([x], 1)
    hidden_tail([x])
    dw.event(2)
    for part, step in ((1, 1), (0, 3)):
        came = lax.rem(x + 4 - step, 4)
        await_bytes(ST.at[came, pl.ds(48 * part, 48)], ag_ring.at[0 if step == 1 else 1, part])
    normalize([left, right])
    hidden([left, right], 0)
    dw.event(3)
    hidden([left, right], 1)
    hidden_tail([left, right])
    dw.event(4)
    for part in (0, 1):
        await_bytes(ST.at[across, pl.ds(48 * part, 48)], ag_ring.at[2, part])
    theirs = pl.ds(pl.multiple_of(512 * x + 256 * (1 - c), 256), 256)
    remote(ST.at[:, :, theirs], XR, sem.at[15], sem.at[16], partner)
    normalize([across])
    hidden([across], 0)
    dw.event(5)
    hidden([across], 1)
    hidden_tail([across])
    dw.event(6)

    def down_of(p, chip, h):
        weights = jnp.concatenate([DW[p, 4 * chip + 2 * h], DW[p, 4 * chip + 2 * h + 1]], axis=1)
        return jnp.dot(H[p].reshape(HALF, HID), weights, preferred_element_type=F32)

    def down(chip, h):
        return down_of(c, chip, h) + down_of(1 - c, chip, h)

    QUARTER = HALF // 2
    top, bottom = pl.ds(0, QUARTER), pl.ds(QUARTER, QUARTER)

    def scatter_across(n, total):
        PB[n, 0] = total.astype(BF16)
        for m, (rows, step) in enumerate(((top, 1), (bottom, 3))):
            remote(PB.at[n, 0, rows], RA.at[n, m], rs_send.at[n, m], ra_recv.at[n, m], along_x(step))

    def scatter_near(n, h):
        for m, (chip, rows) in enumerate(((right, bottom), (left, top))):
            total = down(chip, h)
            PB[n, 1 + m] = total.astype(BF16)
            FO[n, m] = total[:QUARTER] if m == 0 else total[QUARTER:]
            remote(
                PB.at[n, 1 + m, rows], RC.at[m, c, rows], rs_send.at[n, 2 + m], rc_recv.at[m, c, 1 - m],
                (s, 2 * chip + h),
            )

    def scatter_relay(n, h):
        for m, (chip, rows) in enumerate(((right, top), (left, bottom))):
            await_bytes(RA.at[n, m], ra_recv.at[n, m])
            PB[n, 1 + m, rows] = (FO[n, m] + RA[n, m].astype(F32)).astype(BF16)
            remote(
                PB.at[n, 1 + m, rows], RC.at[m, c, rows], rs_send.at[n, 4 + m], rc_recv.at[m, c, m],
                (s, 2 * chip + h),
            )

    early = lax.div(y, 2)
    total = down_of(c, across, early)
    dw.wait_pair(0)
    scatter_across(0, total + down_of(1 - c, across, early))
    dw.event(7)
    scatter_near(0, early)
    dw.wait_pair(1)
    scatter_across(1, down(across, 1 - early))
    scatter_relay(0, early)
    scatter_near(1, 1 - early)
    PB[0, 3] = down(x, 1 - c).astype(BF16)
    remote(PB.at[0, 3], PO.at[c], sem.at[8], sem.at[18], partner)
    scatter_relay(1, 1 - early)
    PO[c] = down(x, c).astype(BF16)
    await_bytes(PO.at[1 - c], sem.at[18])
    sums = []
    for k in (0, 1):
        for m in (0, 1):
            for part, rows in ((0, top), (1, bottom)):
                await_bytes(RC.at[m, k, rows], rc_recv.at[m, k, part])
        total = PO[k].astype(F32) + RC[0, k].astype(F32) + RC[1, k].astype(F32)
        total = total.astype(BF16).astype(F32)
        FF[k] = total
        square = jnp.sum(total * total, axis=1, keepdims=True)
        sums.append(jnp.broadcast_to(square, (HALF, 128)).T[0:1])

    SQB[t] = jnp.concatenate(sums, axis=1)
    for k in range(1, 8):
        remote(SQB.at[t], SQB.at[t], sem.at[13], sem.at[14], (s, lax.rem(t + k, 8)))
    await_bytes(XR, sem.at[16])
    await_bytes(SQB.at[pl.ds(0, 7)], sem.at[14])
    square = SQB[0]
    for j in range(1, 8):
        square = square + SQB[j]
    scale = lax.rsqrt(square * (1.0 / D) + EPS)
    scale = jnp.broadcast_to(scale, (128, TOK)).T
    scale = jnp.concatenate([scale, scale], axis=1)
    gain = GS[2:3]
    mine_cols = pl.ds(pl.multiple_of(512 * x + 256 * c, 256), 256)
    for k, stream in ((c, ST[:, :, mine_cols]), (1 - c, XR[...])):
        stream = stream.reshape(HALF, 256).astype(F32)
        factor = jnp.where(k == 0, scale[:HALF], scale[HALF:])
        out_ref[k] = (stream + FF[k] * factor * gain).astype(BF16)

    gu.finish()
    dw.finish()
    await_bytes(HX, sem.at[0])
    await_bytes(HI, sem.at[2])
    await_bytes(GB.at[pl.ds(0, 7)], sem.at[4])
    await_bytes(RB.at[pl.ds(0, 7)], sem.at[6])
    await_bytes(CB, sem.at[17])
    await_bytes(BRR.at[pl.ds(0, 7)], sem.at[10])
    await_bytes(OW.at[c, pl.ds(0, 3)], ow_sem.at[0])
    await_bytes(OW.at[c], ow_sem.at[1])
    await_bytes(ST.at[pl.ds(0, 3)], sem.at[12])
    for n in (0, 1):
        for m in range(6):
            await_bytes(PB.at[0, 0, top], rs_send.at[n, m])
    await_bytes(PB.at[0, 3], sem.at[8])
    await_bytes(SQB.at[pl.ds(0, 7)], sem.at[13])
    await_bytes(XR, sem.at[15])


def body(
    gate_branch, recur_input, doc_ids, conv_taps, gate_map, input_map, decay_level, decay_extra, out_weight,
    residual, mix_gain, pre_gain, ffn_gain, gate_weight, up_weight, down_weight,
):
    vmem = pl.BlockSpec(memory_space=pltpu.VMEM)
    dma = pltpu.SemaphoreType.DMA
    out = pl.pallas_call(
        layer_kernel,
        name="layer",
        out_shape=pltpu.VMEM((2, HALF, 256), BF16),
        in_specs=[pl.BlockSpec(memory_space=pl.ANY)] * 16,
        out_specs=vmem,
        scratch_shapes=[
            pltpu.VMEM((TOK, CH), BF16),
            pltpu.VMEM((TOK, CH), BF16),
            pltpu.VMEM((6, 128), jnp.int32),
            pltpu.VMEM((4, CH), BF16),
            pltpu.VMEM((2, 64, 64), BF16),
            pltpu.VMEM((2, 64, 64), BF16),
            pltpu.VMEM((1, CH), F32),
            pltpu.VMEM((TOK, CH), F32),
            pltpu.VMEM((8, BLK, 256), BF16),
            pltpu.VMEM((1, 256), F32),
            pltpu.VMEM((1, 256), F32),
            pltpu.VMEM((1, 256), F32),
            pltpu.VMEM((HID, 128), BF16),
            pltpu.VMEM((HID, 128), BF16),
            pltpu.VMEM((2, 16, 128, 1408), BF16),
            pltpu.VMEM((2, 16, HID, 128), BF16),
            pltpu.VMEM((2, 4, 1024, 256), BF16),
            pltpu.VMEM((8, BLK, CH), BF16),
            pltpu.VMEM((8, BLK, CH), BF16),
            pltpu.VMEM((8, BLK, 256), BF16),
            pltpu.VMEM((8, 256), F32),
            pltpu.VMEM((8, 8, 256), F32),
            pltpu.VMEM((16, CH), BF16),
            pltpu.VMEM((6, 128), jnp.int32),
            pltpu.VMEM((TOK + 8, CH), F32),
            pltpu.VMEM((TOK + 8, CH), F32),
            pltpu.VMEM((TOK, CH), F32),
            pltpu.VMEM((TOK, CH), F32),
            pltpu.VMEM((TOK, CH), F32),
            pltpu.VMEM((TOK, CH), F32),
            pltpu.VMEM((TOK, CH), F32),
            pltpu.VMEM((8, CH), F32),
            pltpu.VMEM((REACH, 8, CH), F32),
            pltpu.VMEM((BLK, D), F32),
            pltpu.VMEM((4, BLK, D), BF16),
            pltpu.VMEM((2, BLK, D), BF16),
            pltpu.VMEM((2, 4, BLK, HID), BF16),
            pltpu.VMEM((2, 4, HALF, 256), BF16),
            pltpu.VMEM((2, 2, HALF // 2, 256), BF16),
            pltpu.VMEM((2, 2, HALF, 256), BF16),
            pltpu.VMEM((2, HALF, 256), BF16),
            pltpu.VMEM((2, 2, HALF // 2, 256), F32),
            pltpu.VMEM((2, HALF, 256), F32),
            pltpu.VMEM((8, 1, TOK), F32),
            pltpu.VMEM((4, BLK, 256), BF16),
            pltpu.VMEM((1, D), F32),
            dma((2, 16)),
            dma((2, 16)),
            dma((2,)),
            dma((2,)),
            dma((2,)),
            dma((2,)),
            dma((3, 2)),
            dma((3,)),
            dma((3, 2)),
            dma((2, 2)),
            dma((2, 2, 2)),
            dma((2, 6)),
            dma((16,)),
            dma((19,)),
        ],
        compiler_params=pltpu.CompilerParams(
            collective_id=0, has_side_effects=True, vmem_limit_bytes=60 * 1024 * 1024
        ),
    )(
        gate_branch,
        recur_input,
        doc_ids.reshape(6, 128),
        conv_taps,
        gate_map,
        input_map,
        decay_level.reshape(1, CH),
        decay_extra,
        out_weight,
        residual.reshape(8, BLK, 256),
        mix_gain.reshape(1, 256),
        pre_gain.reshape(1, 256),
        ffn_gain.reshape(1, 256),
        gate_weight.T,
        up_weight.T,
        down_weight,
    )
    return out.reshape(TOK, 256)


def solution(mesh):
    return jax.shard_map(
        body,
        mesh=mesh,
        in_specs=(
            P("sp", "tp"),
            P("sp", "tp"),
            P("sp"),
            P(None, "tp"),
            P("tp", None, None),
            P("tp", None, None),
            P("tp"),
            P("sp", "tp"),
            P(None, "tp"),
            P("sp", "tp"),
            P("tp"),
            P("tp"),
            P("tp"),
            P("sp", "tp"),
            P("sp", "tp"),
            P("tp", "sp"),
        ),
        out_specs=P("sp", "tp"),
        check_vma=False,
    )
```

```python
import jax
import jax.numpy as jnp
from jax import lax
from jax.experimental import pallas as pl
from jax.experimental.pallas import tpu as pltpu
from jax.sharding import PartitionSpec as P

MESH = pl.DeviceIdType.MESH
F32 = jnp.float32
BF16 = jnp.bfloat16

D = 2048
EPS = 1e-06
GATE_POWER = 8.0
TOK = 768
BLK = 96
HALF = 384
CH = 128
HID = 704
REACH = 6


def neg_expm1(u):
    series = 1.0 + u * (1.0 / 9.0)
    for n in (8.0, 7.0, 6.0, 5.0, 4.0, 3.0, 2.0):
        series = 1.0 + u * (1.0 / n) * series
    return jnp.where(u > -0.5, -u * series, 1.0 - jnp.exp(u))


def softplus(v):
    tail = jnp.exp(-jnp.abs(v))
    w = tail / (2.0 + tail)
    square = w * w
    series = jnp.full_like(w, 1.0 / 15.0)
    for n in (13.0, 11.0, 9.0, 7.0, 5.0, 3.0, 1.0):
        series = 1.0 / n + square * series
    return jnp.maximum(v, 0.0) + 2.0 * w * series


class TorusGather:
    def __init__(self, buf, rows, here, ring_send, ring_recv, pair_send, pair_recv):
        self.buf, self.rows = buf, rows
        self.z, self.y, self.c, self.t = here
        self.ring_send, self.ring_recv = ring_send, ring_recv
        self.pair_send, self.pair_recv = pair_send, pair_recv
        self.odd = lax.rem(self.y, 2)
        self.mate, self.other = 1 + 2 * self.odd, 3 - 2 * self.odd

    def slot(self, dz, dy):
        return lax.rem(self.z + dz, 4) * 4 + lax.rem(self.y + dy, 4)

    def at(self, half, a, b):
        return (a, b) if half == 0 else (b, a)

    def span(self, half, part):
        quarter = self.rows // 4
        first = half * 2 * quarter
        return (first, 2 * quarter) if part is None else (first + part * quarter, quarter)

    def piece(self, half, where, part=None):
        first, count = self.span(half, part)
        return self.buf.at[self.c, self.slot(*where), pl.ds(first, count)]

    def send(self, half, where, to, part=None):
        ref = self.piece(half, where, part)
        landed = [lax.rem(at + (4 - step), 4) for at, step in zip(where, to)]
        pltpu.make_async_remote_copy(
            src_ref=ref,
            dst_ref=ref,
            send_sem=self.ring_send,
            recv_sem=self.ring_recv.at[half, landed[0] * 4 + landed[1]],
            device_id=(self.slot(*to), self.t),
            device_id_type=MESH,
        ).start()

    def wait(self, half, where):
        ref = self.piece(half, where)
        pltpu.make_async_copy(ref, ref, self.ring_recv.at[half, where[0] * 4 + where[1]]).wait()
        self.pass_over(ref, where)

    def pass_over(self, ref, where):
        dy = where[1]
        if isinstance(dy, int):
            late = {0: 0, 1: self.odd, 2: 1, 3: 1 - self.odd}[dy]
        else:
            late = 0 if dy is self.mate else 1
        pltpu.make_async_remote_copy(
            src_ref=ref,
            dst_ref=ref,
            send_sem=self.pair_send,
            recv_sem=self.pair_recv.at[late],
            device_id=(self.slot(0, 0), self.t + 1 - 2 * self.c),
            device_id_type=MESH,
        ).start()

    def start(self):
        for half in (0, 1):
            for step in (1, 3):
                self.send(half, (0, 0), self.at(half, 0, step))

    def start_second(self):
        for half in (0, 1):
            for step in (1, 3):
                self.send(half, (0, 0), self.at(half, step, 0))
        self.pass_over(self.buf.at[self.c, self.slot(0, 0)], (0, 0))

    def spread(self, half, b, steps=(1, 3)):
        for step in steps:
            self.send(half, self.at(half, 0, b), self.at(half, step, 0))

    def relay(self, half, a, b):
        self.wait(half, self.at(half, a, b))
        self.send(half, self.at(half, a, b), self.at(half, 4 - a, 0))

    def event(self, number):
        at, wait = self.at, self.wait
        mate, other = self.mate, self.other
        if number == 1:
            for half in (0, 1):
                wait(half, at(half, 0, 3))
                self.send(half, at(half, 0, 3), at(half, 0, 1), part=0)
                wait(half, at(half, 0, 1))
                self.send(half, at(half, 0, 1), at(half, 0, 3), part=1)
            self.spread(0, mate)
            self.spread(0, other, (3,))
            self.spread(1, 3)
            self.spread(1, 1)
        if number == 2:
            self.relay(0, 3, 0)
            wait(0, at(0, 1, 0))
            wait(1, at(1, 0, 2))
            self.spread(1, 2)
            wait(0, at(0, 0, 2))
            self.spread(0, 2, (1,))
            self.spread(0, other, (1,))
            self.relay(1, 3, 0)
            wait(1, at(1, 1, 0))
        if number == 3:
            self.relay(0, 1, mate)
            wait(0, at(0, 3, mate))
            self.relay(1, 1, 3)
            wait(1, at(1, 3, 3))
        if number == 4:
            self.relay(0, 1, other)
            self.spread(0, 2, (3,))
            self.relay(1, 3, 1)
            wait(1, at(1, 1, 1))
            wait(0, at(0, 2, 0))
        if number == 5:
            self.relay(0, 3, 2)
            self.relay(1, 1, 2)
            wait(1, at(1, 3, 2))
            wait(0, at(0, 2, mate))
        if number == 6:
            wait(0, at(0, 3, other))
            wait(0, at(0, 2, other))
            wait(1, at(1, 2, 0))
            wait(1, at(1, 2, 3))
        if number == 7:
            wait(0, at(0, 1, 2))
            wait(0, at(0, 2, 2))
            wait(1, at(1, 2, 1))
            wait(1, at(1, 2, 2))

    def wait_pair(self, late):
        ref = self.buf.at[1 - self.c, pl.ds(0, 8)]
        pltpu.make_async_copy(ref, ref, self.pair_recv.at[late]).wait()

    def finish(self):
        ref = self.buf.at[self.c, pl.ds(0, 15)]
        pltpu.make_async_copy(ref, ref, self.ring_send).wait()
        ref = self.buf.at[self.c]
        pltpu.make_async_copy(ref, ref, self.pair_send).wait()


def layer_kernel(
    gate_hbm, rec_hbm, ids_hbm, taps_hbm, gmap_hbm, imap_hbm, level_hbm, extra_hbm, ow_hbm, res_hbm,
    mixg_hbm, preg_hbm, ffng_hbm, gw_hbm, uw_hbm, dw_hbm,
    out_ref,
    gate_ref, rec_ref, ids_ref, taps_ref, gmap_ref, imap_ref, level_ref, extra_ref, res_ref,
    mixg_ref, preg_ref, ffng_ref, gw_ref, uw_ref,
    GU, DW, OW, RP, GP, BH, BA, HX, HI, XF, IDF, FA, DV, S, PR, GL, CS, CB, MX, SQA, SO, XR, ST, SQC, SC, ACC, H,
    PB, RA, RC, PO, FO, FF, PRE, SQB,
    gu_ring, dw_ring, gu_sem, dw_sem, gu_pair, dw_pair, ba_ring, ba_far, ba_sem, ag_ring, ag_far, ra_recv, rc_recv, rs_send, in_sem, sem,
):
    s, t = lax.axis_index("sp"), lax.axis_index("tp")
    z, y = lax.div(s, 4), lax.rem(s, 4)
    x, c = lax.div(t, 2), lax.rem(t, 2)

    def remote(src, dst, send_sem, recv_sem, device):
        copy = pltpu.make_async_remote_copy(
            src_ref=src, dst_ref=dst, send_sem=send_sem, recv_sem=recv_sem, device_id=device, device_id_type=MESH
        )
        copy.start()

    def await_bytes(ref, semaphore):
        pltpu.make_async_copy(ref, ref, semaphore).wait()

    def along_x(step):
        return (s, lax.rem(x + step, 4) * 2 + c)

    partner = (s, t + 1 - 2 * c)
    here = (z, y, c, t)
    gu = TorusGather(GU, 128, here, gu_sem.at[0], gu_ring, gu_sem.at[1], gu_pair)
    dw = TorusGather(DW, HID, here, dw_sem.at[0], dw_ring, dw_sem.at[1], dw_pair)

    barrier = pltpu.get_barrier_semaphore()
    for k in range(1, REACH + 1):
        for peer in (lax.rem(s + k, 16), lax.rem(s + 16 - k, 16)):
            pl.semaphore_signal(barrier, inc=1, device_id=(peer, t), device_id_type=MESH)
    for k in range(1, 8):
        pl.semaphore_signal(barrier, inc=1, device_id=(s, lax.rem(t + k, 8)), device_id_type=MESH)

    own = z * 4 + y
    loads = []
    for src, dst in (
        (gw_hbm, gw_ref), (uw_hbm, uw_ref), (rec_hbm, rec_ref), (ids_hbm, ids_ref), (gate_hbm, gate_ref),
        (taps_hbm, taps_ref), (gmap_hbm, gmap_ref), (imap_hbm, imap_ref), (level_hbm, level_ref),
        (extra_hbm, extra_ref), (mixg_hbm, mixg_ref), (preg_hbm, preg_ref), (ffng_hbm, ffng_ref), (ow_hbm, OW.at[c]),
        (res_hbm, res_ref), (dw_hbm, DW.at[c, own]),
    ):
        loads.append(pltpu.make_async_copy(src, dst, in_sem.at[len(loads)]))
        loads[-1].start()

    loads[0].wait()
    loads[1].wait()
    for i in range(5):
        for n, ref in enumerate((gw_ref, uw_ref)):
            block = ref[128 * i : 128 * i + 128].astype(F32).T.astype(BF16)
            GU[c, own, :, 256 * i + 128 * n : 256 * i + 128 * n + 128] = block
    block = jnp.concatenate([gw_ref[640:704].astype(F32), uw_ref[640:704].astype(F32)], axis=0)
    GU[c, own, :, 1280:1408] = block.T.astype(BF16)
    for load in loads[2:4]:
        load.wait()
    IDF[8:] = jnp.concatenate(
        [jnp.broadcast_to(ids_ref[r : r + 1, :].astype(F32), (128, 128)).T for r in range(6)], axis=0
    )
    XF[8:] = rec_ref[...].astype(F32)

    pl.semaphore_wait(barrier, 2 * REACH + 7)

    after = (lax.rem(s + 1, 16), t)
    remote(rec_ref.at[pl.ds(TOK - 16, 16)], HX, sem.at[0], sem.at[1], after)
    remote(ids_ref, HI, sem.at[2], sem.at[3], after)
    gu.start()
    for load in loads[4:]:
        load.wait()

    RP[c] = res_ref[c]
    GP[c, 0:1] = mixg_ref[...]
    GP[c, 1:2] = preg_ref[...]
    remote(OW.at[c], OW.at[c], ba_sem.at[1], ba_sem.at[2], partner)
    remote(res_ref.at[1 - c], RP.at[c], ba_sem.at[3], ba_sem.at[4], partner)
    remote(GP.at[c], GP.at[c], ba_sem.at[5], ba_sem.at[6], partner)

    for r in range(6):
        rows = slice(128 * r, 128 * r + 128)
        GL[rows] = jax.nn.gelu(gate_ref[rows].astype(F32), approximate=True)
    pair = [
        jnp.concatenate(
            [
                jnp.concatenate([m[0].astype(F32), jnp.zeros((64, 64), F32)], axis=1),
                jnp.concatenate([jnp.zeros((64, 64), F32), m[1].astype(F32)], axis=1),
            ],
            axis=0,
        )
        for m in (gmap_ref, imap_ref)
    ]
    maps = jnp.concatenate(pair, axis=1).astype(BF16)
    rate = -GATE_POWER * softplus(-level_ref[...])
    taps = taps_ref[...].astype(F32)

    def drive(r):
        at = 8 + 128 * r
        ids = IDF[at : at + 128]
        conv = XF[at : at + 128] * taps[0:1]
        for k in (1, 2, 3):
            same = IDF[at - k : at - k + 128] == ids
            conv = conv + jnp.where(same, XF[at - k : at - k + 128], 0.0) * taps[k : k + 1]
        conv = conv.astype(BF16)
        gates = jax.nn.sigmoid(jnp.dot(conv, maps, preferred_element_type=F32))
        rows = slice(128 * r, 128 * r + 128)
        log_decay = rate * gates[:, :CH] + extra_ref[rows]
        FA[rows] = jnp.where(IDF[at - 1 : at + 127] == ids, jnp.exp(log_decay), 0.0)
        DV[rows] = jnp.sqrt(neg_expm1(2.0 * log_decay)) * gates[:, CH:] * conv.astype(F32)

    for r in range(1, 6):
        drive(r)
    await_bytes(HX, sem.at[1])
    await_bytes(HI, sem.at[3])
    XF[0:8] = HX[...].astype(F32)[8:16]
    rim_ids = jnp.broadcast_to(HI[5:6, :].astype(F32), (128, 128)).T[120:128]
    IDF[0:8] = jnp.where(s > 0, rim_ids, -1.0)

    drive(0)

    state = jnp.zeros((8, CH), F32)
    prod = jnp.ones((8, CH), F32)
    for i in range(BLK):
        at = pl.ds(i, 8, stride=BLK)
        f = FA[at, :]
        state = f * state + DV[at, :]
        prod = f * prod
        S[at, :] = state
        PR[at, :] = prod
    befores = []
    p_all, e_all = jnp.ones((1, CH), F32), jnp.zeros((1, CH), F32)
    for b in range(8):
        befores.append((p_all, e_all))
        e_all = prod[b : b + 1] * e_all + state[b : b + 1]
        p_all = prod[b : b + 1] * p_all
    CS[...] = jnp.concatenate([p_all, e_all, jnp.zeros((6, CH), F32)], axis=0)
    for k in range(1, REACH + 1):
        remote(CS, CB.at[k - 1], sem.at[17], sem.at[9], (lax.rem(s + k, 16), t))
    gu.start_second()
    gu.event(1)

    await_bytes(CB, sem.at[9])
    entering = jnp.zeros((1, CH), F32)
    for k in range(REACH, 0, -1):
        entering = jnp.where(s >= k, CB[k - 1, 0:1] * entering + CB[k - 1, 1:2], 0.0)
    for b in range(8):
        rows = slice(BLK * b, BLK * b + BLK)
        p_before, e_before = befores[b]
        states = S[rows] + PR[rows] * (e_before + p_before * entering)
        half, first = b // 4, BLK * (b % 4)
        BH[half, first : first + BLK] = (states * GL[rows]).astype(BF16)

    QUARTER = HALF // 2
    top, bottom = pl.ds(0, QUARTER), pl.ds(QUARTER, QUARTER)
    left, right, across = lax.rem(x + 3, 4), lax.rem(x + 1, 4), lax.rem(x + 2, 4)
    for part, step in ((0, 1), (1, 3), (1, 1), (0, 3)):
        rows = bottom if part else top
        for k in (0, 1):
            remote(
                BH.at[k, rows], BA.at[x, c, rows], ba_sem.at[0], ba_ring.at[0 if step == 1 else 1, c, part],
                (s, lax.rem(x + step, 4) * 2 + k),
            )
    remote(BH.at[1 - c], BA.at[x, c], sem.at[4], sem.at[5], partner)
    BA[x, c] = BH[c]
    for part, step, chip in ((0, 1, left), (1, 3, right)):
        rows = bottom if part else top
        for k in (0, 1):
            await_bytes(BA.at[chip, k, rows], ba_ring.at[0 if step == 1 else 1, k, part])
        ref = BA.at[chip, :, rows]
        remote(ref, ref, ba_sem.at[0], ba_far.at[part], along_x(step))
    gu.event(2)
    for part, step, chip in ((1, 1, left), (0, 3, right)):
        rows = bottom if part else top
        for k in (0, 1):
            await_bytes(BA.at[chip, k, rows], ba_ring.at[0 if step == 1 else 1, k, part])
    await_bytes(BA.at[x, 1 - c], sem.at[5])
    await_bytes(OW.at[1 - c], ba_sem.at[2])
    await_bytes(RP.at[1 - c], ba_sem.at[4])
    await_bytes(GP.at[1 - c], ba_sem.at[6])
    gu.event(3)
    for part in (0, 1):
        await_bytes(BA.at[across, :, bottom if part else top], ba_far.at[part])

    def as_row(square):
        return jnp.broadcast_to(square, (HALF, 128)).T[0:1]

    def chip_sums(ref, send_sem, recv_sem):
        for step in (1, 2, 3):
            remote(ref.at[x], ref.at[x], send_sem, recv_sem, along_x(step))

    def row_factors(ref, count):
        total = ref[0]
        for j in range(1, count):
            total = total + ref[j]
        return jnp.broadcast_to(lax.rsqrt(total * (1.0 / D) + EPS), (128, total.shape[1])).T

    branch = jnp.concatenate([BA[j // 2, j % 2] for j in range(8)], axis=1)
    square = jnp.zeros((HALF, 1), F32)
    for h in (0, 1):
        mixed = jnp.dot(branch, OW[h], preferred_element_type=F32).astype(BF16).astype(F32)
        MX[h] = mixed
        square = square + jnp.sum(mixed * mixed, axis=1, keepdims=True)
    SQA[x] = as_row(square)
    chip_sums(SQA, sem.at[10], sem.at[11])
    dw.start()
    gu.event(4)
    await_bytes(SQA.at[pl.ds(0, 3)], sem.at[11])
    factor = row_factors(SQA, 4)
    factor = jnp.concatenate([factor, factor], axis=1)
    square = jnp.zeros((HALF, 1), F32)
    for h in (0, 1):
        stream = (RP[h].astype(F32) + MX[h] * factor * GP[h, 0:1]).astype(BF16)
        SO[h] = stream
        stream = stream.astype(F32)
        ST[x, h] = (stream * GP[h, 1:2]).astype(BF16)
        square = square + jnp.sum(stream * stream, axis=1, keepdims=True)
    SQC[x] = as_row(square)
    chip_sums(SQC, sem.at[6], sem.at[7])

    for part, step in ((0, 1), (1, 3), (1, 1), (0, 3)):
        ref = ST.at[x, :, bottom if part else top]
        remote(ref, ref, sem.at[12], ag_ring.at[0 if step == 1 else 1, part], along_x(step))
    remote(SO.at[1 - c], XR, sem.at[15], sem.at[16], partner)
    gu.event(5)
    dw.start_second()

    early = lax.div(y, 2)

    def product(q, h, tile):
        rows = pl.ds(4 * q + 2 * h, 2)
        if tile < 10:
            p, i = tile // 5, tile % 5
            weights = GU[p, rows, :, 256 * i : 256 * i + 256].reshape(256, 256)
        else:
            weights = jnp.concatenate([GU[p, rows, :, 1280:1408].reshape(256, 128) for p in (0, 1)], axis=1)
        return jnp.dot(ST[q, h], weights, preferred_element_type=F32)

    def gather_in(tiles):
        for tile in tiles:
            total = ACC[tile]
            for q in (x, left, right):
                total = total + product(q, 1 - early, tile)
            ACC[tile] = total

    def hidden(tiles):
        factor = SC[...]
        for tile in tiles:
            both = ACC[tile] + product(across, early, tile) + product(across, 1 - early, tile)
            if tile < 10:
                p, i = tile // 5, tile % 5
                act = jax.nn.silu(both[:, :128] * factor) * (both[:, 128:] * factor)
                H[p, :, 128 * i : 128 * i + 128] = act.astype(BF16)
            else:
                for p in (0, 1):
                    tail = both[:, 128 * p : 128 * p + 128] * factor
                    H[p, :, 640:704] = (jax.nn.silu(tail[:, :64]) * tail[:, 64:]).astype(BF16)

    dw.event(1)
    for part, step, chip in ((0, 1, left), (1, 3, right)):
        ref = ST.at[chip, :, bottom if part else top]
        await_bytes(ref, ag_ring.at[0 if step == 1 else 1, part])
        remote(ref, ref, sem.at[12], ag_far.at[part], along_x(step))
    gu.event(6)
    gu.wait_pair(0)
    for tile in range(11):
        ACC[tile] = product(x, early, tile)
    gu.event(7)
    for part, step, chip in ((1, 1, left), (0, 3, right)):
        await_bytes(ST.at[chip, :, bottom if part else top], ag_ring.at[0 if step == 1 else 1, part])
    for tile in range(11):
        ACC[tile] = ACC[tile] + product(left, early, tile) + product(right, early, tile)
    dw.event(2)
    gu.wait_pair(1)
    gather_in(range(6))
    dw.event(3)
    gather_in(range(6, 11))
    await_bytes(SQC.at[pl.ds(0, 3)], sem.at[7])
    SC[...] = row_factors(SQC, 4)
    for part in (0, 1):
        await_bytes(ST.at[across, :, bottom if part else top], ag_far.at[part])
    hidden(range(6))
    dw.event(4)
    hidden(range(6, 11))
    dw.event(5)

    def down_of(p, chip, h):
        weights = jnp.concatenate([DW[p, 4 * chip + 2 * h], DW[p, 4 * chip + 2 * h + 1]], axis=1)
        return jnp.dot(H[p], weights, preferred_element_type=F32)

    def down(chip, h):
        return down_of(c, chip, h) + down_of(1 - c, chip, h)

    def scatter_across(n, h):
        PB[n, 0] = (PRE[0] + down_of(1 - c, across, h)).astype(BF16)
        for m, (rows, step) in enumerate(((top, 1), (bottom, 3))):
            remote(PB.at[n, 0, rows], RA.at[n, m], rs_send.at[n, m], ra_recv.at[n, m], along_x(step))

    def own_products(h):
        for m, chip in enumerate((across, right, left)):
            PRE[m] = down_of(c, chip, h)

    def scatter_near(n, h):
        for m, (chip, rows) in enumerate(((right, bottom), (left, top))):
            total = PRE[1 + m] + down_of(1 - c, chip, h)
            PB[n, 1 + m] = total.astype(BF16)
            FO[n, m] = total[:QUARTER] if m == 0 else total[QUARTER:]
            remote(
                PB.at[n, 1 + m, rows], RC.at[m, c, rows], rs_send.at[n, 2 + m], rc_recv.at[m, c, 1 - m],
                (s, 2 * chip + h),
            )

    def scatter_relay(n, h):
        for m, (chip, rows) in enumerate(((right, top), (left, bottom))):
            await_bytes(RA.at[n, m], ra_recv.at[n, m])
            PB[n, 1 + m, rows] = (FO[n, m] + RA[n, m].astype(F32)).astype(BF16)
            remote(
                PB.at[n, 1 + m, rows], RC.at[m, c, rows], rs_send.at[n, 4 + m], rc_recv.at[m, c, m],
                (s, 2 * chip + h),
            )

    own_products(early)
    dw.wait_pair(0)
    scatter_across(0, early)
    dw.event(6)
    scatter_near(0, early)
    dw.event(7)
    own_products(1 - early)
    dw.wait_pair(1)
    scatter_across(1, 1 - early)
    scatter_relay(0, early)
    scatter_near(1, 1 - early)
    PB[0, 3] = down(x, 1 - c).astype(BF16)
    remote(PB.at[0, 3], PO.at[c], sem.at[8], sem.at[18], partner)
    scatter_relay(1, 1 - early)
    PO[c] = down(x, c).astype(BF16)
    await_bytes(PO.at[1 - c], sem.at[18])
    sums = []
    for k in (0, 1):
        for m in (0, 1):
            for part, rows in ((0, top), (1, bottom)):
                await_bytes(RC.at[m, k, rows], rc_recv.at[m, k, part])
        total = PO[k].astype(F32) + RC[0, k].astype(F32) + RC[1, k].astype(F32)
        total = total.astype(BF16).astype(F32)
        FF[k] = total
        square = jnp.sum(total * total, axis=1, keepdims=True)
        sums.append(as_row(square))

    SQB[t] = jnp.concatenate(sums, axis=1)
    for k in range(1, 8):
        remote(SQB.at[t], SQB.at[t], sem.at[13], sem.at[14], (s, lax.rem(t + k, 8)))
    await_bytes(XR, sem.at[16])
    await_bytes(SQB.at[pl.ds(0, 7)], sem.at[14])
    factors = row_factors(SQB, 8)
    for k in (0, 1):
        factor = factors[HALF * k : HALF * k + HALF]
        FF[k] = FF[k] * jnp.concatenate([factor, factor], axis=1) * ffng_ref[...]
    out_ref[c] = (SO[c].astype(F32) + FF[c]).astype(BF16)
    out_ref[1 - c] = (XR[...].astype(F32) + FF[1 - c]).astype(BF16)

    gu.finish()
    dw.finish()
    await_bytes(HX, sem.at[0])
    await_bytes(HI, sem.at[2])
    await_bytes(CB, sem.at[17])
    await_bytes(BA.at[pl.ds(0, 3)], ba_sem.at[0])
    await_bytes(OW.at[c], ba_sem.at[1])
    await_bytes(RP.at[c], ba_sem.at[3])
    await_bytes(GP.at[c], ba_sem.at[5])
    await_bytes(BH.at[0], sem.at[4])
    await_bytes(SQA.at[pl.ds(0, 3)], sem.at[10])
    await_bytes(SQC.at[pl.ds(0, 3)], sem.at[6])
    await_bytes(XR, sem.at[15])
    await_bytes(ST.at[pl.ds(0, 3)], sem.at[12])
    for n in (0, 1):
        for m in range(6):
            await_bytes(PB.at[0, 0, top], rs_send.at[n, m])
    await_bytes(PB.at[0, 3], sem.at[8])
    await_bytes(SQB.at[pl.ds(0, 7)], sem.at[13])


def body(
    gate_branch, recur_input, doc_ids, conv_taps, gate_map, input_map, decay_level, decay_extra, out_weight,
    residual, mix_gain, pre_gain, ffn_gain, gate_weight, up_weight, down_weight,
):
    vmem = pl.BlockSpec(memory_space=pltpu.VMEM)
    dma = pltpu.SemaphoreType.DMA
    out = pl.pallas_call(
        layer_kernel,
        name="layer",
        out_shape=pltpu.VMEM((2, HALF, 256), BF16),
        in_specs=[pl.BlockSpec(memory_space=pl.ANY)] * 16,
        out_specs=vmem,
        scratch_shapes=[
            pltpu.VMEM((TOK, CH), BF16),
            pltpu.VMEM((TOK, CH), BF16),
            pltpu.VMEM((6, 128), jnp.int32),
            pltpu.VMEM((4, CH), BF16),
            pltpu.VMEM((2, 64, 64), BF16),
            pltpu.VMEM((2, 64, 64), BF16),
            pltpu.VMEM((1, CH), F32),
            pltpu.VMEM((TOK, CH), F32),
            pltpu.VMEM((2, HALF, 256), BF16),
            pltpu.VMEM((1, 256), F32),
            pltpu.VMEM((1, 256), F32),
            pltpu.VMEM((1, 256), F32),
            pltpu.VMEM((HID, 128), BF16),
            pltpu.VMEM((HID, 128), BF16),
            pltpu.VMEM((2, 16, 128, 1408), BF16),
            pltpu.VMEM((2, 16, HID, 128), BF16),
            pltpu.VMEM((2, 1024, 256), BF16),
            pltpu.VMEM((2, HALF, 256), BF16),
            pltpu.VMEM((2, 8, 256), F32),
            pltpu.VMEM((2, HALF, CH), BF16),
            pltpu.VMEM((4, 2, HALF, CH), BF16),
            pltpu.VMEM((16, CH), BF16),
            pltpu.VMEM((6, 128), jnp.int32),
            pltpu.VMEM((TOK + 8, CH), F32),
            pltpu.VMEM((TOK + 8, CH), F32),
            pltpu.VMEM((TOK, CH), F32),
            pltpu.VMEM((TOK, CH), F32),
            pltpu.VMEM((TOK, CH), F32),
            pltpu.VMEM((TOK, CH), F32),
            pltpu.VMEM((TOK, CH), F32),
            pltpu.VMEM((8, CH), F32),
            pltpu.VMEM((REACH, 8, CH), F32),
            pltpu.VMEM((2, HALF, 256), F32),
            pltpu.VMEM((4, 1, HALF), F32),
            pltpu.VMEM((2, HALF, 256), BF16),
            pltpu.VMEM((HALF, 256), BF16),
            pltpu.VMEM((4, 2, HALF, 256), BF16),
            pltpu.VMEM((4, 1, HALF), F32),
            pltpu.VMEM((HALF, 128), F32),
            pltpu.VMEM((11, HALF, 256), F32),
            pltpu.VMEM((2, HALF, HID), BF16),
            pltpu.VMEM((2, 4, HALF, 256), BF16),
            pltpu.VMEM((2, 2, HALF // 2, 256), BF16),
            pltpu.VMEM((2, 2, HALF, 256), BF16),
            pltpu.VMEM((2, HALF, 256), BF16),
            pltpu.VMEM((2, 2, HALF // 2, 256), F32),
            pltpu.VMEM((2, HALF, 256), F32),
            pltpu.VMEM((3, HALF, 256), F32),
            pltpu.VMEM((8, 1, TOK), F32),
            dma((2, 16)),
            dma((2, 16)),
            dma((2,)),
            dma((2,)),
            dma((2,)),
            dma((2,)),
            dma((2, 2, 2)),
            dma((2,)),
            dma((7,)),
            dma((2, 2)),
            dma((2,)),
            dma((2, 2)),
            dma((2, 2, 2)),
            dma((2, 6)),
            dma((16,)),
            dma((19,)),
        ],
        compiler_params=pltpu.CompilerParams(
            collective_id=0, has_side_effects=True, vmem_limit_bytes=60 * 1024 * 1024
        ),
    )(
        gate_branch,
        recur_input,
        doc_ids.reshape(6, 128),
        conv_taps,
        gate_map,
        input_map,
        decay_level.reshape(1, CH),
        decay_extra,
        out_weight,
        residual.reshape(2, HALF, 256),
        mix_gain.reshape(1, 256),
        pre_gain.reshape(1, 256),
        ffn_gain.reshape(1, 256),
        gate_weight.T,
        up_weight.T,
        down_weight,
    )
    return out.reshape(TOK, 256)


def solution(mesh):
    return jax.shard_map(
        body,
        mesh=mesh,
        in_specs=(
            P("sp", "tp"),
            P("sp", "tp"),
            P("sp"),
            P(None, "tp"),
            P("tp", None, None),
            P("tp", None, None),
            P("tp"),
            P("sp", "tp"),
            P(None, "tp"),
            P("sp", "tp"),
            P("tp"),
            P("tp"),
            P("tp"),
            P("sp", "tp"),
            P("sp", "tp"),
            P("tp", "sp"),
        ),
        out_specs=P("sp", "tp"),
        check_vma=False,
    )
```

```python
import jax
import jax.numpy as jnp
from jax import lax
from jax.experimental import pallas as pl
from jax.experimental.pallas import tpu as pltpu
from jax.sharding import PartitionSpec as P

MESH = pl.DeviceIdType.MESH
F32 = jnp.float32
BF16 = jnp.bfloat16

D = 2048
EPS = 1e-06
GATE_POWER = 8.0
TOK = 768
BLK = 96
HALF = 384
CH = 128
HID = 704
REACH = 6


def neg_expm1(u):
    series = 1.0 + u * (1.0 / 9.0)
    for n in (8.0, 7.0, 6.0, 5.0, 4.0, 3.0, 2.0):
        series = 1.0 + u * (1.0 / n) * series
    return jnp.where(u > -0.5, -u * series, 1.0 - jnp.exp(u))


def softplus(v):
    tail = jnp.exp(-jnp.abs(v))
    w = tail / (2.0 + tail)
    square = w * w
    series = jnp.full_like(w, 1.0 / 15.0)
    for n in (13.0, 11.0, 9.0, 7.0, 5.0, 3.0, 1.0):
        series = 1.0 / n + square * series
    return jnp.maximum(v, 0.0) + 2.0 * w * series


TOGETHER = (
    ((0, 0, 3), (0, 0, 1)),
    ((1, 3, 0), (1, 1, 0)),
    ((0, 1, 0), (1, 0, 1)),
    ((0, 3, "m"), (1, 3, 3)),
    ((1, 1, 1), (0, 2, 0)),
    ((1, 2, 3), (0, 2, "m")),
    ((0, 3, "o"), (0, 2, "o"), (1, 0, 2), (1, 3, 2)),
    ((0, 1, 2), (0, 2, 2), (1, 1, 2), (1, 2, 2)),
)
ALONE = (
    (0, 0, 2), (1, 2, 0), (0, 3, 0), (0, 1, "m"), (0, 1, "o"), (0, 3, 2),
    (1, 0, 3), (1, 3, 1), (1, 1, 3), (1, 2, 1),
)
GROUPS = (*TOGETHER, *((one,) for one in ALONE))


class TorusGather:
    def __init__(self, buf, rows, here, ring_send, ring_recv, pair_send, pair_recv):
        self.buf, self.rows = buf, rows
        self.z, self.y, self.c, self.t = here
        self.ring_send, self.ring_recv = ring_send, ring_recv
        self.pair_send, self.pair_recv = pair_send, pair_recv
        self.odd = lax.rem(self.y, 2)
        self.mate, self.other = 1 + 2 * self.odd, 3 - 2 * self.odd

    def slot(self, dz, dy):
        return lax.rem(self.z + dz, 4) * 4 + lax.rem(self.y + dy, 4)

    def at(self, half, a, b):
        return (a, b) if half == 0 else (b, a)

    def span(self, half, part):
        quarter = self.rows // 4
        first = half * 2 * quarter
        return (first, 2 * quarter) if part is None else (first + part * quarter, quarter)

    def piece(self, half, where, part=None):
        first, count = self.span(half, part)
        return self.buf.at[self.c, self.slot(*where), pl.ds(first, count)]

    def named(self, dy):
        return dy if isinstance(dy, int) else "m" if dy is self.mate else "o"

    def group(self, half, where):
        key = (half, where[0], self.named(where[1]))
        return next(n for n, keys in enumerate(GROUPS) if key in keys)

    def send(self, half, where, to, part=None):
        ref = self.piece(half, where, part)
        dz, dy = (where[0] - to[0]) % 4, where[1]
        if isinstance(dy, int):
            dy = (dy - to[1]) % 4
        pltpu.make_async_remote_copy(
            src_ref=ref,
            dst_ref=ref,
            send_sem=self.ring_send,
            recv_sem=self.ring_recv.at[self.group(half, (dz, dy))],
            device_id=(self.slot(*to), self.t),
            device_id_type=MESH,
        ).start()

    def wait(self, *pieces):
        number = self.group(*pieces[0])
        assert len(pieces) == len(GROUPS[number])
        assert all(self.group(*piece) == number for piece in pieces)
        ref = self.piece(*pieces[0])
        if len(pieces) > 1:
            ref = self.buf.at[self.c, pl.ds(0, len(pieces) // 2)]
        pltpu.make_async_copy(ref, ref, self.ring_recv.at[number]).wait()
        for half, where in pieces:
            self.pass_over(self.piece(half, where), where)

    def pass_over(self, ref, where):
        dy = where[1]
        if isinstance(dy, int):
            late = {0: 0, 1: self.odd, 2: 1, 3: 1 - self.odd}[dy]
        else:
            late = 0 if dy is self.mate else 1
        pltpu.make_async_remote_copy(
            src_ref=ref,
            dst_ref=ref,
            send_sem=self.pair_send,
            recv_sem=self.pair_recv.at[late],
            device_id=(self.slot(0, 0), self.t + 1 - 2 * self.c),
            device_id_type=MESH,
        ).start()

    def start(self):
        for half in (0, 1):
            for step in (1, 3):
                self.send(half, (0, 0), self.at(half, 0, step))

    def start_second(self):
        for half in (0, 1):
            for step in (1, 3):
                self.send(half, (0, 0), self.at(half, step, 0))
        self.pass_over(self.buf.at[self.c, self.slot(0, 0)], (0, 0))

    def spread(self, half, b, steps=(1, 3)):
        for step in steps:
            self.send(half, self.at(half, 0, b), self.at(half, step, 0))

    def relay(self, half, a, b):
        self.wait((half, self.at(half, a, b)))
        self.send(half, self.at(half, a, b), self.at(half, 4 - a, 0))

    def event(self, number):
        at, wait = self.at, self.wait
        mate, other = self.mate, self.other
        if number == 1:
            for half in (0, 1):
                wait((half, at(half, 0, 3)), (half, at(half, 0, 1)))
                self.send(half, at(half, 0, 3), at(half, 0, 1), part=0)
                self.send(half, at(half, 0, 1), at(half, 0, 3), part=1)
            self.spread(0, mate)
            self.spread(0, other, (3,))
            self.spread(1, 3)
            self.spread(1, 1)
        if number == 2:
            self.relay(0, 3, 0)
            wait((1, at(1, 0, 2)))
            self.spread(1, 2)
            wait((0, at(0, 0, 2)))
            self.spread(0, 2, (1,))
            self.spread(0, other, (1,))
            self.relay(1, 3, 0)
            wait((0, at(0, 1, 0)), (1, at(1, 1, 0)))
        if number == 3:
            self.relay(0, 1, mate)
            self.relay(1, 1, 3)
            wait((0, at(0, 3, mate)), (1, at(1, 3, 3)))
        if number == 4:
            self.relay(0, 1, other)
            self.spread(0, 2, (3,))
            self.relay(1, 3, 1)
            wait((1, at(1, 1, 1)), (0, at(0, 2, 0)))
        if number == 5:
            self.relay(1, 1, 2)
            wait((1, at(1, 3, 2)), (0, at(0, 2, mate)))
            self.relay(0, 3, 2)
        if number == 6:
            wait((0, at(0, 3, other)), (0, at(0, 2, other)), (1, at(1, 2, 0)), (1, at(1, 2, 3)))
        if number == 7:
            wait((0, at(0, 1, 2)), (0, at(0, 2, 2)), (1, at(1, 2, 1)), (1, at(1, 2, 2)))

    def wait_pair(self, late):
        ref = self.buf.at[1 - self.c, pl.ds(0, 8)]
        pltpu.make_async_copy(ref, ref, self.pair_recv.at[late]).wait()

    def finish(self):
        ref = self.buf.at[self.c, pl.ds(0, 15)]
        pltpu.make_async_copy(ref, ref, self.ring_send).wait()
        ref = self.buf.at[self.c]
        pltpu.make_async_copy(ref, ref, self.pair_send).wait()


def layer_kernel(
    gate_hbm, rec_hbm, ids_hbm, taps_hbm, gmap_hbm, imap_hbm, level_hbm, extra_hbm, ow_hbm, res_hbm,
    mixg_hbm, preg_hbm, ffng_hbm, gw_hbm, uw_hbm, dw_hbm,
    out_ref,
    gate_ref, rec_ref, ids_ref, taps_ref, gmap_ref, imap_ref, level_ref, extra_ref, res_ref,
    mixg_ref, preg_ref, ffng_ref, gw_ref, uw_ref,
    GU, DW, OW, RP, GP, BH, BA, HX, HI, XF, IDF, FA, DV, S, PR, GL, CS, CB, MX, SQA, SO, XR, ST, SQC, SC, ACC, H,
    PB, RA, RC, PO, FO, FF, PRE, SQB,
    gu_ring, dw_ring, gu_pair, dw_pair, ba_ring, ag_ring, ra_recv, rc_recv, own_sem, sem,
):
    s, t = lax.axis_index("sp"), lax.axis_index("tp")
    z, y = lax.div(s, 4), lax.rem(s, 4)
    x, c = lax.div(t, 2), lax.rem(t, 2)

    def remote(src, dst, send_sem, recv_sem, device):
        copy = pltpu.make_async_remote_copy(
            src_ref=src, dst_ref=dst, send_sem=send_sem, recv_sem=recv_sem, device_id=device, device_id_type=MESH
        )
        copy.start()

    def await_bytes(ref, semaphore):
        pltpu.make_async_copy(ref, ref, semaphore).wait()

    def along_x(step):
        return (s, lax.rem(x + step, 4) * 2 + c)

    partner = (s, t + 1 - 2 * c)
    here = (z, y, c, t)
    gu = TorusGather(GU, 128, here, own_sem.at[2], gu_ring, own_sem.at[3], gu_pair)
    dw = TorusGather(DW, HID, here, own_sem.at[14], dw_ring, own_sem.at[15], dw_pair)

    barrier = pltpu.get_barrier_semaphore()
    for k in range(1, REACH + 1):
        for peer in (lax.rem(s + k, 16), lax.rem(s + 16 - k, 16)):
            pl.semaphore_signal(barrier, inc=1, device_id=(peer, t), device_id_type=MESH)
    for k in range(1, 8):
        pl.semaphore_signal(barrier, inc=1, device_id=(s, lax.rem(t + k, 8)), device_id_type=MESH)

    own = z * 4 + y
    loads = []
    for src, dst in (
        (gw_hbm, gw_ref), (uw_hbm, uw_ref), (rec_hbm, rec_ref), (ids_hbm, ids_ref), (gate_hbm, gate_ref),
        (taps_hbm, taps_ref), (gmap_hbm, gmap_ref), (imap_hbm, imap_ref), (level_hbm, level_ref),
        (extra_hbm, extra_ref), (mixg_hbm, mixg_ref), (preg_hbm, preg_ref), (ffng_hbm, ffng_ref), (ow_hbm, OW.at[c]),
        (res_hbm, res_ref), (dw_hbm, DW.at[c, own]),
    ):
        loads.append(pltpu.make_async_copy(src, dst, own_sem.at[len(loads)]))
        loads[-1].start()

    loads[0].wait()
    loads[1].wait()
    for i in range(5):
        for n, ref in enumerate((gw_ref, uw_ref)):
            block = ref[128 * i : 128 * i + 128].astype(F32).T.astype(BF16)
            GU[c, own, :, 256 * i + 128 * n : 256 * i + 128 * n + 128] = block
    block = jnp.concatenate([gw_ref[640:704].astype(F32), uw_ref[640:704].astype(F32)], axis=0)
    GU[c, own, :, 1280:1408] = block.T.astype(BF16)
    for load in loads[2:4]:
        load.wait()
    IDF[8:] = jnp.concatenate(
        [jnp.broadcast_to(ids_ref[r : r + 1, :].astype(F32), (128, 128)).T for r in range(6)], axis=0
    )
    XF[8:] = rec_ref[...].astype(F32)

    pl.semaphore_wait(barrier, 2 * REACH + 7)

    after = (lax.rem(s + 1, 16), t)
    remote(rec_ref.at[pl.ds(TOK - 16, 16)], HX, own_sem.at[0], sem.at[0], after)
    remote(ids_ref, HI, own_sem.at[1], sem.at[1], after)
    gu.start()
    for load in loads[4:]:
        load.wait()

    RP[c] = res_ref[c]
    GP[c, 0:1] = mixg_ref[...]
    GP[c, 1:2] = preg_ref[...]
    remote(OW.at[c], OW.at[c], own_sem.at[4], sem.at[9], partner)
    remote(res_ref.at[1 - c], RP.at[c], own_sem.at[5], sem.at[10], partner)
    remote(GP.at[c], GP.at[c], own_sem.at[6], sem.at[11], partner)

    for r in range(6):
        rows = slice(128 * r, 128 * r + 128)
        GL[rows] = jax.nn.gelu(gate_ref[rows].astype(F32), approximate=True)
    pair = [
        jnp.concatenate(
            [
                jnp.concatenate([m[0].astype(F32), jnp.zeros((64, 64), F32)], axis=1),
                jnp.concatenate([jnp.zeros((64, 64), F32), m[1].astype(F32)], axis=1),
            ],
            axis=0,
        )
        for m in (gmap_ref, imap_ref)
    ]
    maps = jnp.concatenate(pair, axis=1).astype(BF16)
    rate = -GATE_POWER * softplus(-level_ref[...])
    taps = taps_ref[...].astype(F32)

    def drive(r):
        at = 8 + 128 * r
        ids = IDF[at : at + 128]
        conv = XF[at : at + 128] * taps[0:1]
        for k in (1, 2, 3):
            same = IDF[at - k : at - k + 128] == ids
            conv = conv + jnp.where(same, XF[at - k : at - k + 128], 0.0) * taps[k : k + 1]
        conv = conv.astype(BF16)
        gates = jax.nn.sigmoid(jnp.dot(conv, maps, preferred_element_type=F32))
        rows = slice(128 * r, 128 * r + 128)
        log_decay = rate * gates[:, :CH] + extra_ref[rows]
        FA[rows] = jnp.where(IDF[at - 1 : at + 127] == ids, jnp.exp(log_decay), 0.0)
        DV[rows] = jnp.sqrt(neg_expm1(2.0 * log_decay)) * gates[:, CH:] * conv.astype(F32)

    for r in range(1, 6):
        drive(r)
    await_bytes(HX, sem.at[0])
    await_bytes(HI, sem.at[1])
    XF[0:8] = HX[...].astype(F32)[8:16]
    rim_ids = jnp.broadcast_to(HI[5:6, :].astype(F32), (128, 128)).T[120:128]
    IDF[0:8] = jnp.where(s > 0, rim_ids, -1.0)

    drive(0)

    state = jnp.zeros((8, CH), F32)
    prod = jnp.ones((8, CH), F32)
    for i in range(BLK):
        at = pl.ds(i, 8, stride=BLK)
        f = FA[at, :]
        state = f * state + DV[at, :]
        prod = f * prod
        S[at, :] = state
        PR[at, :] = prod
    befores = []
    p_all, e_all = jnp.ones((1, CH), F32), jnp.zeros((1, CH), F32)
    for b in range(8):
        befores.append((p_all, e_all))
        e_all = prod[b : b + 1] * e_all + state[b : b + 1]
        p_all = prod[b : b + 1] * p_all
    CS[...] = jnp.concatenate([p_all, e_all, jnp.zeros((6, CH), F32)], axis=0)
    for k in range(1, REACH + 1):
        remote(CS, CB.at[k - 1], own_sem.at[7], sem.at[2], (lax.rem(s + k, 16), t))
    gu.start_second()
    gu.event(1)

    await_bytes(CB, sem.at[2])
    entering = jnp.zeros((1, CH), F32)
    for k in range(REACH, 0, -1):
        entering = jnp.where(s >= k, CB[k - 1, 0:1] * entering + CB[k - 1, 1:2], 0.0)
    for b in range(8):
        rows = slice(BLK * b, BLK * b + BLK)
        p_before, e_before = befores[b]
        states = S[rows] + PR[rows] * (e_before + p_before * entering)
        half, first = b // 4, BLK * (b % 4)
        BH[half, first : first + BLK] = (states * GL[rows]).astype(BF16)

    QUARTER = HALF // 2
    top, bottom = pl.ds(0, QUARTER), pl.ds(QUARTER, QUARTER)
    left, right, across = lax.rem(x + 3, 4), lax.rem(x + 1, 4), lax.rem(x + 2, 4)
    for part, step in ((0, 1), (1, 3), (1, 1), (0, 3)):
        rows = bottom if part else top
        for k in (0, 1):
            remote(
                BH.at[k, rows], BA.at[x, c, rows], own_sem.at[8], ba_ring.at[0 if step == 1 else 1, part],
                (s, lax.rem(x + step, 4) * 2 + k),
            )
    remote(BH.at[1 - c], BA.at[x, c], own_sem.at[9], sem.at[5], partner)
    BA[x, c] = BH[c]
    for part, step, chip in ((0, 1, left), (1, 3, right)):
        rows = bottom if part else top
        ref = BA.at[chip, :, rows]
        await_bytes(ref, ba_ring.at[0 if step == 1 else 1, part])
        remote(ref, ref, own_sem.at[8], ba_ring.at[2, 0], along_x(step))
    gu.event(2)
    for part, step, chip in ((1, 1, left), (0, 3, right)):
        rows = bottom if part else top
        await_bytes(BA.at[chip, :, rows], ba_ring.at[0 if step == 1 else 1, part])
    await_bytes(BA.at[x, 1 - c], sem.at[5])
    await_bytes(OW.at[1 - c], sem.at[9])
    await_bytes(RP.at[1 - c], sem.at[10])
    await_bytes(GP.at[1 - c], sem.at[11])
    gu.event(3)
    await_bytes(BA.at[across], ba_ring.at[2, 0])

    def as_row(square):
        return jnp.broadcast_to(square, (HALF, 128)).T[0:1]

    def chip_sums(ref, send_sem, recv_sem):
        for step in (1, 2, 3):
            remote(ref.at[x], ref.at[x], send_sem, recv_sem, along_x(step))

    def row_factors(ref, count):
        total = ref[0]
        for j in range(1, count):
            total = total + ref[j]
        return jnp.broadcast_to(lax.rsqrt(total * (1.0 / D) + EPS), (128, total.shape[1])).T

    branch = jnp.concatenate([BA[j // 2, j % 2] for j in range(8)], axis=1)
    square = jnp.zeros((HALF, 1), F32)
    for h in (0, 1):
        mixed = jnp.dot(branch, OW[h], preferred_element_type=F32).astype(BF16).astype(F32)
        MX[h] = mixed
        square = square + jnp.sum(mixed * mixed, axis=1, keepdims=True)
    SQA[x] = as_row(square)
    chip_sums(SQA, own_sem.at[10], sem.at[3])
    dw.start()
    gu.event(4)
    await_bytes(SQA.at[pl.ds(0, 3)], sem.at[3])
    factor = row_factors(SQA, 4)
    factor = jnp.concatenate([factor, factor], axis=1)
    square = jnp.zeros((HALF, 1), F32)
    for h in (0, 1):
        stream = (RP[h].astype(F32) + MX[h] * factor * GP[h, 0:1]).astype(BF16)
        SO[h] = stream
        stream = stream.astype(F32)
        ST[x, h] = (stream * GP[h, 1:2]).astype(BF16)
        square = square + jnp.sum(stream * stream, axis=1, keepdims=True)
    SQC[x] = as_row(square)
    chip_sums(SQC, own_sem.at[11], sem.at[4])

    for part, step in ((0, 1), (1, 3), (1, 1), (0, 3)):
        ref = ST.at[x, :, bottom if part else top]
        remote(ref, ref, own_sem.at[12], ag_ring.at[0 if step == 1 else 1, part], along_x(step))
    remote(SO.at[1 - c], XR, own_sem.at[13], sem.at[6], partner)
    gu.event(5)
    dw.start_second()

    early = lax.div(y, 2)

    def product(q, h, tile):
        rows = pl.ds(4 * q + 2 * h, 2)
        if tile < 10:
            p, i = tile // 5, tile % 5
            weights = GU[p, rows, :, 256 * i : 256 * i + 256].reshape(256, 256)
        else:
            weights = jnp.concatenate([GU[p, rows, :, 1280:1408].reshape(256, 128) for p in (0, 1)], axis=1)
        return jnp.dot(ST[q, h], weights, preferred_element_type=F32)

    def gather_in(tiles):
        for tile in tiles:
            total = ACC[tile]
            for q in (x, left, right):
                total = total + product(q, 1 - early, tile)
            ACC[tile] = total

    def hidden(tiles):
        factor = SC[...]
        for tile in tiles:
            both = ACC[tile] + product(across, early, tile) + product(across, 1 - early, tile)
            if tile < 10:
                p, i = tile // 5, tile % 5
                act = jax.nn.silu(both[:, :128] * factor) * (both[:, 128:] * factor)
                H[p, :, 128 * i : 128 * i + 128] = act.astype(BF16)
            else:
                for p in (0, 1):
                    tail = both[:, 128 * p : 128 * p + 128] * factor
                    H[p, :, 640:704] = (jax.nn.silu(tail[:, :64]) * tail[:, 64:]).astype(BF16)

    dw.event(1)
    for part, step, chip in ((0, 1, left), (1, 3, right)):
        ref = ST.at[chip, :, bottom if part else top]
        await_bytes(ref, ag_ring.at[0 if step == 1 else 1, part])
        remote(ref, ref, own_sem.at[12], ag_ring.at[2, 0], along_x(step))
    gu.event(6)
    gu.wait_pair(0)
    for tile in range(11):
        ACC[tile] = product(x, early, tile)
    gu.event(7)
    for part, step, chip in ((1, 1, left), (0, 3, right)):
        await_bytes(ST.at[chip, :, bottom if part else top], ag_ring.at[0 if step == 1 else 1, part])
    for tile in range(11):
        ACC[tile] = ACC[tile] + product(left, early, tile) + product(right, early, tile)
    dw.event(2)
    gu.wait_pair(1)
    gather_in(range(6))
    dw.event(3)
    gather_in(range(6, 11))
    await_bytes(SQC.at[pl.ds(0, 3)], sem.at[4])
    SC[...] = row_factors(SQC, 4)
    await_bytes(ST.at[across], ag_ring.at[2, 0])
    hidden(range(6))
    dw.event(4)
    hidden(range(6, 11))
    dw.event(5)

    def down_of(p, chip, h):
        weights = jnp.concatenate([DW[p, 4 * chip + 2 * h], DW[p, 4 * chip + 2 * h + 1]], axis=1)
        return jnp.dot(H[p], weights, preferred_element_type=F32)

    def down(chip, h):
        return down_of(c, chip, h) + down_of(1 - c, chip, h)

    def scatter_across(n, h):
        PB[n, 0] = (PRE[0] + down_of(1 - c, across, h)).astype(BF16)
        for m, (rows, step) in enumerate(((top, 1), (bottom, 3))):
            remote(PB.at[n, 0, rows], RA.at[n, m], own_sem.at[16], ra_recv.at[n, m], along_x(step))

    def own_products(h):
        for m, chip in enumerate((across, right, left)):
            PRE[m] = down_of(c, chip, h)

    def scatter_near(n, h):
        for m, (chip, rows) in enumerate(((right, bottom), (left, top))):
            total = PRE[1 + m] + down_of(1 - c, chip, h)
            PB[n, 1 + m] = total.astype(BF16)
            FO[n, m] = total[:QUARTER] if m == 0 else total[QUARTER:]
            remote(
                PB.at[n, 1 + m, rows], RC.at[m, c, rows], own_sem.at[16], rc_recv.at[0],
                (s, 2 * chip + h),
            )

    def scatter_relay(n, h):
        for m, (chip, rows) in enumerate(((right, top), (left, bottom))):
            await_bytes(RA.at[n, m], ra_recv.at[n, m])
            PB[n, 1 + m, rows] = (FO[n, m] + RA[n, m].astype(F32)).astype(BF16)
            remote(
                PB.at[n, 1 + m, rows], RC.at[m, c, rows], own_sem.at[16], rc_recv.at[1],
                (s, 2 * chip + h),
            )

    own_products(early)
    dw.wait_pair(0)
    scatter_across(0, early)
    dw.event(6)
    scatter_near(0, early)
    dw.event(7)
    own_products(1 - early)
    dw.wait_pair(1)
    scatter_across(1, 1 - early)
    scatter_relay(0, early)
    scatter_near(1, 1 - early)
    PB[0, 3] = down(x, 1 - c).astype(BF16)
    remote(PB.at[0, 3], PO.at[c], own_sem.at[17], sem.at[8], partner)
    scatter_relay(1, 1 - early)
    PO[c] = down(x, c).astype(BF16)
    await_bytes(PO.at[1 - c], sem.at[8])
    await_bytes(RC.at[0], rc_recv.at[0])
    for k in (0, 1):
        FF[k, :QUARTER] = PO[k, :QUARTER].astype(F32) + RC[1, k, :QUARTER].astype(F32)
        FF[k, QUARTER:] = PO[k, QUARTER:].astype(F32) + RC[0, k, QUARTER:].astype(F32)
    await_bytes(RC.at[0], rc_recv.at[1])
    sums = []
    for k in (0, 1):
        last = jnp.concatenate([RC[0, k, :QUARTER], RC[1, k, QUARTER:]], axis=0)
        total = (FF[k] + last.astype(F32)).astype(BF16).astype(F32)
        FF[k] = total
        square = jnp.sum(total * total, axis=1, keepdims=True)
        sums.append(as_row(square))

    SQB[t] = jnp.concatenate(sums, axis=1)
    for k in range(1, 8):
        remote(SQB.at[t], SQB.at[t], own_sem.at[18], sem.at[7], (s, lax.rem(t + k, 8)))
    await_bytes(XR, sem.at[6])
    await_bytes(SQB.at[pl.ds(0, 7)], sem.at[7])
    factors = row_factors(SQB, 8)
    for k in (0, 1):
        factor = factors[HALF * k : HALF * k + HALF]
        FF[k] = FF[k] * jnp.concatenate([factor, factor], axis=1) * ffng_ref[...]
    out_ref[c] = (SO[c].astype(F32) + FF[c]).astype(BF16)
    out_ref[1 - c] = (XR[...].astype(F32) + FF[1 - c]).astype(BF16)

    gu.finish()
    dw.finish()
    await_bytes(HX, own_sem.at[0])
    await_bytes(HI, own_sem.at[1])
    await_bytes(CB, own_sem.at[7])
    await_bytes(BA.at[pl.ds(0, 3)], own_sem.at[8])
    await_bytes(OW.at[c], own_sem.at[4])
    await_bytes(RP.at[c], own_sem.at[5])
    await_bytes(GP.at[c], own_sem.at[6])
    await_bytes(BH.at[0], own_sem.at[9])
    await_bytes(SQA.at[pl.ds(0, 3)], own_sem.at[10])
    await_bytes(SQC.at[pl.ds(0, 3)], own_sem.at[11])
    await_bytes(XR, own_sem.at[13])
    await_bytes(ST.at[pl.ds(0, 3)], own_sem.at[12])
    await_bytes(PB.at[:, pl.ds(0, 3)], own_sem.at[16])
    await_bytes(PB.at[0, 3], own_sem.at[17])
    await_bytes(SQB.at[pl.ds(0, 7)], own_sem.at[18])


def body(
    gate_branch, recur_input, doc_ids, conv_taps, gate_map, input_map, decay_level, decay_extra, out_weight,
    residual, mix_gain, pre_gain, ffn_gain, gate_weight, up_weight, down_weight,
):
    vmem = pl.BlockSpec(memory_space=pltpu.VMEM)
    dma = pltpu.SemaphoreType.DMA
    out = pl.pallas_call(
        layer_kernel,
        name="layer",
        out_shape=pltpu.VMEM((2, HALF, 256), BF16),
        in_specs=[pl.BlockSpec(memory_space=pl.ANY)] * 16,
        out_specs=vmem,
        scratch_shapes=[
            pltpu.VMEM((TOK, CH), BF16),
            pltpu.VMEM((TOK, CH), BF16),
            pltpu.VMEM((6, 128), jnp.int32),
            pltpu.VMEM((4, CH), BF16),
            pltpu.VMEM((2, 64, 64), BF16),
            pltpu.VMEM((2, 64, 64), BF16),
            pltpu.VMEM((1, CH), F32),
            pltpu.VMEM((TOK, CH), F32),
            pltpu.VMEM((2, HALF, 256), BF16),
            pltpu.VMEM((1, 256), F32),
            pltpu.VMEM((1, 256), F32),
            pltpu.VMEM((1, 256), F32),
            pltpu.VMEM((HID, 128), BF16),
            pltpu.VMEM((HID, 128), BF16),
            pltpu.VMEM((2, 16, 128, 1408), BF16),
            pltpu.VMEM((2, 16, HID, 128), BF16),
            pltpu.VMEM((2, 1024, 256), BF16),
            pltpu.VMEM((2, HALF, 256), BF16),
            pltpu.VMEM((2, 8, 256), F32),
            pltpu.VMEM((2, HALF, CH), BF16),
            pltpu.VMEM((4, 2, HALF, CH), BF16),
            pltpu.VMEM((16, CH), BF16),
            pltpu.VMEM((6, 128), jnp.int32),
            pltpu.VMEM((TOK + 8, CH), F32),
            pltpu.VMEM((TOK + 8, CH), F32),
            pltpu.VMEM((TOK, CH), F32),
            pltpu.VMEM((TOK, CH), F32),
            pltpu.VMEM((TOK, CH), F32),
            pltpu.VMEM((TOK, CH), F32),
            pltpu.VMEM((TOK, CH), F32),
            pltpu.VMEM((8, CH), F32),
            pltpu.VMEM((REACH, 8, CH), F32),
            pltpu.VMEM((2, HALF, 256), F32),
            pltpu.VMEM((4, 1, HALF), F32),
            pltpu.VMEM((2, HALF, 256), BF16),
            pltpu.VMEM((HALF, 256), BF16),
            pltpu.VMEM((4, 2, HALF, 256), BF16),
            pltpu.VMEM((4, 1, HALF), F32),
            pltpu.VMEM((HALF, 128), F32),
            pltpu.VMEM((11, HALF, 256), F32),
            pltpu.VMEM((2, HALF, HID), BF16),
            pltpu.VMEM((2, 4, HALF, 256), BF16),
            pltpu.VMEM((2, 2, HALF // 2, 256), BF16),
            pltpu.VMEM((2, 2, HALF, 256), BF16),
            pltpu.VMEM((2, HALF, 256), BF16),
            pltpu.VMEM((2, 2, HALF // 2, 256), F32),
            pltpu.VMEM((2, HALF, 256), F32),
            pltpu.VMEM((3, HALF, 256), F32),
            pltpu.VMEM((8, 1, TOK), F32),
            dma((len(GROUPS),)),
            dma((len(GROUPS),)),
            dma((2,)),
            dma((2,)),
            dma((3, 2)),
            dma((3, 2)),
            dma((2, 2)),
            dma((2,)),
            dma((19,)),
            dma((12,)),
        ],
        compiler_params=pltpu.CompilerParams(
            collective_id=0, has_side_effects=True, vmem_limit_bytes=60 * 1024 * 1024
        ),
    )(
        gate_branch,
        recur_input,
        doc_ids.reshape(6, 128),
        conv_taps,
        gate_map,
        input_map,
        decay_level.reshape(1, CH),
        decay_extra,
        out_weight,
        residual.reshape(2, HALF, 256),
        mix_gain.reshape(1, 256),
        pre_gain.reshape(1, 256),
        ffn_gain.reshape(1, 256),
        gate_weight.T,
        up_weight.T,
        down_weight,
    )
    return out.reshape(TOK, 256)


def solution(mesh):
    return jax.shard_map(
        body,
        mesh=mesh,
        in_specs=(
            P("sp", "tp"),
            P("sp", "tp"),
            P("sp"),
            P(None, "tp"),
            P("tp", None, None),
            P("tp", None, None),
            P("tp"),
            P("sp", "tp"),
            P(None, "tp"),
            P("sp", "tp"),
            P("tp"),
            P("tp"),
            P("tp"),
            P("sp", "tp"),
            P("sp", "tp"),
            P("tp", "sp"),
        ),
        out_specs=P("sp", "tp"),
        check_vma=False,
    )
```

```python
import jax
import jax.numpy as jnp
from jax import lax
from jax.experimental import pallas as pl
from jax.experimental.pallas import tpu as pltpu
from jax.sharding import PartitionSpec as P

MESH = pl.DeviceIdType.MESH
F32 = jnp.float32
BF16 = jnp.bfloat16

D = 2048
EPS = 1e-06
GATE_POWER = 8.0
TOK = 768
BLK = 96
HALF = 384
CH = 128
HID = 704
REACH = 6


def neg_expm1(u):
    series = 1.0 + u * (1.0 / 9.0)
    for n in (8.0, 7.0, 6.0, 5.0, 4.0, 3.0, 2.0):
        series = 1.0 + u * (1.0 / n) * series
    return jnp.where(u > -0.5, -u * series, 1.0 - jnp.exp(u))


def softplus(v):
    tail = jnp.exp(-jnp.abs(v))
    w = tail / (2.0 + tail)
    square = w * w
    series = jnp.full_like(w, 1.0 / 15.0)
    for n in (13.0, 11.0, 9.0, 7.0, 5.0, 3.0, 1.0):
        series = 1.0 / n + square * series
    return jnp.maximum(v, 0.0) + 2.0 * w * series


TOGETHER = (
    ((0, 0, 3), (0, 0, 1)),
    ((1, 3, 0), (1, 1, 0)),
    ((0, 1, 0), (1, 0, 1)),
    ((0, 3, "m"), (1, 3, 3)),
    ((1, 1, 1), (0, 2, 0)),
    ((1, 2, 3), (0, 2, "m")),
    ((0, 3, "o"), (0, 2, "o"), (1, 0, 2), (1, 3, 2)),
    ((0, 1, 2), (0, 2, 2), (1, 1, 2), (1, 2, 2)),
)
ALONE = (
    (0, 0, 2), (1, 2, 0), (0, 3, 0), (0, 1, "m"), (0, 1, "o"), (0, 3, 2),
    (1, 0, 3), (1, 3, 1), (1, 1, 3), (1, 2, 1),
)
GROUPS = (*TOGETHER, *((one,) for one in ALONE))


class TorusGather:
    def __init__(self, buf, rows, here, ring_send, ring_recv, pair_send, pair_recv):
        self.buf, self.rows = buf, rows
        self.z, self.y, self.c, self.t = here
        self.ring_send, self.ring_recv = ring_send, ring_recv
        self.pair_send, self.pair_recv = pair_send, pair_recv
        self.odd = lax.rem(self.y, 2)
        self.mate, self.other = 1 + 2 * self.odd, 3 - 2 * self.odd

    def slot(self, dz, dy):
        return lax.rem(self.z + dz, 4) * 4 + lax.rem(self.y + dy, 4)

    def at(self, half, a, b):
        return (a, b) if half == 0 else (b, a)

    def span(self, half, part):
        quarter = self.rows // 4
        first = half * 2 * quarter
        return (first, 2 * quarter) if part is None else (first + part * quarter, quarter)

    def piece(self, half, where, part=None):
        first, count = self.span(half, part)
        return self.buf.at[self.c, self.slot(*where), pl.ds(first, count)]

    def named(self, dy):
        return dy if isinstance(dy, int) else "m" if dy is self.mate else "o"

    def group(self, half, where):
        key = (half, where[0], self.named(where[1]))
        return next(n for n, keys in enumerate(GROUPS) if key in keys)

    def send(self, half, where, to, part=None):
        ref = self.piece(half, where, part)
        dz, dy = (where[0] - to[0]) % 4, where[1]
        if isinstance(dy, int):
            dy = (dy - to[1]) % 4
        pltpu.make_async_remote_copy(
            src_ref=ref,
            dst_ref=ref,
            send_sem=self.ring_send,
            recv_sem=self.ring_recv.at[self.group(half, (dz, dy))],
            device_id=(self.slot(*to), self.t),
            device_id_type=MESH,
        ).start()

    def wait(self, *pieces):
        number = self.group(*pieces[0])
        assert len(pieces) == len(GROUPS[number])
        assert all(self.group(*piece) == number for piece in pieces)
        ref = self.piece(*pieces[0])
        if len(pieces) > 1:
            ref = self.buf.at[self.c, pl.ds(0, len(pieces) // 2)]
        pltpu.make_async_copy(ref, ref, self.ring_recv.at[number]).wait()
        for half, where in pieces:
            self.pass_over(self.piece(half, where), where)

    def pass_over(self, ref, where):
        dy = where[1]
        if isinstance(dy, int):
            stage = {0: 0, 1: 1 + self.odd, 2: 2, 3: 2 - self.odd}[dy]
        else:
            stage = 1 if dy is self.mate else 2
        pltpu.make_async_remote_copy(
            src_ref=ref,
            dst_ref=ref,
            send_sem=self.pair_send,
            recv_sem=self.pair_recv.at[stage],
            device_id=(self.slot(0, 0), self.t + 1 - 2 * self.c),
            device_id_type=MESH,
        ).start()

    def start(self):
        for half in (0, 1):
            for step in (1, 3):
                self.send(half, (0, 0), self.at(half, 0, step))

    def start_second(self):
        for half in (0, 1):
            for step in (1, 3):
                self.send(half, (0, 0), self.at(half, step, 0))
        self.pass_over(self.buf.at[self.c, self.slot(0, 0)], (0, 0))

    def spread(self, half, b, steps=(1, 3)):
        for step in steps:
            self.send(half, self.at(half, 0, b), self.at(half, step, 0))

    def relay(self, half, a, b):
        self.wait((half, self.at(half, a, b)))
        self.send(half, self.at(half, a, b), self.at(half, 4 - a, 0))

    def event(self, number):
        at, wait = self.at, self.wait
        mate, other = self.mate, self.other
        if number == 1:
            for half in (0, 1):
                wait((half, at(half, 0, 3)), (half, at(half, 0, 1)))
                self.send(half, at(half, 0, 3), at(half, 0, 1), part=0)
                self.send(half, at(half, 0, 1), at(half, 0, 3), part=1)
            self.spread(0, mate)
            self.spread(0, other, (3,))
            self.spread(1, 3)
            self.spread(1, 1)
        if number == 2:
            self.relay(0, 3, 0)
            wait((1, at(1, 0, 2)))
            self.spread(1, 2)
            wait((0, at(0, 0, 2)))
            self.spread(0, 2, (1,))
            self.spread(0, other, (1,))
            self.relay(1, 3, 0)
            wait((0, at(0, 1, 0)), (1, at(1, 1, 0)))
        if number == 3:
            self.relay(0, 1, mate)
            self.relay(1, 1, 3)
            wait((0, at(0, 3, mate)), (1, at(1, 3, 3)))
        if number == 4:
            self.relay(0, 1, other)
            self.spread(0, 2, (3,))
            self.relay(1, 3, 1)
            wait((1, at(1, 1, 1)), (0, at(0, 2, 0)))
        if number == 5:
            self.relay(1, 1, 2)
            wait((1, at(1, 3, 2)), (0, at(0, 2, mate)))
            self.relay(0, 3, 2)
        if number == 6:
            wait((0, at(0, 3, other)), (0, at(0, 2, other)), (1, at(1, 2, 0)), (1, at(1, 2, 3)))
        if number == 7:
            wait((0, at(0, 1, 2)), (0, at(0, 2, 2)), (1, at(1, 2, 1)), (1, at(1, 2, 2)))

    def wait_pair(self, stage):
        ref = self.buf.at[1 - self.c, pl.ds(0, (4, 4, 8)[stage])]
        pltpu.make_async_copy(ref, ref, self.pair_recv.at[stage]).wait()

    def finish(self):
        ref = self.buf.at[self.c, pl.ds(0, 15)]
        pltpu.make_async_copy(ref, ref, self.ring_send).wait()
        ref = self.buf.at[self.c]
        pltpu.make_async_copy(ref, ref, self.pair_send).wait()


def layer_kernel(
    gate_hbm, rec_hbm, ids_hbm, taps_hbm, gmap_hbm, imap_hbm, level_hbm, extra_hbm, ow_hbm, res_hbm,
    mixg_hbm, preg_hbm, ffng_hbm, gw_hbm, uw_hbm, dw_hbm,
    out_ref,
    gate_ref, rec_ref, ids_ref, taps_ref, gmap_ref, imap_ref, level_ref, extra_ref, res_ref,
    mixg_ref, preg_ref, ffng_ref, gw_ref, uw_ref,
    GU, DW, OW, RP, GP, BH, BA, HX, HI, XF, IDF, FA, DV, S, PR, GL, CS, CB, MX, SQA, SO, XR, ST, SQC, SC, ACC, H,
    PB, PS, RA, RC, PO, FO, FL, FF, PRE, LPRE, SQB,
    gu_ring, dw_ring, gu_pair, dw_pair, ba_ring, ag_ring, ra_recv, rc_recv, own_sem, sem,
):
    s, t = lax.axis_index("sp"), lax.axis_index("tp")
    z, y = lax.div(s, 4), lax.rem(s, 4)
    x, c = lax.div(t, 2), lax.rem(t, 2)

    def remote(src, dst, send_sem, recv_sem, device):
        copy = pltpu.make_async_remote_copy(
            src_ref=src, dst_ref=dst, send_sem=send_sem, recv_sem=recv_sem, device_id=device, device_id_type=MESH
        )
        copy.start()

    def await_bytes(ref, semaphore):
        pltpu.make_async_copy(ref, ref, semaphore).wait()

    def along_x(step):
        return (s, lax.rem(x + step, 4) * 2 + c)

    partner = (s, t + 1 - 2 * c)
    here = (z, y, c, t)
    gu = TorusGather(GU, 128, here, own_sem.at[2], gu_ring, own_sem.at[3], gu_pair)
    dw = TorusGather(DW, HID, here, own_sem.at[14], dw_ring, own_sem.at[15], dw_pair)

    barrier = pltpu.get_barrier_semaphore()
    for k in range(1, REACH + 1):
        for peer in (lax.rem(s + k, 16), lax.rem(s + 16 - k, 16)):
            pl.semaphore_signal(barrier, inc=1, device_id=(peer, t), device_id_type=MESH)
    for k in range(1, 8):
        pl.semaphore_signal(barrier, inc=1, device_id=(s, lax.rem(t + k, 8)), device_id_type=MESH)

    own = z * 4 + y
    loads = []
    for src, dst in (
        (gw_hbm, gw_ref), (uw_hbm, uw_ref), (rec_hbm, rec_ref), (ids_hbm, ids_ref), (gate_hbm, gate_ref),
        (taps_hbm, taps_ref), (gmap_hbm, gmap_ref), (imap_hbm, imap_ref), (level_hbm, level_ref),
        (extra_hbm, extra_ref), (mixg_hbm, mixg_ref), (preg_hbm, preg_ref), (ffng_hbm, ffng_ref), (ow_hbm, OW.at[c]),
        (res_hbm, res_ref), (dw_hbm, DW.at[c, own]),
    ):
        loads.append(pltpu.make_async_copy(src, dst, own_sem.at[len(loads)]))
        loads[-1].start()

    loads[0].wait()
    loads[1].wait()
    for i in range(5):
        for n, ref in enumerate((gw_ref, uw_ref)):
            block = ref[128 * i : 128 * i + 128].astype(F32).T.astype(BF16)
            GU[c, own, :, 256 * i + 128 * n : 256 * i + 128 * n + 128] = block
    block = jnp.concatenate([gw_ref[640:704].astype(F32), uw_ref[640:704].astype(F32)], axis=0)
    GU[c, own, :, 1280:1408] = block.T.astype(BF16)
    for load in loads[2:4]:
        load.wait()
    IDF[8:] = jnp.concatenate(
        [jnp.broadcast_to(ids_ref[r : r + 1, :].astype(F32), (128, 128)).T for r in range(6)], axis=0
    )
    XF[8:] = rec_ref[...].astype(F32)

    pl.semaphore_wait(barrier, 2 * REACH + 7)

    after = (lax.rem(s + 1, 16), t)
    remote(rec_ref.at[pl.ds(TOK - 16, 16)], HX, own_sem.at[0], sem.at[0], after)
    remote(ids_ref, HI, own_sem.at[1], sem.at[1], after)
    gu.start()
    for load in loads[4:]:
        load.wait()

    RP[c] = res_ref[c]
    GP[c, 0:1] = mixg_ref[...]
    GP[c, 1:2] = preg_ref[...]
    remote(OW.at[c], OW.at[c], own_sem.at[4], sem.at[9], partner)
    remote(res_ref.at[1 - c], RP.at[c], own_sem.at[5], sem.at[10], partner)
    remote(GP.at[c], GP.at[c], own_sem.at[6], sem.at[11], partner)

    for r in range(6):
        rows = slice(128 * r, 128 * r + 128)
        GL[rows] = jax.nn.gelu(gate_ref[rows].astype(F32), approximate=True)
    pair = [
        jnp.concatenate(
            [
                jnp.concatenate([m[0].astype(F32), jnp.zeros((64, 64), F32)], axis=1),
                jnp.concatenate([jnp.zeros((64, 64), F32), m[1].astype(F32)], axis=1),
            ],
            axis=0,
        )
        for m in (gmap_ref, imap_ref)
    ]
    maps = jnp.concatenate(pair, axis=1).astype(BF16)
    rate = -GATE_POWER * softplus(-level_ref[...])
    taps = taps_ref[...].astype(F32)

    def drive(r):
        at = 8 + 128 * r
        ids = IDF[at : at + 128]
        conv = XF[at : at + 128] * taps[0:1]
        for k in (1, 2, 3):
            same = IDF[at - k : at - k + 128] == ids
            conv = conv + jnp.where(same, XF[at - k : at - k + 128], 0.0) * taps[k : k + 1]
        conv = conv.astype(BF16)
        gates = jax.nn.sigmoid(jnp.dot(conv, maps, preferred_element_type=F32))
        rows = slice(128 * r, 128 * r + 128)
        log_decay = rate * gates[:, :CH] + extra_ref[rows]
        FA[rows] = jnp.where(IDF[at - 1 : at + 127] == ids, jnp.exp(log_decay), 0.0)
        DV[rows] = jnp.sqrt(neg_expm1(2.0 * log_decay)) * gates[:, CH:] * conv.astype(F32)

    for r in range(1, 6):
        drive(r)
    await_bytes(HX, sem.at[0])
    await_bytes(HI, sem.at[1])
    XF[0:8] = HX[...].astype(F32)[8:16]
    rim_ids = jnp.broadcast_to(HI[5:6, :].astype(F32), (128, 128)).T[120:128]
    IDF[0:8] = jnp.where(s > 0, rim_ids, -1.0)

    drive(0)

    state = jnp.zeros((8, CH), F32)
    prod = jnp.ones((8, CH), F32)
    for i in range(BLK):
        at = pl.ds(i, 8, stride=BLK)
        f = FA[at, :]
        state = f * state + DV[at, :]
        prod = f * prod
        S[at, :] = state
        PR[at, :] = prod
    befores = []
    p_all, e_all = jnp.ones((1, CH), F32), jnp.zeros((1, CH), F32)
    for b in range(8):
        befores.append((p_all, e_all))
        e_all = prod[b : b + 1] * e_all + state[b : b + 1]
        p_all = prod[b : b + 1] * p_all
    CS[...] = jnp.concatenate([p_all, e_all, jnp.zeros((6, CH), F32)], axis=0)
    for k in range(1, REACH + 1):
        remote(CS, CB.at[k - 1], own_sem.at[7], sem.at[2], (lax.rem(s + k, 16), t))
    gu.start_second()
    gu.event(1)

    await_bytes(CB, sem.at[2])
    entering = jnp.zeros((1, CH), F32)
    for k in range(REACH, 0, -1):
        entering = jnp.where(s >= k, CB[k - 1, 0:1] * entering + CB[k - 1, 1:2], 0.0)
    for b in range(8):
        rows = slice(BLK * b, BLK * b + BLK)
        p_before, e_before = befores[b]
        states = S[rows] + PR[rows] * (e_before + p_before * entering)
        half, first = b // 4, BLK * (b % 4)
        BH[half, first : first + BLK] = (states * GL[rows]).astype(BF16)

    QUARTER = HALF // 2
    top, bottom = pl.ds(0, QUARTER), pl.ds(QUARTER, QUARTER)
    left, right, across = lax.rem(x + 3, 4), lax.rem(x + 1, 4), lax.rem(x + 2, 4)
    for part, step in ((0, 1), (1, 3), (1, 1), (0, 3)):
        rows = bottom if part else top
        for k in (0, 1):
            remote(
                BH.at[k, rows], BA.at[x, c, rows], own_sem.at[8], ba_ring.at[0 if step == 1 else 1, part],
                (s, lax.rem(x + step, 4) * 2 + k),
            )
    remote(BH.at[1 - c], BA.at[x, c], own_sem.at[9], sem.at[5], partner)
    BA[x, c] = BH[c]
    for part, step, chip in ((0, 1, left), (1, 3, right)):
        rows = bottom if part else top
        ref = BA.at[chip, :, rows]
        await_bytes(ref, ba_ring.at[0 if step == 1 else 1, part])
        remote(ref, ref, own_sem.at[8], ba_ring.at[2, 0], along_x(step))
    gu.event(2)
    for part, step, chip in ((1, 1, left), (0, 3, right)):
        rows = bottom if part else top
        await_bytes(BA.at[chip, :, rows], ba_ring.at[0 if step == 1 else 1, part])
    await_bytes(BA.at[x, 1 - c], sem.at[5])
    await_bytes(OW.at[1 - c], sem.at[9])
    await_bytes(RP.at[1 - c], sem.at[10])
    await_bytes(GP.at[1 - c], sem.at[11])
    gu.event(3)
    await_bytes(BA.at[across], ba_ring.at[2, 0])

    def as_row(square):
        return jnp.broadcast_to(square, (HALF, 128)).T[0:1]

    def chip_sums(ref, send_sem, recv_sem):
        for step in (1, 2, 3):
            remote(ref.at[x], ref.at[x], send_sem, recv_sem, along_x(step))

    def row_factors(ref, count):
        total = ref[0]
        for j in range(1, count):
            total = total + ref[j]
        return jnp.broadcast_to(lax.rsqrt(total * (1.0 / D) + EPS), (128, total.shape[1])).T

    branch = jnp.concatenate([BA[j // 2, j % 2] for j in range(8)], axis=1)
    square = jnp.zeros((HALF, 1), F32)
    for h in (0, 1):
        mixed = jnp.dot(branch, OW[h], preferred_element_type=F32).astype(BF16).astype(F32)
        MX[h] = mixed
        square = square + jnp.sum(mixed * mixed, axis=1, keepdims=True)
    SQA[x] = as_row(square)
    chip_sums(SQA, own_sem.at[10], sem.at[3])
    dw.start()
    gu.event(4)
    await_bytes(SQA.at[pl.ds(0, 3)], sem.at[3])
    factor = row_factors(SQA, 4)
    factor = jnp.concatenate([factor, factor], axis=1)
    square = jnp.zeros((HALF, 1), F32)
    for h in (0, 1):
        stream = (RP[h].astype(F32) + MX[h] * factor * GP[h, 0:1]).astype(BF16)
        SO[h] = stream
        stream = stream.astype(F32)
        ST[x, h] = (stream * GP[h, 1:2]).astype(BF16)
        square = square + jnp.sum(stream * stream, axis=1, keepdims=True)
    SQC[x] = as_row(square)
    chip_sums(SQC, own_sem.at[11], sem.at[4])

    for part, step in ((0, 1), (1, 3), (1, 1), (0, 3)):
        ref = ST.at[x, :, bottom if part else top]
        remote(ref, ref, own_sem.at[12], ag_ring.at[0 if step == 1 else 1, part], along_x(step))
    remote(SO.at[1 - c], XR, own_sem.at[13], sem.at[6], partner)
    gu.event(5)
    dw.start_second()

    early = lax.div(y, 2)

    def product(q, h, tile):
        rows = pl.ds(4 * q + 2 * h, 2)
        if tile < 10:
            p, i = tile // 5, tile % 5
            weights = GU[p, rows, :, 256 * i : 256 * i + 256].reshape(256, 256)
        else:
            weights = jnp.concatenate([GU[p, rows, :, 1280:1408].reshape(256, 128) for p in (0, 1)], axis=1)
        return jnp.dot(ST[q, h], weights, preferred_element_type=F32)

    def gather_in(tiles):
        for tile in tiles:
            total = ACC[tile]
            for q in (x, left, right):
                total = total + product(q, 1 - early, tile)
            ACC[tile] = total

    def hidden(tiles):
        factor = SC[...]
        for tile in tiles:
            both = ACC[tile] + product(across, early, tile) + product(across, 1 - early, tile)
            if tile < 10:
                p, i = tile // 5, tile % 5
                act = jax.nn.silu(both[:, :128] * factor) * (both[:, 128:] * factor)
                H[p, :, 128 * i : 128 * i + 128] = act.astype(BF16)
            else:
                for p in (0, 1):
                    tail = both[:, 128 * p : 128 * p + 128] * factor
                    H[p, :, 640:704] = (jax.nn.silu(tail[:, :64]) * tail[:, 64:]).astype(BF16)

    dw.event(1)
    for part, step, chip in ((0, 1, left), (1, 3, right)):
        ref = ST.at[chip, :, bottom if part else top]
        await_bytes(ref, ag_ring.at[0 if step == 1 else 1, part])
        remote(ref, ref, own_sem.at[12], ag_ring.at[2, 0], along_x(step))
    gu.event(6)
    gu.wait_pair(0)
    gu.wait_pair(1)
    for tile in range(11):
        ACC[tile] = product(x, early, tile)
    gu.event(7)
    for part, step, chip in ((1, 1, left), (0, 3, right)):
        await_bytes(ST.at[chip, :, bottom if part else top], ag_ring.at[0 if step == 1 else 1, part])
    for tile in range(11):
        ACC[tile] = ACC[tile] + product(left, early, tile) + product(right, early, tile)
    dw.event(2)
    gu.wait_pair(2)
    gather_in(range(6))
    dw.event(3)
    gather_in(range(6, 11))
    await_bytes(SQC.at[pl.ds(0, 3)], sem.at[4])
    SC[...] = row_factors(SQC, 4)
    await_bytes(ST.at[across], ag_ring.at[2, 0])
    hidden(range(6))
    dw.event(4)
    hidden(range(6, 11))
    def columns(p, chip, slot):
        return jnp.dot(H[p], DW[p, 4 * chip + slot], preferred_element_type=F32)

    def down_of(p, chip, h):
        weights = jnp.concatenate([DW[p, 4 * chip + 2 * h], DW[p, 4 * chip + 2 * h + 1]], axis=1)
        return jnp.dot(H[p], weights, preferred_element_type=F32)

    def down(chip, h):
        return down_of(c, chip, h) + down_of(1 - c, chip, h)

    def send_sum(src, dst, semaphore, device):
        remote(src, dst, own_sem.at[16], semaphore, device)

    odd = lax.rem(y, 2)
    blocks = ((y, odd), (y + 1 - 2 * odd, 1 - odd))
    near = ((right, bottom, top), (left, top, bottom))

    def block_own(q):
        PRE[q] = columns(c, across, blocks[q][0])

    def block_across(q):
        slot, j = blocks[q]
        PB[0, 0, j] = (PRE[q] + columns(1 - c, across, slot)).astype(BF16)
        for m, (rows, step) in enumerate(((top, 1), (bottom, 3))):
            send_sum(PB.at[0, 0, j, rows], RA.at[0, m, j], ra_recv.at[q, m], along_x(step))

    def block_near(q):
        slot, j = blocks[q]
        for m, (chip, rows, _) in enumerate(near):
            total = columns(c, chip, slot) + columns(1 - c, chip, slot)
            PB[0, 1 + m, j] = total.astype(BF16)
            FO[q, m] = total[:QUARTER] if m == 0 else total[QUARTER:]
            send_sum(PB.at[0, 1 + m, j, rows], RC.at[m, c, j, rows], rc_recv.at[0], (s, 2 * chip + early))

    def block_relay(q):
        j = blocks[q][1]
        for m, (chip, _, rows) in enumerate(near):
            await_bytes(RA.at[0, m, j], ra_recv.at[q, m])
            PB[0, 1 + m, j, rows] = (FO[q, m] + RA[0, m, j].astype(F32)).astype(BF16)
            send_sum(PB.at[0, 1 + m, j, rows], RC.at[m, c, j, rows], rc_recv.at[1], (s, 2 * chip + early))

    late = 1 - early

    def late_own():
        for m, chip in enumerate((across, right, left)):
            LPRE[m] = down_of(c, chip, late)

    def late_total(m, chip):
        return LPRE[m] + down_of(1 - c, chip, late)

    def late_across():
        total = late_total(0, across)
        for j in (0, 1):
            PB[1, 0, j] = total[:, 128 * j : 128 * j + 128].astype(BF16)
        for m, (rows, step) in enumerate(((top, 1), (bottom, 3))):
            send_sum(PB.at[1, 0, :, rows], RA.at[1, m], ra_recv.at[2, m], along_x(step))

    def late_near():
        for m, (chip, rows, _) in enumerate(near):
            total = late_total(1 + m, chip)
            FL[m] = total[:QUARTER] if m == 0 else total[QUARTER:]
            for j in (0, 1):
                PB[1, 1 + m, j] = total[:, 128 * j : 128 * j + 128].astype(BF16)
            send_sum(PB.at[1, 1 + m, :, rows], RC.at[m, c, :, rows], rc_recv.at[0], (s, 2 * chip + late))

    def late_relay():
        for m, (chip, _, rows) in enumerate(near):
            await_bytes(RA.at[1, m], ra_recv.at[2, m])
            for j in (0, 1):
                total = FL[m, :, 128 * j : 128 * j + 128] + RA[1, m, j].astype(F32)
                PB[1, 1 + m, j, rows] = total.astype(BF16)
            send_sum(PB.at[1, 1 + m, :, rows], RC.at[m, c, :, rows], rc_recv.at[1], (s, 2 * chip + late))

    block_own(0)
    dw.event(5)
    dw.wait_pair(0)
    block_across(0)
    block_near(0)
    block_own(1)
    dw.wait_pair(1)
    block_across(1)
    dw.event(6)
    block_near(1)
    block_relay(0)
    dw.event(7)
    late_own()
    dw.wait_pair(2)
    late_across()
    block_relay(1)
    late_near()
    PS[...] = down(x, 1 - c).astype(BF16)
    remote(PS, PO.at[c], own_sem.at[17], sem.at[8], partner)
    late_relay()
    PO[c] = down(x, c).astype(BF16)
    await_bytes(PO.at[1 - c], sem.at[8])
    def came(m, k, rows):
        return jnp.concatenate([RC[m, k, 0, rows], RC[m, k, 1, rows]], axis=1)

    head, rest = slice(0, QUARTER), slice(QUARTER, HALF)
    await_bytes(RC.at[0], rc_recv.at[0])
    for k in (0, 1):
        FF[k, head] = PO[k, head].astype(F32) + came(1, k, head).astype(F32)
        FF[k, rest] = PO[k, rest].astype(F32) + came(0, k, rest).astype(F32)
    await_bytes(RC.at[0], rc_recv.at[1])
    sums = []
    for k in (0, 1):
        last = jnp.concatenate([came(0, k, head), came(1, k, rest)], axis=0)
        total = (FF[k] + last.astype(F32)).astype(BF16).astype(F32)
        FF[k] = total
        square = jnp.sum(total * total, axis=1, keepdims=True)
        sums.append(as_row(square))

    SQB[t] = jnp.concatenate(sums, axis=1)
    for k in range(1, 8):
        remote(SQB.at[t], SQB.at[t], own_sem.at[18], sem.at[7], (s, lax.rem(t + k, 8)))
    await_bytes(XR, sem.at[6])
    await_bytes(SQB.at[pl.ds(0, 7)], sem.at[7])
    factors = row_factors(SQB, 8)
    for k in (0, 1):
        factor = factors[HALF * k : HALF * k + HALF]
        FF[k] = FF[k] * jnp.concatenate([factor, factor], axis=1) * ffng_ref[...]
    out_ref[c] = (SO[c].astype(F32) + FF[c]).astype(BF16)
    out_ref[1 - c] = (XR[...].astype(F32) + FF[1 - c]).astype(BF16)

    gu.finish()
    dw.finish()
    await_bytes(HX, own_sem.at[0])
    await_bytes(HI, own_sem.at[1])
    await_bytes(CB, own_sem.at[7])
    await_bytes(BA.at[pl.ds(0, 3)], own_sem.at[8])
    await_bytes(OW.at[c], own_sem.at[4])
    await_bytes(RP.at[c], own_sem.at[5])
    await_bytes(GP.at[c], own_sem.at[6])
    await_bytes(BH.at[0], own_sem.at[9])
    await_bytes(SQA.at[pl.ds(0, 3)], own_sem.at[10])
    await_bytes(SQC.at[pl.ds(0, 3)], own_sem.at[11])
    await_bytes(XR, own_sem.at[13])
    await_bytes(ST.at[pl.ds(0, 3)], own_sem.at[12])
    await_bytes(PB, own_sem.at[16])
    await_bytes(PS, own_sem.at[17])
    await_bytes(SQB.at[pl.ds(0, 7)], own_sem.at[18])


def body(
    gate_branch, recur_input, doc_ids, conv_taps, gate_map, input_map, decay_level, decay_extra, out_weight,
    residual, mix_gain, pre_gain, ffn_gain, gate_weight, up_weight, down_weight,
):
    vmem = pl.BlockSpec(memory_space=pltpu.VMEM)
    dma = pltpu.SemaphoreType.DMA
    out = pl.pallas_call(
        layer_kernel,
        name="layer",
        out_shape=pltpu.VMEM((2, HALF, 256), BF16),
        in_specs=[pl.BlockSpec(memory_space=pl.ANY)] * 16,
        out_specs=vmem,
        scratch_shapes=[
            pltpu.VMEM((TOK, CH), BF16),
            pltpu.VMEM((TOK, CH), BF16),
            pltpu.VMEM((6, 128), jnp.int32),
            pltpu.VMEM((4, CH), BF16),
            pltpu.VMEM((2, 64, 64), BF16),
            pltpu.VMEM((2, 64, 64), BF16),
            pltpu.VMEM((1, CH), F32),
            pltpu.VMEM((TOK, CH), F32),
            pltpu.VMEM((2, HALF, 256), BF16),
            pltpu.VMEM((1, 256), F32),
            pltpu.VMEM((1, 256), F32),
            pltpu.VMEM((1, 256), F32),
            pltpu.VMEM((HID, 128), BF16),
            pltpu.VMEM((HID, 128), BF16),
            pltpu.VMEM((2, 16, 128, 1408), BF16),
            pltpu.VMEM((2, 16, HID, 128), BF16),
            pltpu.VMEM((2, 1024, 256), BF16),
            pltpu.VMEM((2, HALF, 256), BF16),
            pltpu.VMEM((2, 8, 256), F32),
            pltpu.VMEM((2, HALF, CH), BF16),
            pltpu.VMEM((4, 2, HALF, CH), BF16),
            pltpu.VMEM((16, CH), BF16),
            pltpu.VMEM((6, 128), jnp.int32),
            pltpu.VMEM((TOK + 8, CH), F32),
            pltpu.VMEM((TOK + 8, CH), F32),
            pltpu.VMEM((TOK, CH), F32),
            pltpu.VMEM((TOK, CH), F32),
            pltpu.VMEM((TOK, CH), F32),
            pltpu.VMEM((TOK, CH), F32),
            pltpu.VMEM((TOK, CH), F32),
            pltpu.VMEM((8, CH), F32),
            pltpu.VMEM((REACH, 8, CH), F32),
            pltpu.VMEM((2, HALF, 256), F32),
            pltpu.VMEM((4, 1, HALF), F32),
            pltpu.VMEM((2, HALF, 256), BF16),
            pltpu.VMEM((HALF, 256), BF16),
            pltpu.VMEM((4, 2, HALF, 256), BF16),
            pltpu.VMEM((4, 1, HALF), F32),
            pltpu.VMEM((HALF, 128), F32),
            pltpu.VMEM((11, HALF, 256), F32),
            pltpu.VMEM((2, HALF, HID), BF16),
            pltpu.VMEM((2, 3, 2, HALF, 128), BF16),
            pltpu.VMEM((HALF, 256), BF16),
            pltpu.VMEM((2, 2, 2, HALF // 2, 128), BF16),
            pltpu.VMEM((2, 2, 2, HALF, 128), BF16),
            pltpu.VMEM((2, HALF, 256), BF16),
            pltpu.VMEM((2, 2, HALF // 2, 128), F32),
            pltpu.VMEM((2, HALF // 2, 256), F32),
            pltpu.VMEM((2, HALF, 256), F32),
            pltpu.VMEM((2, HALF, 128), F32),
            pltpu.VMEM((3, HALF, 256), F32),
            pltpu.VMEM((8, 1, TOK), F32),
            dma((len(GROUPS),)),
            dma((len(GROUPS),)),
            dma((3,)),
            dma((3,)),
            dma((3, 2)),
            dma((3, 2)),
            dma((3, 2)),
            dma((2,)),
            dma((19,)),
            dma((12,)),
        ],
        compiler_params=pltpu.CompilerParams(
            collective_id=0, has_side_effects=True, vmem_limit_bytes=60 * 1024 * 1024
        ),
    )(
        gate_branch,
        recur_input,
        doc_ids.reshape(6, 128),
        conv_taps,
        gate_map,
        input_map,
        decay_level.reshape(1, CH),
        decay_extra,
        out_weight,
        residual.reshape(2, HALF, 256),
        mix_gain.reshape(1, 256),
        pre_gain.reshape(1, 256),
        ffn_gain.reshape(1, 256),
        gate_weight.T,
        up_weight.T,
        down_weight,
    )
    return out.reshape(TOK, 256)


def solution(mesh):
    return jax.shard_map(
        body,
        mesh=mesh,
        in_specs=(
            P("sp", "tp"),
            P("sp", "tp"),
            P("sp"),
            P(None, "tp"),
            P("tp", None, None),
            P("tp", None, None),
            P("tp"),
            P("sp", "tp"),
            P(None, "tp"),
            P("sp", "tp"),
            P("tp"),
            P("tp"),
            P("tp"),
            P("sp", "tp"),
            P("sp", "tp"),
            P("tp", "sp"),
        ),
        out_specs=P("sp", "tp"),
        check_vma=False,
    )
```

```python
import jax
import jax.numpy as jnp
from jax import lax
from jax.experimental import pallas as pl
from jax.experimental.pallas import tpu as pltpu
from jax.sharding import PartitionSpec as P

MESH = pl.DeviceIdType.MESH
F32 = jnp.float32
BF16 = jnp.bfloat16

D = 2048
EPS = 1e-06
GATE_POWER = 8.0
TOK = 768
BLK = 96
HALF = 384
CH = 128
HID = 704
REACH = 6


def neg_expm1(u):
    series = 1.0 + u * (1.0 / 9.0)
    for n in (8.0, 7.0, 6.0, 5.0, 4.0, 3.0, 2.0):
        series = 1.0 + u * (1.0 / n) * series
    return jnp.where(u > -0.5, -u * series, 1.0 - jnp.exp(u))


def softplus(v):
    tail = jnp.exp(-jnp.abs(v))
    w = tail / (2.0 + tail)
    square = w * w
    series = jnp.full_like(w, 1.0 / 15.0)
    for n in (13.0, 11.0, 9.0, 7.0, 5.0, 3.0, 1.0):
        series = 1.0 / n + square * series
    return jnp.maximum(v, 0.0) + 2.0 * w * series


TOGETHER = (
    ((0, 0, 3), (0, 0, 1)),
    ((1, 3, 0), (1, 1, 0)),
    ((0, 1, 0), (1, 0, 1)),
    ((0, 3, "m"), (1, 3, 3)),
    ((1, 1, 1), (0, 2, 0)),
    ((1, 2, 3), (0, 2, "m")),
    ((0, 3, "o"), (0, 2, "o"), (1, 0, 2), (1, 3, 2)),
    ((0, 1, 2), (0, 2, 2), (1, 1, 2), (1, 2, 2)),
)
ALONE = (
    (0, 0, 2), (1, 2, 0), (0, 3, 0), (0, 1, "m"), (0, 1, "o"), (0, 3, 2),
    (1, 0, 3), (1, 3, 1), (1, 1, 3), (1, 2, 1),
)
GROUPS = (*TOGETHER, *((one,) for one in ALONE))


class TorusGather:
    def __init__(self, buf, rows, here, ring_send, ring_recv, pair_send, pair_recv):
        self.buf, self.rows = buf, rows
        self.z, self.y, self.c, self.t = here
        self.ring_send, self.ring_recv = ring_send, ring_recv
        self.pair_send, self.pair_recv = pair_send, pair_recv
        self.odd = lax.rem(self.y, 2)
        self.mate, self.other = 1 + 2 * self.odd, 3 - 2 * self.odd

    def slot(self, dz, dy):
        return lax.rem(self.z + dz, 4) * 4 + lax.rem(self.y + dy, 4)

    def at(self, half, a, b):
        return (a, b) if half == 0 else (b, a)

    def span(self, half, part):
        quarter = self.rows // 4
        first = half * 2 * quarter
        return (first, 2 * quarter) if part is None else (first + part * quarter, quarter)

    def piece(self, half, where, part=None):
        first, count = self.span(half, part)
        return self.buf.at[self.c, self.slot(*where), pl.ds(first, count)]

    def named(self, dy):
        return dy if isinstance(dy, int) else "m" if dy is self.mate else "o"

    def group(self, half, where):
        key = (half, where[0], self.named(where[1]))
        return next(n for n, keys in enumerate(GROUPS) if key in keys)

    def send(self, half, where, to, part=None):
        ref = self.piece(half, where, part)
        dz, dy = (where[0] - to[0]) % 4, where[1]
        if isinstance(dy, int):
            dy = (dy - to[1]) % 4
        pltpu.make_async_remote_copy(
            src_ref=ref,
            dst_ref=ref,
            send_sem=self.ring_send,
            recv_sem=self.ring_recv.at[self.group(half, (dz, dy))],
            device_id=(self.slot(*to), self.t),
            device_id_type=MESH,
        ).start()

    def wait(self, *pieces):
        number = self.group(*pieces[0])
        assert len(pieces) == len(GROUPS[number])
        assert all(self.group(*piece) == number for piece in pieces)
        ref = self.piece(*pieces[0])
        if len(pieces) > 1:
            ref = self.buf.at[self.c, pl.ds(0, len(pieces) // 2)]
        pltpu.make_async_copy(ref, ref, self.ring_recv.at[number]).wait()
        for half, where in pieces:
            self.pass_over(self.piece(half, where), where)

    def pass_over(self, ref, where):
        dy = where[1]
        if isinstance(dy, int):
            stage = {0: 0, 1: 1 + self.odd, 2: 2, 3: 2 - self.odd}[dy]
        else:
            stage = 1 if dy is self.mate else 2
        pltpu.make_async_remote_copy(
            src_ref=ref,
            dst_ref=ref,
            send_sem=self.pair_send,
            recv_sem=self.pair_recv.at[stage],
            device_id=(self.slot(0, 0), self.t + 1 - 2 * self.c),
            device_id_type=MESH,
        ).start()

    def start(self):
        for half in (0, 1):
            for step in (1, 3):
                self.send(half, (0, 0), self.at(half, 0, step))

    def start_second(self):
        for half in (0, 1):
            for step in (1, 3):
                self.send(half, (0, 0), self.at(half, step, 0))
        self.pass_over(self.buf.at[self.c, self.slot(0, 0)], (0, 0))

    def spread(self, half, b, steps=(1, 3)):
        for step in steps:
            self.send(half, self.at(half, 0, b), self.at(half, step, 0))

    def relay(self, half, a, b):
        self.wait((half, self.at(half, a, b)))
        self.send(half, self.at(half, a, b), self.at(half, 4 - a, 0))

    def event(self, number):
        at, wait = self.at, self.wait
        mate, other = self.mate, self.other
        if number == 1:
            for half in (0, 1):
                wait((half, at(half, 0, 3)), (half, at(half, 0, 1)))
                self.send(half, at(half, 0, 3), at(half, 0, 1), part=0)
                self.send(half, at(half, 0, 1), at(half, 0, 3), part=1)
            self.spread(0, mate)
            self.spread(0, other, (3,))
            self.spread(1, 3)
            self.spread(1, 1)
        if number == 2:
            self.relay(0, 3, 0)
            wait((1, at(1, 0, 2)))
            self.spread(1, 2)
            wait((0, at(0, 0, 2)))
            self.spread(0, 2, (1,))
            self.spread(0, other, (1,))
            self.relay(1, 3, 0)
            wait((0, at(0, 1, 0)), (1, at(1, 1, 0)))
        if number == 3:
            self.relay(0, 1, mate)
            self.relay(1, 1, 3)
            wait((0, at(0, 3, mate)), (1, at(1, 3, 3)))
        if number == 4:
            self.relay(0, 1, other)
            self.spread(0, 2, (3,))
            self.relay(1, 3, 1)
            wait((1, at(1, 1, 1)), (0, at(0, 2, 0)))
        if number == 5:
            self.relay(1, 1, 2)
            wait((1, at(1, 3, 2)), (0, at(0, 2, mate)))
            self.relay(0, 3, 2)
        if number == 6:
            wait((0, at(0, 3, other)), (0, at(0, 2, other)), (1, at(1, 2, 0)), (1, at(1, 2, 3)))
        if number == 7:
            wait((0, at(0, 1, 2)), (0, at(0, 2, 2)), (1, at(1, 2, 1)), (1, at(1, 2, 2)))

    def wait_pair(self, stage):
        ref = self.buf.at[1 - self.c, pl.ds(0, (4, 4, 8)[stage])]
        pltpu.make_async_copy(ref, ref, self.pair_recv.at[stage]).wait()

    def finish(self):
        ref = self.buf.at[self.c, pl.ds(0, 15)]
        pltpu.make_async_copy(ref, ref, self.ring_send).wait()
        ref = self.buf.at[self.c]
        pltpu.make_async_copy(ref, ref, self.pair_send).wait()


def layer_kernel(
    gate_hbm, rec_hbm, ids_hbm, taps_hbm, gmap_hbm, imap_hbm, level_hbm, extra_hbm, ow_hbm, res_hbm,
    mixg_hbm, preg_hbm, ffng_hbm, gw_hbm, uw_hbm, dw_hbm,
    out_ref,
    gate_ref, rec_ref, ids_ref, taps_ref, gmap_ref, imap_ref, level_ref, extra_ref, res_ref,
    mixg_ref, preg_ref, ffng_ref, gw_ref, uw_ref,
    GU, DW, OW, RP, GP, BH, BA, HX, HI, XF, IDF, FA, DV, S, PR, GL, CS, CB, MX, SQA, SO, XR, ST, SQC, SC, ACC, H,
    PB, PS, RA, RC, PO, FO, FL, FF, PRE, LPRE, SQB,
    gu_ring, dw_ring, gu_pair, dw_pair, ba_ring, ag_ring, ra_recv, rc_recv, own_sem, sem,
):
    s, t = lax.axis_index("sp"), lax.axis_index("tp")
    z, y = lax.div(s, 4), lax.rem(s, 4)
    x, c = lax.div(t, 2), lax.rem(t, 2)

    def remote(src, dst, send_sem, recv_sem, device):
        copy = pltpu.make_async_remote_copy(
            src_ref=src, dst_ref=dst, send_sem=send_sem, recv_sem=recv_sem, device_id=device, device_id_type=MESH
        )
        copy.start()

    def await_bytes(ref, semaphore):
        pltpu.make_async_copy(ref, ref, semaphore).wait()

    def along_x(step):
        return (s, lax.rem(x + step, 4) * 2 + c)

    partner = (s, t + 1 - 2 * c)
    here = (z, y, c, t)
    gu = TorusGather(GU, 128, here, own_sem.at[2], gu_ring, own_sem.at[3], gu_pair)
    dw = TorusGather(DW, HID, here, own_sem.at[14], dw_ring, own_sem.at[15], dw_pair)

    barrier = pltpu.get_barrier_semaphore()
    for k in range(1, REACH + 1):
        for peer in (lax.rem(s + k, 16), lax.rem(s + 16 - k, 16)):
            pl.semaphore_signal(barrier, inc=1, device_id=(peer, t), device_id_type=MESH)
    for k in range(1, 8):
        pl.semaphore_signal(barrier, inc=1, device_id=(s, lax.rem(t + k, 8)), device_id_type=MESH)

    own = z * 4 + y
    loads = []
    for src, dst in (
        (gw_hbm, gw_ref), (uw_hbm, uw_ref), (rec_hbm, rec_ref), (ids_hbm, ids_ref), (gate_hbm, gate_ref),
        (taps_hbm, taps_ref), (gmap_hbm, gmap_ref), (imap_hbm, imap_ref), (level_hbm, level_ref),
        (extra_hbm, extra_ref), (mixg_hbm, mixg_ref), (preg_hbm, preg_ref), (ffng_hbm, ffng_ref), (ow_hbm, OW.at[c]),
        (res_hbm, res_ref), (dw_hbm, DW.at[c, own]),
    ):
        loads.append(pltpu.make_async_copy(src, dst, own_sem.at[len(loads)]))
        loads[-1].start()

    loads[0].wait()
    loads[1].wait()
    for i in range(5):
        for n, ref in enumerate((gw_ref, uw_ref)):
            block = ref[128 * i : 128 * i + 128].astype(F32).T.astype(BF16)
            GU[c, own, :, 256 * i + 128 * n : 256 * i + 128 * n + 128] = block
    block = jnp.concatenate([gw_ref[640:704].astype(F32), uw_ref[640:704].astype(F32)], axis=0)
    GU[c, own, :, 1280:1408] = block.T.astype(BF16)
    for load in loads[2:4]:
        load.wait()
    IDF[8:] = jnp.concatenate(
        [jnp.broadcast_to(ids_ref[r : r + 1, :].astype(F32), (128, 128)).T for r in range(6)], axis=0
    )
    XF[8:] = rec_ref[...].astype(F32)

    pl.semaphore_wait(barrier, 2 * REACH + 7)

    after = (lax.rem(s + 1, 16), t)
    remote(rec_ref.at[pl.ds(TOK - 16, 16)], HX, own_sem.at[0], sem.at[0], after)
    remote(ids_ref, HI, own_sem.at[1], sem.at[1], after)
    gu.start()
    for load in loads[4:]:
        load.wait()

    RP[c] = res_ref[c]
    GP[c, 0:1] = mixg_ref[...]
    GP[c, 1:2] = preg_ref[...]
    remote(OW.at[c], OW.at[c], own_sem.at[4], sem.at[9], partner)
    remote(res_ref.at[1 - c], RP.at[c], own_sem.at[5], sem.at[10], partner)
    remote(GP.at[c], GP.at[c], own_sem.at[6], sem.at[11], partner)

    for r in range(6):
        rows = slice(128 * r, 128 * r + 128)
        GL[rows] = jax.nn.gelu(gate_ref[rows].astype(F32), approximate=True)
    pair = [
        jnp.concatenate(
            [
                jnp.concatenate([m[0].astype(F32), jnp.zeros((64, 64), F32)], axis=1),
                jnp.concatenate([jnp.zeros((64, 64), F32), m[1].astype(F32)], axis=1),
            ],
            axis=0,
        )
        for m in (gmap_ref, imap_ref)
    ]
    maps = jnp.concatenate(pair, axis=1).astype(BF16)
    rate = -GATE_POWER * softplus(-level_ref[...])
    taps = taps_ref[...].astype(F32)

    def drive(r):
        at = 8 + 128 * r
        ids = IDF[at : at + 128]
        conv = XF[at : at + 128] * taps[0:1]
        for k in (1, 2, 3):
            same = IDF[at - k : at - k + 128] == ids
            conv = conv + jnp.where(same, XF[at - k : at - k + 128], 0.0) * taps[k : k + 1]
        conv = conv.astype(BF16)
        gates = jax.nn.sigmoid(jnp.dot(conv, maps, preferred_element_type=F32))
        rows = slice(128 * r, 128 * r + 128)
        log_decay = rate * gates[:, :CH] + extra_ref[rows]
        FA[rows] = jnp.where(IDF[at - 1 : at + 127] == ids, jnp.exp(log_decay), 0.0)
        DV[rows] = jnp.sqrt(neg_expm1(2.0 * log_decay)) * gates[:, CH:] * conv.astype(F32)

    for r in range(1, 6):
        drive(r)
    await_bytes(HX, sem.at[0])
    await_bytes(HI, sem.at[1])
    XF[0:8] = HX[...].astype(F32)[8:16]
    rim_ids = jnp.broadcast_to(HI[5:6, :].astype(F32), (128, 128)).T[120:128]
    IDF[0:8] = jnp.where(s > 0, rim_ids, -1.0)

    drive(0)

    state = jnp.zeros((8, CH), F32)
    prod = jnp.ones((8, CH), F32)
    for i in range(BLK):
        at = pl.ds(i, 8, stride=BLK)
        f = FA[at, :]
        state = f * state + DV[at, :]
        prod = f * prod
        S[at, :] = state
        PR[at, :] = prod
    befores = []
    p_all, e_all = jnp.ones((1, CH), F32), jnp.zeros((1, CH), F32)
    for b in range(8):
        befores.append((p_all, e_all))
        e_all = prod[b : b + 1] * e_all + state[b : b + 1]
        p_all = prod[b : b + 1] * p_all
    CS[...] = jnp.concatenate([p_all, e_all, jnp.zeros((6, CH), F32)], axis=0)
    for k in range(1, REACH + 1):
        remote(CS, CB.at[k - 1], own_sem.at[7], sem.at[2], (lax.rem(s + k, 16), t))
    gu.start_second()
    gu.event(1)

    await_bytes(CB, sem.at[2])
    entering = jnp.zeros((1, CH), F32)
    for k in range(REACH, 0, -1):
        entering = jnp.where(s >= k, CB[k - 1, 0:1] * entering + CB[k - 1, 1:2], 0.0)
    for b in range(8):
        rows = slice(BLK * b, BLK * b + BLK)
        p_before, e_before = befores[b]
        states = S[rows] + PR[rows] * (e_before + p_before * entering)
        half, first = b // 4, BLK * (b % 4)
        BH[half, first : first + BLK] = (states * GL[rows]).astype(BF16)

    QUARTER = HALF // 2
    top, bottom = pl.ds(0, QUARTER), pl.ds(QUARTER, QUARTER)
    left, right, across = lax.rem(x + 3, 4), lax.rem(x + 1, 4), lax.rem(x + 2, 4)
    for part, step in ((0, 1), (1, 3), (1, 1), (0, 3)):
        rows = bottom if part else top
        for k in (0, 1):
            remote(
                BH.at[k, rows], BA.at[x, c, rows], own_sem.at[8], ba_ring.at[0 if step == 1 else 1, part],
                (s, lax.rem(x + step, 4) * 2 + k),
            )
    remote(BH.at[1 - c], BA.at[x, c], own_sem.at[9], sem.at[5], partner)
    BA[x, c] = BH[c]
    for part, step, chip in ((0, 1, left), (1, 3, right)):
        rows = bottom if part else top
        ref = BA.at[chip, :, rows]
        await_bytes(ref, ba_ring.at[0 if step == 1 else 1, part])
        remote(ref, ref, own_sem.at[8], ba_ring.at[2, 0], along_x(step))
    gu.event(2)
    for part, step, chip in ((1, 1, left), (0, 3, right)):
        rows = bottom if part else top
        await_bytes(BA.at[chip, :, rows], ba_ring.at[0 if step == 1 else 1, part])
    await_bytes(BA.at[x, 1 - c], sem.at[5])
    await_bytes(OW.at[1 - c], sem.at[9])
    await_bytes(RP.at[1 - c], sem.at[10])
    await_bytes(GP.at[1 - c], sem.at[11])
    gu.event(3)
    await_bytes(BA.at[across], ba_ring.at[2, 0])

    def as_row(square):
        return jnp.broadcast_to(square, (HALF, 128)).T[0:1]

    def chip_sums(ref, send_sem, recv_sem):
        for step in (1, 2, 3):
            remote(ref.at[x], ref.at[x], send_sem, recv_sem, along_x(step))

    def row_factors(ref, count):
        total = ref[0]
        for j in range(1, count):
            total = total + ref[j]
        return jnp.broadcast_to(lax.rsqrt(total * (1.0 / D) + EPS), (128, total.shape[1])).T

    branch = jnp.concatenate([BA[j // 2, j % 2] for j in range(8)], axis=1)
    square = jnp.zeros((HALF, 1), F32)
    for h in (0, 1):
        mixed = jnp.dot(branch, OW[h], preferred_element_type=F32).astype(BF16).astype(F32)
        MX[h] = mixed
        square = square + jnp.sum(mixed * mixed, axis=1, keepdims=True)
    SQA[x] = as_row(square)
    chip_sums(SQA, own_sem.at[10], sem.at[3])
    dw.start()
    gu.event(4)
    await_bytes(SQA.at[pl.ds(0, 3)], sem.at[3])
    factor = row_factors(SQA, 4)
    factor = jnp.concatenate([factor, factor], axis=1)
    square = jnp.zeros((HALF, 1), F32)
    for h in (0, 1):
        stream = (RP[h].astype(F32) + MX[h] * factor * GP[h, 0:1]).astype(BF16)
        SO[h] = stream
        stream = stream.astype(F32)
        ST[x, h] = (stream * GP[h, 1:2]).astype(BF16)
        square = square + jnp.sum(stream * stream, axis=1, keepdims=True)
    SQC[x] = as_row(square)
    chip_sums(SQC, own_sem.at[11], sem.at[4])

    for part, step in ((0, 1), (1, 3), (1, 1), (0, 3)):
        ref = ST.at[x, :, bottom if part else top]
        remote(ref, ref, own_sem.at[12], ag_ring.at[0 if step == 1 else 1, part], along_x(step))
    remote(SO.at[1 - c], XR, own_sem.at[13], sem.at[6], partner)
    gu.event(5)
    dw.start_second()

    early = lax.div(y, 2)

    def product(q, h, tile):
        rows = pl.ds(4 * q + 2 * h, 2)
        if tile < 10:
            p, i = tile // 5, tile % 5
            weights = GU[p, rows, :, 256 * i : 256 * i + 256].reshape(256, 256)
        else:
            weights = jnp.concatenate([GU[p, rows, :, 1280:1408].reshape(256, 128) for p in (0, 1)], axis=1)
        return jnp.dot(ST[q, h], weights, preferred_element_type=F32)

    def gather_in(tiles):
        for tile in tiles:
            total = ACC[tile]
            for q in (x, left, right):
                total = total + product(q, 1 - early, tile)
            ACC[tile] = total

    def hidden(tiles):
        factor = SC[...]
        for tile in tiles:
            both = ACC[tile] + product(across, early, tile) + product(across, 1 - early, tile)
            if tile < 10:
                p, i = tile // 5, tile % 5
                act = jax.nn.silu(both[:, :128] * factor) * (both[:, 128:] * factor)
                H[p, :, 128 * i : 128 * i + 128] = act.astype(BF16)
            else:
                for p in (0, 1):
                    tail = both[:, 128 * p : 128 * p + 128] * factor
                    H[p, :, 640:704] = (jax.nn.silu(tail[:, :64]) * tail[:, 64:]).astype(BF16)

    dw.event(1)
    for part, step, chip in ((0, 1, left), (1, 3, right)):
        ref = ST.at[chip, :, bottom if part else top]
        await_bytes(ref, ag_ring.at[0 if step == 1 else 1, part])
        remote(ref, ref, own_sem.at[12], ag_ring.at[2, 0], along_x(step))
    gu.event(6)
    gu.wait_pair(0)
    gu.wait_pair(1)
    for tile in range(11):
        ACC[tile] = product(x, early, tile)
    gu.event(7)
    for part, step, chip in ((1, 1, left), (0, 3, right)):
        await_bytes(ST.at[chip, :, bottom if part else top], ag_ring.at[0 if step == 1 else 1, part])
    for tile in range(11):
        ACC[tile] = ACC[tile] + product(left, early, tile) + product(right, early, tile)
    dw.event(2)
    gu.wait_pair(2)
    gather_in(range(6))
    dw.event(3)
    gather_in(range(6, 11))
    await_bytes(SQC.at[pl.ds(0, 3)], sem.at[4])
    SC[...] = row_factors(SQC, 4)
    await_bytes(ST.at[across], ag_ring.at[2, 0])
    hidden(range(6))
    dw.event(4)
    hidden(range(6, 11))
    def columns(p, *slots):
        weights = jnp.concatenate([DW[p, slot] for slot in slots], axis=1)
        return jnp.dot(H[p], weights, preferred_element_type=F32)

    def down_of(p, chip, h):
        weights = jnp.concatenate([DW[p, 4 * chip + 2 * h], DW[p, 4 * chip + 2 * h + 1]], axis=1)
        return jnp.dot(H[p], weights, preferred_element_type=F32)

    def down(chip, h):
        return down_of(c, chip, h) + down_of(1 - c, chip, h)

    def send_sum(src, dst, semaphore, device):
        remote(src, dst, own_sem.at[16], semaphore, device)

    odd = lax.rem(y, 2)
    blocks = ((y, odd), (y + 1 - 2 * odd, 1 - odd))
    near = ((right, bottom, top), (left, top, bottom))

    def block_own(q):
        PRE[q] = columns(c, 4 * across + blocks[q][0])

    def block_across(q):
        slot, j = blocks[q]
        PB[0, 0, j] = (PRE[q] + columns(1 - c, 4 * across + slot)).astype(BF16)
        for m, (rows, step) in enumerate(((top, 1), (bottom, 3))):
            send_sum(PB.at[0, 0, j, rows], RA.at[0, m, j], ra_recv.at[q, m], along_x(step))

    def block_near(q):
        slot, j = blocks[q]
        slots = (4 * right + slot, 4 * left + slot)
        both = columns(c, *slots) + columns(1 - c, *slots)
        for m, (chip, rows, _) in enumerate(near):
            total = both[:, 128 * m : 128 * m + 128]
            PB[0, 1 + m, j] = total.astype(BF16)
            FO[q, m] = total[:QUARTER] if m == 0 else total[QUARTER:]
            send_sum(PB.at[0, 1 + m, j, rows], RC.at[m, c, j, rows], rc_recv.at[0], (s, 2 * chip + early))

    def block_relay(q):
        j = blocks[q][1]
        for m, (chip, _, rows) in enumerate(near):
            await_bytes(RA.at[0, m, j], ra_recv.at[q, m])
            PB[0, 1 + m, j, rows] = (FO[q, m] + RA[0, m, j].astype(F32)).astype(BF16)
            send_sum(PB.at[0, 1 + m, j, rows], RC.at[m, c, j, rows], rc_recv.at[1], (s, 2 * chip + early))

    late = 1 - early

    def late_own():
        LPRE[0] = down_of(c, across, late)
        both = columns(c, *near_slots)
        LPRE[1] = both[:, :256]
        LPRE[2] = both[:, 256:]

    near_slots = [4 * chip + 2 * late + j for chip in (right, left) for j in (0, 1)]

    def late_across():
        total = LPRE[0] + down_of(1 - c, across, late)
        for j in (0, 1):
            PB[1, 0, j] = total[:, 128 * j : 128 * j + 128].astype(BF16)
        for m, (rows, step) in enumerate(((top, 1), (bottom, 3))):
            send_sum(PB.at[1, 0, :, rows], RA.at[1, m], ra_recv.at[2, m], along_x(step))

    def late_near():
        both = columns(1 - c, *near_slots)
        for m, (chip, rows, _) in enumerate(near):
            total = LPRE[1 + m] + both[:, 256 * m : 256 * m + 256]
            FL[m] = total[:QUARTER] if m == 0 else total[QUARTER:]
            for j in (0, 1):
                PB[1, 1 + m, j] = total[:, 128 * j : 128 * j + 128].astype(BF16)
            send_sum(PB.at[1, 1 + m, :, rows], RC.at[m, c, :, rows], rc_recv.at[0], (s, 2 * chip + late))

    def late_relay():
        for m, (chip, _, rows) in enumerate(near):
            await_bytes(RA.at[1, m], ra_recv.at[2, m])
            for j in (0, 1):
                total = FL[m, :, 128 * j : 128 * j + 128] + RA[1, m, j].astype(F32)
                PB[1, 1 + m, j, rows] = total.astype(BF16)
            send_sum(PB.at[1, 1 + m, :, rows], RC.at[m, c, :, rows], rc_recv.at[1], (s, 2 * chip + late))

    block_own(0)
    dw.event(5)
    dw.wait_pair(0)
    block_across(0)
    block_near(0)
    block_own(1)
    dw.wait_pair(1)
    block_across(1)
    dw.event(6)
    block_near(1)
    dw.event(7)
    block_relay(0)
    late_own()
    dw.wait_pair(2)
    late_across()
    block_relay(1)
    late_near()
    PS[...] = down(x, 1 - c).astype(BF16)
    remote(PS, PO.at[c], own_sem.at[17], sem.at[8], partner)
    late_relay()
    PO[c] = down(x, c).astype(BF16)
    await_bytes(PO.at[1 - c], sem.at[8])
    def came(m, k, rows):
        return jnp.concatenate([RC[m, k, 0, rows], RC[m, k, 1, rows]], axis=1)

    head, rest = slice(0, QUARTER), slice(QUARTER, HALF)
    await_bytes(RC.at[0], rc_recv.at[0])
    for k in (0, 1):
        FF[k, head] = PO[k, head].astype(F32) + came(1, k, head).astype(F32)
        FF[k, rest] = PO[k, rest].astype(F32) + came(0, k, rest).astype(F32)
    await_bytes(RC.at[0], rc_recv.at[1])
    sums = []
    for k in (0, 1):
        last = jnp.concatenate([came(0, k, head), came(1, k, rest)], axis=0)
        total = (FF[k] + last.astype(F32)).astype(BF16).astype(F32)
        FF[k] = total
        square = jnp.sum(total * total, axis=1, keepdims=True)
        sums.append(as_row(square))

    SQB[t] = jnp.concatenate(sums, axis=1)
    for k in range(1, 8):
        remote(SQB.at[t], SQB.at[t], own_sem.at[18], sem.at[7], (s, lax.rem(t + k, 8)))
    await_bytes(XR, sem.at[6])
    await_bytes(SQB.at[pl.ds(0, 7)], sem.at[7])
    factors = row_factors(SQB, 8)
    for k in (0, 1):
        factor = factors[HALF * k : HALF * k + HALF]
        FF[k] = FF[k] * jnp.concatenate([factor, factor], axis=1) * ffng_ref[...]
    out_ref[c] = (SO[c].astype(F32) + FF[c]).astype(BF16)
    out_ref[1 - c] = (XR[...].astype(F32) + FF[1 - c]).astype(BF16)

    gu.finish()
    dw.finish()
    await_bytes(HX, own_sem.at[0])
    await_bytes(HI, own_sem.at[1])
    await_bytes(CB, own_sem.at[7])
    await_bytes(BA.at[pl.ds(0, 3)], own_sem.at[8])
    await_bytes(OW.at[c], own_sem.at[4])
    await_bytes(RP.at[c], own_sem.at[5])
    await_bytes(GP.at[c], own_sem.at[6])
    await_bytes(BH.at[0], own_sem.at[9])
    await_bytes(SQA.at[pl.ds(0, 3)], own_sem.at[10])
    await_bytes(SQC.at[pl.ds(0, 3)], own_sem.at[11])
    await_bytes(XR, own_sem.at[13])
    await_bytes(ST.at[pl.ds(0, 3)], own_sem.at[12])
    await_bytes(PB, own_sem.at[16])
    await_bytes(PS, own_sem.at[17])
    await_bytes(SQB.at[pl.ds(0, 7)], own_sem.at[18])


def body(
    gate_branch, recur_input, doc_ids, conv_taps, gate_map, input_map, decay_level, decay_extra, out_weight,
    residual, mix_gain, pre_gain, ffn_gain, gate_weight, up_weight, down_weight,
):
    vmem = pl.BlockSpec(memory_space=pltpu.VMEM)
    dma = pltpu.SemaphoreType.DMA
    out = pl.pallas_call(
        layer_kernel,
        name="layer",
        out_shape=pltpu.VMEM((2, HALF, 256), BF16),
        in_specs=[pl.BlockSpec(memory_space=pl.ANY)] * 16,
        out_specs=vmem,
        scratch_shapes=[
            pltpu.VMEM((TOK, CH), BF16),
            pltpu.VMEM((TOK, CH), BF16),
            pltpu.VMEM((6, 128), jnp.int32),
            pltpu.VMEM((4, CH), BF16),
            pltpu.VMEM((2, 64, 64), BF16),
            pltpu.VMEM((2, 64, 64), BF16),
            pltpu.VMEM((1, CH), F32),
            pltpu.VMEM((TOK, CH), F32),
            pltpu.VMEM((2, HALF, 256), BF16),
            pltpu.VMEM((1, 256), F32),
            pltpu.VMEM((1, 256), F32),
            pltpu.VMEM((1, 256), F32),
            pltpu.VMEM((HID, 128), BF16),
            pltpu.VMEM((HID, 128), BF16),
            pltpu.VMEM((2, 16, 128, 1408), BF16),
            pltpu.VMEM((2, 16, HID, 128), BF16),
            pltpu.VMEM((2, 1024, 256), BF16),
            pltpu.VMEM((2, HALF, 256), BF16),
            pltpu.VMEM((2, 8, 256), F32),
            pltpu.VMEM((2, HALF, CH), BF16),
            pltpu.VMEM((4, 2, HALF, CH), BF16),
            pltpu.VMEM((16, CH), BF16),
            pltpu.VMEM((6, 128), jnp.int32),
            pltpu.VMEM((TOK + 8, CH), F32),
            pltpu.VMEM((TOK + 8, CH), F32),
            pltpu.VMEM((TOK, CH), F32),
            pltpu.VMEM((TOK, CH), F32),
            pltpu.VMEM((TOK, CH), F32),
            pltpu.VMEM((TOK, CH), F32),
            pltpu.VMEM((TOK, CH), F32),
            pltpu.VMEM((8, CH), F32),
            pltpu.VMEM((REACH, 8, CH), F32),
            pltpu.VMEM((2, HALF, 256), F32),
            pltpu.VMEM((4, 1, HALF), F32),
            pltpu.VMEM((2, HALF, 256), BF16),
            pltpu.VMEM((HALF, 256), BF16),
            pltpu.VMEM((4, 2, HALF, 256), BF16),
            pltpu.VMEM((4, 1, HALF), F32),
            pltpu.VMEM((HALF, 128), F32),
            pltpu.VMEM((11, HALF, 256), F32),
            pltpu.VMEM((2, HALF, HID), BF16),
            pltpu.VMEM((2, 3, 2, HALF, 128), BF16),
            pltpu.VMEM((HALF, 256), BF16),
            pltpu.VMEM((2, 2, 2, HALF // 2, 128), BF16),
            pltpu.VMEM((2, 2, 2, HALF, 128), BF16),
            pltpu.VMEM((2, HALF, 256), BF16),
            pltpu.VMEM((2, 2, HALF // 2, 128), F32),
            pltpu.VMEM((2, HALF // 2, 256), F32),
            pltpu.VMEM((2, HALF, 256), F32),
            pltpu.VMEM((2, HALF, 128), F32),
            pltpu.VMEM((3, HALF, 256), F32),
            pltpu.VMEM((8, 1, TOK), F32),
            dma((len(GROUPS),)),
            dma((len(GROUPS),)),
            dma((3,)),
            dma((3,)),
            dma((3, 2)),
            dma((3, 2)),
            dma((3, 2)),
            dma((2,)),
            dma((19,)),
            dma((12,)),
        ],
        compiler_params=pltpu.CompilerParams(
            collective_id=0, has_side_effects=True, vmem_limit_bytes=60 * 1024 * 1024
        ),
    )(
        gate_branch,
        recur_input,
        doc_ids.reshape(6, 128),
        conv_taps,
        gate_map,
        input_map,
        decay_level.reshape(1, CH),
        decay_extra,
        out_weight,
        residual.reshape(2, HALF, 256),
        mix_gain.reshape(1, 256),
        pre_gain.reshape(1, 256),
        ffn_gain.reshape(1, 256),
        gate_weight.T,
        up_weight.T,
        down_weight,
    )
    return out.reshape(TOK, 256)


def solution(mesh):
    return jax.shard_map(
        body,
        mesh=mesh,
        in_specs=(
            P("sp", "tp"),
            P("sp", "tp"),
            P("sp"),
            P(None, "tp"),
            P("tp", None, None),
            P("tp", None, None),
            P("tp"),
            P("sp", "tp"),
            P(None, "tp"),
            P("sp", "tp"),
            P("tp"),
            P("tp"),
            P("tp"),
            P("sp", "tp"),
            P("sp", "tp"),
            P("tp", "sp"),
        ),
        out_specs=P("sp", "tp"),
        check_vma=False,
    )
```

```python
import jax
import jax.numpy as jnp
from jax import lax
from jax.experimental import pallas as pl
from jax.experimental.pallas import tpu as pltpu
from jax.sharding import PartitionSpec as P

MESH = pl.DeviceIdType.MESH
F32 = jnp.float32
BF16 = jnp.bfloat16

D = 2048
EPS = 1e-06
GATE_POWER = 8.0
TOK = 768
BLK = 96
HALF = 384
CH = 128
HID = 704
REACH = 6


def neg_expm1(u):
    series = 1.0 + u * (1.0 / 9.0)
    for n in (8.0, 7.0, 6.0, 5.0, 4.0, 3.0, 2.0):
        series = 1.0 + u * (1.0 / n) * series
    return jnp.where(u > -0.5, -u * series, 1.0 - jnp.exp(u))


def softplus(v):
    tail = jnp.exp(-jnp.abs(v))
    w = tail / (2.0 + tail)
    square = w * w
    series = jnp.full_like(w, 1.0 / 15.0)
    for n in (13.0, 11.0, 9.0, 7.0, 5.0, 3.0, 1.0):
        series = 1.0 / n + square * series
    return jnp.maximum(v, 0.0) + 2.0 * w * series


TOGETHER = (
    ((0, 0, 3), (0, 0, 1)),
    ((1, 3, 0), (1, 1, 0)),
    ((0, 1, 0), (1, 0, 1)),
    ((0, 3, "m"), (1, 3, 3)),
    ((1, 1, 1), (0, 2, 0)),
    ((1, 2, 3), (0, 2, "m")),
    ((0, 3, "o"), (0, 2, "o"), (1, 0, 2), (1, 3, 2)),
    ((0, 1, 2), (0, 2, 2), (1, 1, 2), (1, 2, 2)),
)
ALONE = (
    (0, 0, 2), (1, 2, 0), (0, 3, 0), (0, 1, "m"), (0, 1, "o"), (0, 3, 2),
    (1, 0, 3), (1, 3, 1), (1, 1, 3), (1, 2, 1),
)
GROUPS = (*TOGETHER, *((one,) for one in ALONE))


class TorusGather:
    def __init__(self, buf, rows, here, ring_send, ring_recv, pair_send, pair_recv):
        self.buf, self.rows = buf, rows
        self.z, self.y, self.c, self.t = here
        self.ring_send, self.ring_recv = ring_send, ring_recv
        self.pair_send, self.pair_recv = pair_send, pair_recv
        self.odd = lax.rem(self.y, 2)
        self.mate, self.other = 1 + 2 * self.odd, 3 - 2 * self.odd

    def slot(self, dz, dy):
        return lax.rem(self.z + dz, 4) * 4 + lax.rem(self.y + dy, 4)

    def at(self, half, a, b):
        return (a, b) if half == 0 else (b, a)

    def span(self, half, part):
        quarter = self.rows // 4
        first = half * 2 * quarter
        return (first, 2 * quarter) if part is None else (first + part * quarter, quarter)

    def piece(self, half, where, part=None):
        first, count = self.span(half, part)
        return self.buf.at[self.c, self.slot(*where), pl.ds(first, count)]

    def named(self, dy):
        return dy if isinstance(dy, int) else "m" if dy is self.mate else "o"

    def group(self, half, where):
        key = (half, where[0], self.named(where[1]))
        return next(n for n, keys in enumerate(GROUPS) if key in keys)

    def send(self, half, where, to, part=None):
        ref = self.piece(half, where, part)
        dz, dy = (where[0] - to[0]) % 4, where[1]
        if isinstance(dy, int):
            dy = (dy - to[1]) % 4
        pltpu.make_async_remote_copy(
            src_ref=ref,
            dst_ref=ref,
            send_sem=self.ring_send,
            recv_sem=self.ring_recv.at[self.group(half, (dz, dy))],
            device_id=(self.slot(*to), self.t),
            device_id_type=MESH,
        ).start()

    def wait(self, *pieces):
        number = self.group(*pieces[0])
        assert len(pieces) == len(GROUPS[number])
        assert all(self.group(*piece) == number for piece in pieces)
        ref = self.piece(*pieces[0])
        if len(pieces) > 1:
            ref = self.buf.at[self.c, pl.ds(0, len(pieces) // 2)]
        pltpu.make_async_copy(ref, ref, self.ring_recv.at[number]).wait()
        for half, where in pieces:
            self.pass_over(self.piece(half, where), where)

    def pass_over(self, ref, where):
        dy = where[1]
        if isinstance(dy, int):
            stage = {0: 0, 1: 1 + self.odd, 2: 2, 3: 2 - self.odd}[dy]
        else:
            stage = 1 if dy is self.mate else 2
        pltpu.make_async_remote_copy(
            src_ref=ref,
            dst_ref=ref,
            send_sem=self.pair_send,
            recv_sem=self.pair_recv.at[stage],
            device_id=(self.slot(0, 0), self.t + 1 - 2 * self.c),
            device_id_type=MESH,
        ).start()

    def start(self):
        for half in (0, 1):
            for step in (1, 3):
                self.send(half, (0, 0), self.at(half, 0, step))

    def start_second(self):
        for half in (0, 1):
            for step in (1, 3):
                self.send(half, (0, 0), self.at(half, step, 0))
        self.pass_over(self.buf.at[self.c, self.slot(0, 0)], (0, 0))

    def spread(self, half, b, steps=(1, 3)):
        for step in steps:
            self.send(half, self.at(half, 0, b), self.at(half, step, 0))

    def relay(self, half, a, b):
        self.wait((half, self.at(half, a, b)))
        self.send(half, self.at(half, a, b), self.at(half, 4 - a, 0))

    def event(self, number):
        at, wait = self.at, self.wait
        mate, other = self.mate, self.other
        if number == 1:
            for half in (0, 1):
                wait((half, at(half, 0, 3)), (half, at(half, 0, 1)))
                self.send(half, at(half, 0, 3), at(half, 0, 1), part=0)
                self.send(half, at(half, 0, 1), at(half, 0, 3), part=1)
            self.spread(0, mate)
            self.spread(0, other, (3,))
            self.spread(1, 3)
            self.spread(1, 1)
        if number == 2:
            self.relay(0, 3, 0)
            wait((1, at(1, 0, 2)))
            self.spread(1, 2)
            wait((0, at(0, 0, 2)))
            self.spread(0, 2, (1,))
            self.spread(0, other, (1,))
            self.relay(1, 3, 0)
            wait((0, at(0, 1, 0)), (1, at(1, 1, 0)))
        if number == 3:
            self.relay(0, 1, mate)
            self.relay(1, 1, 3)
            wait((0, at(0, 3, mate)), (1, at(1, 3, 3)))
        if number == 4:
            self.relay(0, 1, other)
            self.spread(0, 2, (3,))
            self.relay(1, 3, 1)
            wait((1, at(1, 1, 1)), (0, at(0, 2, 0)))
        if number == 5:
            self.relay(1, 1, 2)
            wait((1, at(1, 3, 2)), (0, at(0, 2, mate)))
            self.relay(0, 3, 2)
        if number == 6:
            wait((0, at(0, 3, other)), (0, at(0, 2, other)), (1, at(1, 2, 0)), (1, at(1, 2, 3)))
        if number == 7:
            wait((0, at(0, 1, 2)), (0, at(0, 2, 2)), (1, at(1, 2, 1)), (1, at(1, 2, 2)))

    def wait_pair(self, stage):
        ref = self.buf.at[1 - self.c, pl.ds(0, (4, 4, 8)[stage])]
        pltpu.make_async_copy(ref, ref, self.pair_recv.at[stage]).wait()

    def finish(self):
        ref = self.buf.at[self.c, pl.ds(0, 15)]
        pltpu.make_async_copy(ref, ref, self.ring_send).wait()
        ref = self.buf.at[self.c]
        pltpu.make_async_copy(ref, ref, self.pair_send).wait()


def layer_kernel(
    gate_hbm, rec_hbm, ids_hbm, taps_hbm, gmap_hbm, imap_hbm, level_hbm, extra_hbm, ow_hbm, res_hbm,
    mixg_hbm, preg_hbm, ffng_hbm, gw_hbm, uw_hbm, dw_hbm,
    out_ref,
    gate_ref, rec_ref, ids_ref, taps_ref, gmap_ref, imap_ref, level_ref, extra_ref, res_ref,
    mixg_ref, preg_ref, ffng_ref, gw_ref, uw_ref,
    GU, DW, OW, RP, GP, BH, BA, HX, HI, XF, IDF, FA, DV, S, PR, GL, CS, CB, MX, SQA, SO, XR, ST, SQC, SC, ACC, H,
    PB, PS, RA, RC, PO, FO, FL, FF, PRE, LPRE, SQB,
    gu_ring, dw_ring, gu_pair, dw_pair, ba_ring, ag_ring, ra_recv, rc_recv, own_sem, sem,
):
    s, t = lax.axis_index("sp"), lax.axis_index("tp")
    z, y = lax.div(s, 4), lax.rem(s, 4)
    x, c = lax.div(t, 2), lax.rem(t, 2)

    def remote(src, dst, send_sem, recv_sem, device):
        copy = pltpu.make_async_remote_copy(
            src_ref=src, dst_ref=dst, send_sem=send_sem, recv_sem=recv_sem, device_id=device, device_id_type=MESH
        )
        copy.start()

    def await_bytes(ref, semaphore):
        pltpu.make_async_copy(ref, ref, semaphore).wait()

    def along_x(step):
        return (s, lax.rem(x + step, 4) * 2 + c)

    partner = (s, t + 1 - 2 * c)
    here = (z, y, c, t)
    gu = TorusGather(GU, 128, here, own_sem.at[2], gu_ring, own_sem.at[3], gu_pair)
    dw = TorusGather(DW, HID, here, own_sem.at[14], dw_ring, own_sem.at[15], dw_pair)

    barrier = pltpu.get_barrier_semaphore()
    for k in range(1, REACH + 1):
        for peer in (lax.rem(s + k, 16), lax.rem(s + 16 - k, 16)):
            pl.semaphore_signal(barrier, inc=1, device_id=(peer, t), device_id_type=MESH)
    for k in range(1, 8):
        pl.semaphore_signal(barrier, inc=1, device_id=(s, lax.rem(t + k, 8)), device_id_type=MESH)

    own = z * 4 + y
    loads = []
    for src, dst in (
        (gw_hbm, gw_ref), (uw_hbm, uw_ref), (rec_hbm, rec_ref), (ids_hbm, ids_ref), (gate_hbm, gate_ref),
        (taps_hbm, taps_ref), (gmap_hbm, gmap_ref), (imap_hbm, imap_ref), (level_hbm, level_ref),
        (extra_hbm, extra_ref), (mixg_hbm, mixg_ref), (preg_hbm, preg_ref), (ffng_hbm, ffng_ref), (ow_hbm, OW.at[c]),
        (res_hbm, res_ref), (dw_hbm, DW.at[c, own]),
    ):
        loads.append(pltpu.make_async_copy(src, dst, own_sem.at[len(loads)]))
        loads[-1].start()

    loads[0].wait()
    loads[1].wait()
    for i in range(5):
        for n, ref in enumerate((gw_ref, uw_ref)):
            block = ref[128 * i : 128 * i + 128].astype(F32).T.astype(BF16)
            GU[c, own, :, 256 * i + 128 * n : 256 * i + 128 * n + 128] = block
    block = jnp.concatenate([gw_ref[640:704].astype(F32), uw_ref[640:704].astype(F32)], axis=0)
    GU[c, own, :, 1280:1408] = block.T.astype(BF16)
    for load in loads[2:4]:
        load.wait()
    pl.semaphore_wait(barrier, 2 * REACH + 7)

    after = (lax.rem(s + 1, 16), t)
    remote(rec_ref.at[pl.ds(TOK - 16, 16)], HX, own_sem.at[0], sem.at[0], after)
    remote(ids_ref, HI, own_sem.at[1], sem.at[1], after)
    gu.start()
    for load in loads[4:]:
        load.wait()

    RP[c] = res_ref[c]
    GP[c, 0:1] = mixg_ref[...]
    GP[c, 1:2] = preg_ref[...]
    remote(OW.at[c], OW.at[c], own_sem.at[4], sem.at[9], partner)
    remote(res_ref.at[1 - c], RP.at[c], own_sem.at[5], sem.at[10], partner)
    remote(GP.at[c], GP.at[c], own_sem.at[6], sem.at[11], partner)

    IDF[8:] = jnp.concatenate(
        [jnp.broadcast_to(ids_ref[r : r + 1, :].astype(F32), (128, 128)).T for r in range(6)], axis=0
    )
    XF[8:] = rec_ref[...].astype(F32)

    for r in range(6):
        rows = slice(128 * r, 128 * r + 128)
        GL[rows] = jax.nn.gelu(gate_ref[rows].astype(F32), approximate=True)
    pair = [
        jnp.concatenate(
            [
                jnp.concatenate([m[0].astype(F32), jnp.zeros((64, 64), F32)], axis=1),
                jnp.concatenate([jnp.zeros((64, 64), F32), m[1].astype(F32)], axis=1),
            ],
            axis=0,
        )
        for m in (gmap_ref, imap_ref)
    ]
    maps = jnp.concatenate(pair, axis=1).astype(BF16)
    rate = -GATE_POWER * softplus(-level_ref[...])
    taps = taps_ref[...].astype(F32)

    def drive(r):
        at = 8 + 128 * r
        ids = IDF[at : at + 128]
        conv = XF[at : at + 128] * taps[0:1]
        for k in (1, 2, 3):
            same = IDF[at - k : at - k + 128] == ids
            conv = conv + jnp.where(same, XF[at - k : at - k + 128], 0.0) * taps[k : k + 1]
        conv = conv.astype(BF16)
        gates = jax.nn.sigmoid(jnp.dot(conv, maps, preferred_element_type=F32))
        rows = slice(128 * r, 128 * r + 128)
        log_decay = rate * gates[:, :CH] + extra_ref[rows]
        FA[rows] = jnp.where(IDF[at - 1 : at + 127] == ids, jnp.exp(log_decay), 0.0)
        DV[rows] = jnp.sqrt(neg_expm1(2.0 * log_decay)) * gates[:, CH:] * conv.astype(F32)

    for r in range(1, 6):
        drive(r)
    await_bytes(HX, sem.at[0])
    await_bytes(HI, sem.at[1])
    XF[0:8] = HX[...].astype(F32)[8:16]
    rim_ids = jnp.broadcast_to(HI[5:6, :].astype(F32), (128, 128)).T[120:128]
    IDF[0:8] = jnp.where(s > 0, rim_ids, -1.0)

    drive(0)

    state = jnp.zeros((8, CH), F32)
    prod = jnp.ones((8, CH), F32)
    for i in range(BLK):
        at = pl.ds(i, 8, stride=BLK)
        f = FA[at, :]
        state = f * state + DV[at, :]
        prod = f * prod
        S[at, :] = state
        PR[at, :] = prod
    befores = []
    p_all, e_all = jnp.ones((1, CH), F32), jnp.zeros((1, CH), F32)
    for b in range(8):
        befores.append((p_all, e_all))
        e_all = prod[b : b + 1] * e_all + state[b : b + 1]
        p_all = prod[b : b + 1] * p_all
    CS[...] = jnp.concatenate([p_all, e_all, jnp.zeros((6, CH), F32)], axis=0)
    for k in range(1, REACH + 1):
        remote(CS, CB.at[k - 1], own_sem.at[7], sem.at[2], (lax.rem(s + k, 16), t))
    gu.start_second()
    gu.event(1)

    await_bytes(CB, sem.at[2])
    entering = jnp.zeros((1, CH), F32)
    for k in range(REACH, 0, -1):
        entering = jnp.where(s >= k, CB[k - 1, 0:1] * entering + CB[k - 1, 1:2], 0.0)
    for b in range(8):
        rows = slice(BLK * b, BLK * b + BLK)
        p_before, e_before = befores[b]
        states = S[rows] + PR[rows] * (e_before + p_before * entering)
        half, first = b // 4, BLK * (b % 4)
        BH[half, first : first + BLK] = (states * GL[rows]).astype(BF16)

    QUARTER = HALF // 2
    top, bottom = pl.ds(0, QUARTER), pl.ds(QUARTER, QUARTER)
    left, right, across = lax.rem(x + 3, 4), lax.rem(x + 1, 4), lax.rem(x + 2, 4)
    for part, step in ((0, 1), (1, 3), (1, 1), (0, 3)):
        rows = bottom if part else top
        for k in (0, 1):
            remote(
                BH.at[k, rows], BA.at[x, c, rows], own_sem.at[8], ba_ring.at[0 if step == 1 else 1, part],
                (s, lax.rem(x + step, 4) * 2 + k),
            )
    remote(BH.at[1 - c], BA.at[x, c], own_sem.at[9], sem.at[5], partner)
    BA[x, c] = BH[c]
    for part, step, chip in ((0, 1, left), (1, 3, right)):
        rows = bottom if part else top
        ref = BA.at[chip, :, rows]
        await_bytes(ref, ba_ring.at[0 if step == 1 else 1, part])
        remote(ref, ref, own_sem.at[8], ba_ring.at[2, 0], along_x(step))
    gu.event(2)
    for part, step, chip in ((1, 1, left), (0, 3, right)):
        rows = bottom if part else top
        await_bytes(BA.at[chip, :, rows], ba_ring.at[0 if step == 1 else 1, part])
    await_bytes(BA.at[x, 1 - c], sem.at[5])
    await_bytes(OW.at[1 - c], sem.at[9])
    await_bytes(RP.at[1 - c], sem.at[10])
    await_bytes(GP.at[1 - c], sem.at[11])
    gu.event(3)
    await_bytes(BA.at[across], ba_ring.at[2, 0])

    def as_row(square):
        return jnp.broadcast_to(square, (HALF, 128)).T[0:1]

    def chip_sums(ref, send_sem, recv_sem):
        for step in (1, 2, 3):
            remote(ref.at[x], ref.at[x], send_sem, recv_sem, along_x(step))

    def row_factors(ref, count):
        total = ref[0]
        for j in range(1, count):
            total = total + ref[j]
        return jnp.broadcast_to(lax.rsqrt(total * (1.0 / D) + EPS), (128, total.shape[1])).T

    branch = jnp.concatenate([BA[j // 2, j % 2] for j in range(8)], axis=1)
    square = jnp.zeros((HALF, 1), F32)
    for h in (0, 1):
        mixed = jnp.dot(branch, OW[h], preferred_element_type=F32).astype(BF16).astype(F32)
        MX[h] = mixed
        square = square + jnp.sum(mixed * mixed, axis=1, keepdims=True)
    SQA[x] = as_row(square)
    chip_sums(SQA, own_sem.at[10], sem.at[3])
    dw.start()
    gu.event(4)
    await_bytes(SQA.at[pl.ds(0, 3)], sem.at[3])
    factor = row_factors(SQA, 4)
    factor = jnp.concatenate([factor, factor], axis=1)
    square = jnp.zeros((HALF, 1), F32)
    for h in (0, 1):
        stream = (RP[h].astype(F32) + MX[h] * factor * GP[h, 0:1]).astype(BF16)
        SO[h] = stream
        stream = stream.astype(F32)
        ST[x, h] = (stream * GP[h, 1:2]).astype(BF16)
        square = square + jnp.sum(stream * stream, axis=1, keepdims=True)
    SQC[x] = as_row(square)
    chip_sums(SQC, own_sem.at[11], sem.at[4])

    for part, step in ((0, 1), (1, 3), (1, 1), (0, 3)):
        ref = ST.at[x, :, bottom if part else top]
        remote(ref, ref, own_sem.at[12], ag_ring.at[0 if step == 1 else 1, part], along_x(step))
    remote(SO.at[1 - c], XR, own_sem.at[13], sem.at[6], partner)
    gu.event(5)
    dw.start_second()

    early = lax.div(y, 2)

    def product(q, h, tile):
        rows = pl.ds(4 * q + 2 * h, 2)
        if tile < 10:
            p, i = tile // 5, tile % 5
            weights = GU[p, rows, :, 256 * i : 256 * i + 256].reshape(256, 256)
        else:
            weights = jnp.concatenate([GU[p, rows, :, 1280:1408].reshape(256, 128) for p in (0, 1)], axis=1)
        return jnp.dot(ST[q, h], weights, preferred_element_type=F32)

    def gather_in(tiles):
        for tile in tiles:
            total = ACC[tile]
            for q in (x, left, right):
                total = total + product(q, 1 - early, tile)
            ACC[tile] = total

    def hidden(tiles):
        factor = SC[...]
        for tile in tiles:
            both = ACC[tile] + product(across, early, tile) + product(across, 1 - early, tile)
            if tile < 10:
                p, i = tile // 5, tile % 5
                act = jax.nn.silu(both[:, :128] * factor) * (both[:, 128:] * factor)
                H[p, :, 128 * i : 128 * i + 128] = act.astype(BF16)
            else:
                for p in (0, 1):
                    tail = both[:, 128 * p : 128 * p + 128] * factor
                    H[p, :, 640:704] = (jax.nn.silu(tail[:, :64]) * tail[:, 64:]).astype(BF16)

    dw.event(1)
    for part, step, chip in ((0, 1, left), (1, 3, right)):
        ref = ST.at[chip, :, bottom if part else top]
        await_bytes(ref, ag_ring.at[0 if step == 1 else 1, part])
        remote(ref, ref, own_sem.at[12], ag_ring.at[2, 0], along_x(step))
    gu.event(6)
    gu.wait_pair(0)
    gu.wait_pair(1)
    for tile in range(11):
        ACC[tile] = product(x, early, tile)
    gu.event(7)
    for part, step, chip in ((1, 1, left), (0, 3, right)):
        await_bytes(ST.at[chip, :, bottom if part else top], ag_ring.at[0 if step == 1 else 1, part])
    for tile in range(11):
        ACC[tile] = ACC[tile] + product(left, early, tile) + product(right, early, tile)
    dw.event(2)
    gu.wait_pair(2)
    gather_in(range(6))
    dw.event(3)
    gather_in(range(6, 11))
    await_bytes(SQC.at[pl.ds(0, 3)], sem.at[4])
    SC[...] = row_factors(SQC, 4)
    await_bytes(ST.at[across], ag_ring.at[2, 0])
    hidden(range(6))
    dw.event(4)
    hidden(range(6, 11))
    def columns(p, *slots):
        weights = jnp.concatenate([DW[p, slot] for slot in slots], axis=1)
        return jnp.dot(H[p], weights, preferred_element_type=F32)

    def down_of(p, chip, h):
        weights = jnp.concatenate([DW[p, 4 * chip + 2 * h], DW[p, 4 * chip + 2 * h + 1]], axis=1)
        return jnp.dot(H[p], weights, preferred_element_type=F32)

    def down(chip, h):
        return down_of(c, chip, h) + down_of(1 - c, chip, h)

    def send_sum(src, dst, semaphore, device):
        remote(src, dst, own_sem.at[16], semaphore, device)

    odd = lax.rem(y, 2)
    blocks = ((y, odd), (y + 1 - 2 * odd, 1 - odd))
    near = ((right, bottom, top), (left, top, bottom))

    def block_own(q):
        PRE[q] = columns(c, 4 * across + blocks[q][0])

    def block_across(q):
        slot, j = blocks[q]
        PB[0, 0, j] = (PRE[q] + columns(1 - c, 4 * across + slot)).astype(BF16)
        for m, (rows, step) in enumerate(((top, 1), (bottom, 3))):
            send_sum(PB.at[0, 0, j, rows], RA.at[0, m, j], ra_recv.at[q, m], along_x(step))

    def block_near(q):
        slot, j = blocks[q]
        slots = (4 * right + slot, 4 * left + slot)
        both = columns(c, *slots) + columns(1 - c, *slots)
        for m, (chip, rows, _) in enumerate(near):
            total = both[:, 128 * m : 128 * m + 128]
            PB[0, 1 + m, j] = total.astype(BF16)
            FO[q, m] = total[:QUARTER] if m == 0 else total[QUARTER:]
            send_sum(PB.at[0, 1 + m, j, rows], RC.at[m, c, j, rows], rc_recv.at[0], (s, 2 * chip + early))

    def block_relay(q):
        j = blocks[q][1]
        for m, (chip, _, rows) in enumerate(near):
            await_bytes(RA.at[0, m, j], ra_recv.at[q, m])
            PB[0, 1 + m, j, rows] = (FO[q, m] + RA[0, m, j].astype(F32)).astype(BF16)
            send_sum(PB.at[0, 1 + m, j, rows], RC.at[m, c, j, rows], rc_recv.at[1], (s, 2 * chip + early))

    late = 1 - early

    def late_own():
        LPRE[0] = down_of(c, across, late)
        both = columns(c, *near_slots)
        LPRE[1] = both[:, :256]
        LPRE[2] = both[:, 256:]

    near_slots = [4 * chip + 2 * late + j for chip in (right, left) for j in (0, 1)]

    def late_across():
        total = LPRE[0] + down_of(1 - c, across, late)
        for j in (0, 1):
            PB[1, 0, j] = total[:, 128 * j : 128 * j + 128].astype(BF16)
        for m, (rows, step) in enumerate(((top, 1), (bottom, 3))):
            send_sum(PB.at[1, 0, :, rows], RA.at[1, m], ra_recv.at[2, m], along_x(step))

    def late_near():
        both = columns(1 - c, *near_slots)
        for m, (chip, rows, _) in enumerate(near):
            total = LPRE[1 + m] + both[:, 256 * m : 256 * m + 256]
            FL[m] = total[:QUARTER] if m == 0 else total[QUARTER:]
            for j in (0, 1):
                PB[1, 1 + m, j] = total[:, 128 * j : 128 * j + 128].astype(BF16)
            send_sum(PB.at[1, 1 + m, :, rows], RC.at[m, c, :, rows], rc_recv.at[0], (s, 2 * chip + late))

    def late_relay():
        for m, (chip, _, rows) in enumerate(near):
            await_bytes(RA.at[1, m], ra_recv.at[2, m])
            for j in (0, 1):
                total = FL[m, :, 128 * j : 128 * j + 128] + RA[1, m, j].astype(F32)
                PB[1, 1 + m, j, rows] = total.astype(BF16)
            send_sum(PB.at[1, 1 + m, :, rows], RC.at[m, c, :, rows], rc_recv.at[1], (s, 2 * chip + late))

    block_own(0)
    dw.event(5)
    dw.wait_pair(0)
    block_across(0)
    block_near(0)
    block_own(1)
    dw.wait_pair(1)
    block_across(1)
    dw.event(6)
    block_near(1)
    dw.event(7)
    late_own()
    block_relay(0)
    dw.wait_pair(2)
    late_across()
    block_relay(1)
    late_near()
    PS[...] = down(x, 1 - c).astype(BF16)
    remote(PS, PO.at[c], own_sem.at[17], sem.at[8], partner)
    late_relay()
    PO[c] = down(x, c).astype(BF16)
    await_bytes(PO.at[1 - c], sem.at[8])
    def came(m, k, rows):
        return jnp.concatenate([RC[m, k, 0, rows], RC[m, k, 1, rows]], axis=1)

    head, rest = slice(0, QUARTER), slice(QUARTER, HALF)
    await_bytes(RC.at[0], rc_recv.at[0])
    for k in (0, 1):
        FF[k, head] = PO[k, head].astype(F32) + came(1, k, head).astype(F32)
        FF[k, rest] = PO[k, rest].astype(F32) + came(0, k, rest).astype(F32)
    await_bytes(RC.at[0], rc_recv.at[1])
    sums = []
    for k in (0, 1):
        last = jnp.concatenate([came(0, k, head), came(1, k, rest)], axis=0)
        total = (FF[k] + last.astype(F32)).astype(BF16).astype(F32)
        FF[k] = total
        square = jnp.sum(total * total, axis=1, keepdims=True)
        sums.append(as_row(square))

    SQB[t] = jnp.concatenate(sums, axis=1)
    for k in range(1, 8):
        remote(SQB.at[t], SQB.at[t], own_sem.at[18], sem.at[7], (s, lax.rem(t + k, 8)))
    await_bytes(XR, sem.at[6])
    await_bytes(SQB.at[pl.ds(0, 7)], sem.at[7])
    factors = row_factors(SQB, 8)
    for k in (0, 1):
        factor = factors[HALF * k : HALF * k + HALF]
        FF[k] = FF[k] * jnp.concatenate([factor, factor], axis=1) * ffng_ref[...]
    out_ref[c] = (SO[c].astype(F32) + FF[c]).astype(BF16)
    out_ref[1 - c] = (XR[...].astype(F32) + FF[1 - c]).astype(BF16)

    gu.finish()
    dw.finish()
    await_bytes(HX, own_sem.at[0])
    await_bytes(HI, own_sem.at[1])
    await_bytes(CB, own_sem.at[7])
    await_bytes(BA.at[pl.ds(0, 3)], own_sem.at[8])
    await_bytes(OW.at[c], own_sem.at[4])
    await_bytes(RP.at[c], own_sem.at[5])
    await_bytes(GP.at[c], own_sem.at[6])
    await_bytes(BH.at[0], own_sem.at[9])
    await_bytes(SQA.at[pl.ds(0, 3)], own_sem.at[10])
    await_bytes(SQC.at[pl.ds(0, 3)], own_sem.at[11])
    await_bytes(XR, own_sem.at[13])
    await_bytes(ST.at[pl.ds(0, 3)], own_sem.at[12])
    await_bytes(PB, own_sem.at[16])
    await_bytes(PS, own_sem.at[17])
    await_bytes(SQB.at[pl.ds(0, 7)], own_sem.at[18])


def body(
    gate_branch, recur_input, doc_ids, conv_taps, gate_map, input_map, decay_level, decay_extra, out_weight,
    residual, mix_gain, pre_gain, ffn_gain, gate_weight, up_weight, down_weight,
):
    vmem = pl.BlockSpec(memory_space=pltpu.VMEM)
    dma = pltpu.SemaphoreType.DMA
    out = pl.pallas_call(
        layer_kernel,
        name="layer",
        out_shape=pltpu.VMEM((2, HALF, 256), BF16),
        in_specs=[pl.BlockSpec(memory_space=pl.ANY)] * 16,
        out_specs=vmem,
        scratch_shapes=[
            pltpu.VMEM((TOK, CH), BF16),
            pltpu.VMEM((TOK, CH), BF16),
            pltpu.VMEM((6, 128), jnp.int32),
            pltpu.VMEM((4, CH), BF16),
            pltpu.VMEM((2, 64, 64), BF16),
            pltpu.VMEM((2, 64, 64), BF16),
            pltpu.VMEM((1, CH), F32),
            pltpu.VMEM((TOK, CH), F32),
            pltpu.VMEM((2, HALF, 256), BF16),
            pltpu.VMEM((1, 256), F32),
            pltpu.VMEM((1, 256), F32),
            pltpu.VMEM((1, 256), F32),
            pltpu.VMEM((HID, 128), BF16),
            pltpu.VMEM((HID, 128), BF16),
            pltpu.VMEM((2, 16, 128, 1408), BF16),
            pltpu.VMEM((2, 16, HID, 128), BF16),
            pltpu.VMEM((2, 1024, 256), BF16),
            pltpu.VMEM((2, HALF, 256), BF16),
            pltpu.VMEM((2, 8, 256), F32),
            pltpu.VMEM((2, HALF, CH), BF16),
            pltpu.VMEM((4, 2, HALF, CH), BF16),
            pltpu.VMEM((16, CH), BF16),
            pltpu.VMEM((6, 128), jnp.int32),
            pltpu.VMEM((TOK + 8, CH), F32),
            pltpu.VMEM((TOK + 8, CH), F32),
            pltpu.VMEM((TOK, CH), F32),
            pltpu.VMEM((TOK, CH), F32),
            pltpu.VMEM((TOK, CH), F32),
            pltpu.VMEM((TOK, CH), F32),
            pltpu.VMEM((TOK, CH), F32),
            pltpu.VMEM((8, CH), F32),
            pltpu.VMEM((REACH, 8, CH), F32),
            pltpu.VMEM((2, HALF, 256), F32),
            pltpu.VMEM((4, 1, HALF), F32),
            pltpu.VMEM((2, HALF, 256), BF16),
            pltpu.VMEM((HALF, 256), BF16),
            pltpu.VMEM((4, 2, HALF, 256), BF16),
            pltpu.VMEM((4, 1, HALF), F32),
            pltpu.VMEM((HALF, 128), F32),
            pltpu.VMEM((11, HALF, 256), F32),
            pltpu.VMEM((2, HALF, HID), BF16),
            pltpu.VMEM((2, 3, 2, HALF, 128), BF16),
            pltpu.VMEM((HALF, 256), BF16),
            pltpu.VMEM((2, 2, 2, HALF // 2, 128), BF16),
            pltpu.VMEM((2, 2, 2, HALF, 128), BF16),
            pltpu.VMEM((2, HALF, 256), BF16),
            pltpu.VMEM((2, 2, HALF // 2, 128), F32),
            pltpu.VMEM((2, HALF // 2, 256), F32),
            pltpu.VMEM((2, HALF, 256), F32),
            pltpu.VMEM((2, HALF, 128), F32),
            pltpu.VMEM((3, HALF, 256), F32),
            pltpu.VMEM((8, 1, TOK), F32),
            dma((len(GROUPS),)),
            dma((len(GROUPS),)),
            dma((3,)),
            dma((3,)),
            dma((3, 2)),
            dma((3, 2)),
            dma((3, 2)),
            dma((2,)),
            dma((19,)),
            dma((12,)),
        ],
        compiler_params=pltpu.CompilerParams(
            collective_id=0, has_side_effects=True, vmem_limit_bytes=60 * 1024 * 1024
        ),
    )(
        gate_branch,
        recur_input,
        doc_ids.reshape(6, 128),
        conv_taps,
        gate_map,
        input_map,
        decay_level.reshape(1, CH),
        decay_extra,
        out_weight,
        residual.reshape(2, HALF, 256),
        mix_gain.reshape(1, 256),
        pre_gain.reshape(1, 256),
        ffn_gain.reshape(1, 256),
        gate_weight.T,
        up_weight.T,
        down_weight,
    )
    return out.reshape(TOK, 256)


def solution(mesh):
    return jax.shard_map(
        body,
        mesh=mesh,
        in_specs=(
            P("sp", "tp"),
            P("sp", "tp"),
            P("sp"),
            P(None, "tp"),
            P("tp", None, None),
            P("tp", None, None),
            P("tp"),
            P("sp", "tp"),
            P(None, "tp"),
            P("sp", "tp"),
            P("tp"),
            P("tp"),
            P("tp"),
            P("sp", "tp"),
            P("sp", "tp"),
            P("tp", "sp"),
        ),
        out_specs=P("sp", "tp"),
        check_vma=False,
    )
```
